128 devices in a mesh: dp: 4 (over x), kv: 16 (over z, y), tp: 2 (over core).
Axes of the slice: x: 4, y: 4, z: 4, core: 2. Of those that a mesh axis runs over, the one named last changes fastest.
Arguments:
- tokens: bfloat16 [512, 2048], P('dp', 'kv'), may hold values from -18 to 18
- mix_gain: float32 [2048], P('kv'), may hold values from 0.1 to 1.9
- w_query: bfloat16 [2048, 1024], P('kv', 'tp'), may hold values from -0.125 to 0.125
- w_key: bfloat16 [2048, 1024], P('kv', 'tp'), may hold values from -0.125 to 0.125
- w_value: bfloat16 [2048, 2048], P('kv', 'tp'), may hold values from -0.125 to 0.125
- w_outgate: bfloat16 [2048, 2048], P('kv', 'tp'), may hold values from -0.125 to 0.125
- w_gates: bfloat16 [2048, 16], replicated, may hold values from -0.25 to 0.25
- forget_bias: float32 [8], P('tp'), may hold values from -1 to 3
- memory: float32 [512, 8, 128, 256], P(('dp', 'kv'), 'tp'), may hold values from -4 to 4
- normalizer: float32 [512, 8, 128], P(('dp', 'kv'), 'tp'), may hold values from -4 to 4
- stabilizer: float32 [512, 8], P(('dp', 'kv'), 'tp'), may hold values from -4 to 4
- head_gain: float32 [8, 256], P('tp'), may hold values from 0.1 to 1.9
- w_out: bfloat16 [2048, 2048], P('tp', 'kv'), may hold values from -0.125 to 0.125
- mlp_gain: float32 [2048], replicated, may hold values from 0.1 to 1.9
- w_gate: bfloat16 [2048, 5632], P(None, ('kv', 'tp')), may hold values from -0.125 to 0.125
- w_up: bfloat16 [2048, 5632], P(None, ('kv', 'tp')), may hold values from -0.125 to 0.125
- w_down: bfloat16 [5632, 2048], P(('kv', 'tp')), may hold values from -0.15625 to 0.15625
Outputs:
- mixed_out: bfloat16 [512, 2048], P('dp', ('kv', 'tp'))
- new_memory: float32 [512, 8, 128, 256], P(('dp', 'kv'), 'tp')
- new_normalizer: float32 [512, 8, 128], P(('dp', 'kv'), 'tp')
- new_stabilizer: float32 [512, 8], P(('dp', 'kv'), 'tp')
The draws below stay inside these ranges and needn't reach their ends.
All inputs are finite; a program needn't handle non-finite values.
Results may differ from the reference program's by a relative error of at most 0.02.
Values may be sent and summed in bfloat16 or wider, within the bound.
A program may use at most 64 MiB of HBM per device.

```python
import math
import jax
import jax.numpy as jnp
from jax import lax

D = 2048
HEADS = 8
QK = 128
VD = 256
FF = 5632
BATCH = 512
N_TP = 2


def draw_tokens(key, part):
    normal_key = jax.random.fold_in(jax.random.fold_in(key, 11), 0)
    columns = jnp.exp(jnp.linspace(0.0, math.log(3.0), D)).astype(jnp.float32)
    values_drawn = jnp.clip(jax.random.normal(normal_key, (BATCH, D), jnp.float32), -4.0, 4.0)
    return (values_drawn * columns).astype(jnp.bfloat16)


def strengthened(entries, stream_key, source, target, parts, factor):
    def block_of(dim):
        return (jnp.arange(entries.shape[dim]) // (entries.shape[dim] // parts)).reshape((-1,) + (1,) * (entries.ndim - 1 - dim))

    near = jax.random.permutation(stream_key, parts)[block_of(target)]
    far = (block_of(target) + parts // 2) % parts
    return jnp.where((block_of(source) == near) | (block_of(source) == far), factor * entries, entries)


def level_of(key, dims, cuts, least, largest):
    level, own = 1.0, jax.random.fold_in(key, 6)
    for axis_at, shards_of in cuts:
        heights = jnp.exp(jax.random.uniform(jax.random.fold_in(own, axis_at), (shards_of,), jnp.float32, least / len(cuts), largest / len(cuts)))
        level = level * jnp.repeat(heights, dims[axis_at] // shards_of).reshape([-1 if axis == axis_at else 1 for axis in range(len(dims))])
    return level


def centred(key, dims, width, bound, cuts=(), held_as=jnp.bfloat16):
    array = width * jax.random.normal(key, dims, jnp.float32)
    if cuts:
        array = array * level_of(key, dims, cuts, -0.22, 0.18)
    return jnp.clip(array, -bound, bound).astype(held_as)


def heavy_noise(stream_key, dims, scale, reach, shards, heavy, kind=jnp.bfloat16):
    values = scale * jax.random.normal(stream_key, dims, jnp.float32)
    if shards:
        values = values * level_of(stream_key, dims, shards, -0.22, 0.18)
    return jnp.clip(strengthened(values, jax.random.fold_in(stream_key, 3), *heavy), -reach, reach).astype(kind)


def setup_inputs(seed: int = 0) -> dict:
    arg_keys = jax.random.split(jax.random.key(seed), 18)
    tokens = draw_tokens(jax.random.fold_in(arg_keys[17], 71), 0)
    mix_gain = jnp.clip(1.0 + 0.18 * jax.random.normal(arg_keys[1], (D,), jnp.float32), 0.1, 1.9)
    w_query = centred(arg_keys[2], (D, HEADS * QK), D ** -0.5, 0.125, ((0, 16), (1, 2)))
    w_key = centred(arg_keys[3], (D, HEADS * QK), D ** -0.5, 0.125, ((0, 16), (1, 2)))
    w_value = centred(arg_keys[4], (D, HEADS * VD), D ** -0.5, 0.125, ((0, 16), (1, 2)))
    w_outgate = centred(arg_keys[5], (D, HEADS * VD), D ** -0.5, 0.125, ((0, 16), (1, 2)))
    w_gates = centred(arg_keys[6], (D, 2 * HEADS), (D // 4) ** -0.5, 0.25)
    forget_bias = jnp.clip(-1.0 + 4.0 * jax.random.uniform(arg_keys[7], (HEADS,), jnp.float32) ** level_of(arg_keys[7], (HEADS,), ((0, 2),), -0.2, 0.2), -1.0, 3.0)
    memory = centred(arg_keys[8], (BATCH, HEADS, QK, VD), 0.5, 4.0, ((0, 64), (1, 2)), jnp.float32)
    normalizer = centred(arg_keys[9], (BATCH, HEADS, QK), 0.5, 4.0, ((0, 64), (1, 2)), jnp.float32)
    stabilizer = centred(arg_keys[10], (BATCH, HEADS), 1.0, 4.0, ((0, 64), (1, 2)), jnp.float32)
    head_gain = jnp.clip(1.0 + 0.18 * jax.random.normal(arg_keys[11], (HEADS, VD), jnp.float32), 0.1, 1.9)
    w_out = centred(arg_keys[12], (HEADS * VD, D), (HEADS * VD) ** -0.5, 0.125, ((0, 2), (1, 16)))
    mlp_gain = jnp.clip(1.0 + 0.18 * jax.random.normal(arg_keys[13], (D,), jnp.float32), 0.1, 1.9)
    w_gate = centred(arg_keys[14], (D, FF), D ** -0.5, 0.125, ((1, 32),))
    w_up = centred(arg_keys[15], (D, FF), D ** -0.5, 0.125, ((1, 32),))
    w_down = heavy_noise(arg_keys[16], (FF, D), FF ** -0.5, 0.15625, ((0, 32),), (0, 1, 32, 2.75))
    return {"tokens": tokens, "mix_gain": mix_gain, "w_query": w_query, "w_key": w_key, "w_value": w_value, "w_outgate": w_outgate, "w_gates": w_gates, "forget_bias": forget_bias, "memory": memory, "normalizer": normalizer, "stabilizer": stabilizer, "head_gain": head_gain, "w_out": w_out, "mlp_gain": mlp_gain, "w_gate": w_gate, "w_up": w_up, "w_down": w_down}


EPSILON = 1e-06

def reference(tokens, mix_gain, w_query, w_key, w_value, w_outgate, w_gates, forget_bias, memory, normalizer, stabilizer, head_gain, w_out, mlp_gain, w_gate, w_up, w_down):
    activations = tokens.astype(jnp.float32)
    batch_rows = tokens.shape[0]
    inverse = lax.rsqrt(lax.optimization_barrier(jnp.mean(activations * activations, axis=1, keepdims=True)) + EPSILON)
    scaled = (activations * mix_gain).astype(jnp.bfloat16)
    query_rows = (jnp.dot(scaled, w_query, preferred_element_type=jnp.float32) * inverse).astype(jnp.bfloat16)
    key_rows = (jnp.dot(scaled, w_key, preferred_element_type=jnp.float32) * (inverse * QK ** (-0.5))).astype(jnp.bfloat16)
    value_rows = (jnp.dot(scaled, w_value, preferred_element_type=jnp.float32) * inverse).astype(jnp.bfloat16)
    outgate = (jnp.dot(scaled, w_outgate, preferred_element_type=jnp.float32) * inverse).astype(jnp.bfloat16)
    gate_pre = jnp.dot(scaled, w_gates, preferred_element_type=jnp.float32) * inverse
    input_pre = gate_pre[:, :HEADS]
    log_forget = jax.nn.log_sigmoid(gate_pre[:, HEADS:] + forget_bias)
    new_stabilizer = jnp.maximum(log_forget + stabilizer, input_pre)
    forget_scale = jnp.exp(log_forget + stabilizer - new_stabilizer)
    input_scale = jnp.exp(input_pre - new_stabilizer)
    query_heads = query_rows.astype(jnp.float32).reshape(batch_rows, HEADS, QK)
    key_heads = key_rows.astype(jnp.float32).reshape(batch_rows, HEADS, QK)
    value_heads = value_rows.astype(jnp.float32).reshape(batch_rows, HEADS, VD)
    new_normalizer = forget_scale[..., None] * normalizer + input_scale[..., None] * key_heads
    denominator = lax.optimization_barrier(jnp.sum(query_heads * new_normalizer, axis=2))
    carried = jnp.einsum('bhd,bhde->bhe', query_heads, memory, precision=lax.Precision.HIGHEST)
    query_key = lax.optimization_barrier(jnp.sum(query_heads * key_heads, axis=2))
    numerator = forget_scale[..., None] * carried + (input_scale * query_key)[..., None] * value_heads
    new_memory = forget_scale[..., None, None] * memory + (input_scale[..., None] * key_heads)[..., None] * value_heads[:, :, None, :]
    head_out = numerator / jnp.maximum(jnp.abs(denominator), 1.0)[..., None]
    normed = head_out * lax.rsqrt(lax.optimization_barrier(jnp.mean(head_out * head_out, axis=2, keepdims=True)) + EPSILON) * head_gain
    mixed_heads = (normed.reshape(batch_rows, HEADS * VD) * jax.nn.sigmoid(outgate.astype(jnp.float32))).astype(jnp.bfloat16)
    group_width = HEADS * VD // N_TP
    branch = jnp.zeros((batch_rows, D), jnp.float32)
    for group in range(N_TP):
        partial_out = jnp.dot(mixed_heads[:, group * group_width:(group + 1) * group_width], w_out[group * group_width:(group + 1) * group_width], preferred_element_type=jnp.float32).astype(jnp.bfloat16)
        branch = branch + lax.optimization_barrier(partial_out).astype(jnp.float32)
    residual = (activations + branch).astype(jnp.bfloat16)
    resid_float = residual.astype(jnp.float32)
    inverse_two = lax.rsqrt(lax.optimization_barrier(jnp.mean(resid_float * resid_float, axis=1, keepdims=True)) + EPSILON)
    mlp_in = (resid_float * inverse_two * mlp_gain).astype(jnp.bfloat16)
    gate_value = jnp.dot(mlp_in, w_gate, preferred_element_type=jnp.float32)
    up_value = jnp.dot(mlp_in, w_up, preferred_element_type=jnp.float32)
    hidden = (jax.nn.silu(gate_value) * up_value).astype(jnp.bfloat16)
    mixed_out = (jnp.dot(hidden, w_down, preferred_element_type=jnp.float32) + resid_float).astype(jnp.bfloat16)
    return (mixed_out, new_memory, new_normalizer, new_stabilizer)
```

```python
import jax
import jax.numpy as jnp
from jax import lax
from jax.experimental import pallas as pl
from jax.experimental.pallas import tpu as pltpu
from jax.sharding import PartitionSpec as P

QK = 128
VD = 256
EPSILON = 1e-06
ROW = 4
KV = 16
SEQ = 8
HEADS = 4
MESH = pl.DeviceIdType.MESH
F32 = jnp.float32
BF16 = jnp.bfloat16

FAR = sorted(
    [(a, b) for a in range(ROW) for b in range(ROW) if (a, b) != (0, 0)],
    key=lambda o: -(min(o[0], ROW - o[0]) + min(o[1], ROW - o[1])),
)


def dot(a, b):
    return jnp.dot(a, b, preferred_element_type=F32)


def layer(
    tok_h, gain_h, wq_h, wk_h, wv_h, wo_h, wgates_h, bias_h, mem_h, nrm_h, stab_h, hgain_h, wout_h, mgain_h,
    wg_h, wu_h, wd_h,
    out_ref, nmem_ref, nnrm_ref, nstab_ref,
    tok, gain, wq, wk, wv, wo, wgates, bias, mem, nrm, stab, hgain, wout, mgain, wg, wu, wd,
    pwg, pwu, pwd, ext, a1_send, a1_recv, a2_send, a2_recv, carried, heads, half_send, half_recv, resid, rows,
    down_send, down_recv,
    in_sem, a_ssem, a_rsem, w_ssem, w_rsem, c_ssem, c_rsem, d_ssem, d_rsem, e_ssem, e_rsem, g_ssem, g_rsem,
):
    me = lax.axis_index("kv")
    tp = lax.axis_index("tp")
    z, y = me // ROW, me % ROW
    other = 1 - tp

    def chip(dz, dy):
        return ((z + dz) % ROW) * ROW + (y + dy) % ROW

    barrier = pltpu.get_barrier_semaphore()
    for dz, dy in FAR:
        for core in (tp, other):
            pl.semaphore_signal(
                barrier, inc=1, device_id={"kv": chip(dz, dy), "tp": core}, device_id_type=MESH
            )
    pl.semaphore_signal(barrier, inc=1, device_id={"tp": other}, device_id_type=MESH)

    loads = {}

    def load(name, src, dst):
        loads[name] = pltpu.make_async_copy(src, dst, in_sem.at[len(loads)])
        loads[name].start()

    load("tok", tok_h, tok)
    load("gain", gain_h, gain)
    load("wq", wq_h, wq)
    load("wk", wk_h, wk)
    load("wgates", wgates_h.at[pl.ds(pl.multiple_of(me * QK, QK), QK), :], wgates)
    load("wv", wv_h, wv)
    load("wo", wo_h, wo)
    load("mem", mem_h, mem)
    load("bias", bias_h, bias)
    load("nrm", nrm_h, nrm)
    load("stab", stab_h, stab)
    load("hgain", hgain_h, hgain)
    load("wout", wout_h, wout)
    load("mgain", mgain_h, mgain)
    load("wg", wg_h, wg)
    load("wu", wu_h, wu)
    load("wd", wd_h, wd)

    def ready(*names):
        for name in names:
            loads[name].wait()

    def send(src, dst, ssem, rsem, **device):
        pltpu.make_async_remote_copy(
            src_ref=src, dst_ref=dst, send_sem=ssem, recv_sem=rsem, device_id=device, device_id_type=MESH
        ).start()

    def wait_for(ref, sem):
        pltpu.make_async_copy(ref, ref, sem).wait()

    ready("tok", "gain")
    activations = tok[...].astype(F32)
    scaled = (activations * gain[...]).astype(BF16)
    square = jnp.sum(activations * activations, axis=1, keepdims=True)
    ext[...] = jnp.zeros_like(ext)
    ready("wq", "wk", "wgates")
    ext[:, 0:16] = dot(scaled, wgates[...])
    lane = lax.broadcasted_iota(jnp.int32, (128, 128), 1)
    extra = jnp.where(lane == 16, square, ext[...])

    def put(dst, at, value):
        dst[:, :, at : at + value.shape[1]] = value.reshape(KV, SEQ, value.shape[1]).astype(BF16)

    put(a1_send, 0, dot(scaled, wq[...]))
    put(a1_send, 512, dot(scaled, wk[...]))
    put(a1_send, 1024, extra)
    pl.semaphore_wait(barrier, 2 * KV - 1)
    for slot, (dz, dy) in enumerate(FAR):
        to = chip(dz, dy)
        send(a1_send.at[to], a1_recv.at[slot], a_ssem.at[0], a_rsem.at[0], kv=to)
    ready("wv", "wo")
    put(a2_send, 0, dot(scaled, wv[...]))
    put(a2_send, 1024, dot(scaled, wo[...]))
    for slot, (dz, dy) in enumerate(FAR):
        to = chip(dz, dy)
        send(a2_send.at[to], a2_recv.at[slot], a_ssem.at[1], a_rsem.at[1], kv=to)
    for at, (src, dst) in enumerate(((wg_h, pwg), (wu_h, pwu), (wd_h, pwd))):
        send(src, dst, w_ssem.at[at], w_rsem.at[at], tp=other)

    def total_of(own, others):
        total = own[me].astype(F32)
        for slot in range(KV - 1):
            total = total + others[slot].astype(F32)
        return total

    def by_head(value, width):
        return jnp.concatenate([value[:, h * width : (h + 1) * width] for h in range(HEADS)], axis=0)

    wait_for(a1_recv, a_rsem.at[0])
    first = total_of(a1_send, a1_recv)
    inverse = lax.rsqrt(first[:, 1040:1041] * (1.0 / (KV * QK)) + EPSILON)
    query = (first[:, 0:512] * inverse).astype(BF16).astype(F32)
    key = (first[:, 512:1024] * (inverse * QK ** (-0.5))).astype(BF16).astype(F32)
    gate_pre = first[:, 1024:1152] * inverse
    low = tp == 0
    input_pre = jnp.where(low, gate_pre[:, 0:4], gate_pre[:, 4:8])
    forget_pre = jnp.where(low, gate_pre[:, 8:12], gate_pre[:, 12:16])
    ready("bias", "nrm", "stab", "hgain")
    raw = forget_pre + bias[...]
    log_forget = jnp.minimum(raw, 0.0) - jnp.log1p(jnp.exp(-jnp.abs(raw)))
    shifted = log_forget + stab[...]
    new_stab = jnp.maximum(shifted, input_pre)
    nstab_ref[...] = new_stab
    forget_scale = by_head(jnp.exp(shifted - new_stab), 1)
    input_scale = by_head(jnp.exp(input_pre - new_stab), 1)
    query_heads = by_head(query, QK)
    key_heads = by_head(key, QK)
    old_normalizer = jnp.concatenate([nrm[:, h, :] for h in range(HEADS)], axis=0)
    new_normalizer = forget_scale * old_normalizer + input_scale * key_heads
    for h in range(HEADS):
        nnrm_ref[:, h, :] = new_normalizer[h * SEQ : (h + 1) * SEQ]
    denominator = jnp.sum(query_heads * new_normalizer, axis=1, keepdims=True)
    query_key = jnp.sum(query_heads * key_heads, axis=1, keepdims=True)
    query_cols = jnp.transpose(query_heads).astype(BF16)
    key_cols = jnp.transpose(key_heads).astype(BF16)
    pair_row = lax.broadcasted_iota(jnp.int32, (HEADS * SEQ, QK), 0)
    ready("mem")
    for pair in range(HEADS * SEQ):
        h, s = pair // SEQ, pair % SEQ
        spread = dot(query_cols, jnp.where(pair_row == pair, 1.0, 0.0).astype(BF16))
        old = mem[s, h]
        low_half = jnp.sum(old[:, 0:128] * spread, axis=0, keepdims=True)
        high_half = jnp.sum(old[:, 128:256] * spread, axis=0, keepdims=True)
        carried[pair : pair + 1, 0:128] = low_half
        carried[pair : pair + 1, 128:256] = high_half

    wait_for(a2_recv, a_rsem.at[1])
    second = total_of(a2_send, a2_recv) * inverse
    value_heads = by_head(second[:, 0:1024].astype(BF16).astype(F32), VD)
    outgate = by_head(second[:, 1024:2048].astype(BF16).astype(F32), VD)
    numerator = forget_scale * carried[...] + (input_scale * query_key) * value_heads
    head_out = numerator / jnp.maximum(jnp.abs(denominator), 1.0)
    gain_rows = jnp.concatenate(
        [jnp.broadcast_to(hgain[h : h + 1, :], (SEQ, VD)) for h in range(HEADS)], axis=0
    )
    normed = (
        head_out * lax.rsqrt(jnp.mean(head_out * head_out, axis=1, keepdims=True) + EPSILON) * gain_rows
    )
    mixed = normed * jax.nn.sigmoid(outgate)
    heads[me] = jnp.concatenate(
        [mixed[h * SEQ : (h + 1) * SEQ] for h in range(HEADS)], axis=1
    ).astype(BF16)

    for dz, dy in FAR:
        send(heads.at[me], heads.at[me], c_ssem, c_rsem, kv=chip(dz, dy))
    value_row = lax.broadcasted_iota(jnp.int32, (HEADS * SEQ, VD), 0)
    for pair in range(HEADS * SEQ):
        h, s = pair // SEQ, pair % SEQ
        outer = dot(key_cols, jnp.where(value_row == pair, value_heads, 0.0).astype(BF16))
        nmem_ref[s, h] = (
            forget_scale[pair : pair + 1, :] * mem[s, h] + input_scale[pair : pair + 1, :] * outer
        )
    ready("wout", "mgain")
    wait_for(heads.at[0:15], c_rsem)
    gathered = heads[...].astype(F32).reshape(KV * SEQ, HEADS * VD).astype(BF16)

    half_send[...] = dot(gathered, wout[...]).astype(BF16)
    send(half_send, half_recv, d_ssem, d_rsem, tp=other)
    wait_for(half_recv, d_rsem)
    branch = half_send[...].astype(F32) + half_recv[...].astype(F32)
    residual = (tok[...].astype(F32) + branch).astype(BF16)
    resid[...] = residual.astype(F32)
    rows[me] = jnp.where(low, resid[0:64, :], resid[64:128, :]).astype(BF16)

    for dz, dy in FAR:
        send(rows.at[me], rows.at[me], e_ssem, e_rsem, kv=chip(dz, dy))
    ready("wg", "wu", "wd")
    wait_for(pwg, w_rsem.at[0])
    wait_for(pwu, w_rsem.at[1])
    wait_for(pwd, w_rsem.at[2])
    wait_for(rows.at[0:15], e_rsem)
    whole = jnp.concatenate([rows[j].astype(F32) for j in range(KV)], axis=1)
    inverse_two = lax.rsqrt(jnp.mean(whole * whole, axis=1, keepdims=True) + EPSILON)
    mlp_in = (whole * inverse_two * mgain[...]).astype(BF16)

    def hidden_of(gate_w, up_w):
        return (jax.nn.silu(dot(mlp_in, gate_w[...])) * dot(mlp_in, up_w[...])).astype(BF16)

    hidden_own = hidden_of(wg, wu)
    hidden_other = hidden_of(pwg, pwu)

    lane_two = lax.broadcasted_iota(jnp.int32, (32, 128), 1)
    slot = me * 2 + tp
    for dz in (2, 1, 3, 0):
        cols = pl.ds(pl.multiple_of(((z + dz) % ROW) * 512, 512), 512)
        part = dot(hidden_own, wd[:, cols]) + dot(hidden_other, pwd[:, cols])
        for at in range(ROW):
            top = part[0:32, at * 128 : (at + 1) * 128]
            bottom = part[32:64, at * 128 : (at + 1) * 128]
            down_send[dz, at, 0] = jnp.where(lane_two < 64, top, pltpu.roll(bottom, 64, 1)).astype(BF16)
            down_send[dz, at, 1] = jnp.where(lane_two < 64, pltpu.roll(top, 64, 1), bottom).astype(BF16)
        for dy in (2, 1, 3, 0):
            column = (y + dy) % ROW
            for core in (tp, other):
                if (dz, dy) != (0, 0) or core is other:
                    send(
                        down_send.at[dz, column, core], down_recv.at[slot], g_ssem, g_rsem,
                        kv=chip(dz, dy), tp=core,
                    )
    down_recv[slot] = down_send[0, y, tp]
    wait_for(down_recv.at[0:31], g_rsem)
    pieces = []
    for core in range(2):
        total = down_recv[core].astype(F32)
        for j in range(1, KV):
            total = total + down_recv[2 * j + core].astype(F32)
        pieces += [total[:, 0:64], total[:, 64:128]]
    summed = jnp.concatenate(pieces, axis=0)
    own = jnp.where(low, resid[:, 0:64], resid[:, 64:128])
    out_ref[...] = (summed + own).astype(BF16)

    wait_for(a1_recv, a_ssem.at[0])
    wait_for(a2_recv, a_ssem.at[1])
    wait_for(pwg, w_ssem.at[0])
    wait_for(pwu, w_ssem.at[1])
    wait_for(pwd, w_ssem.at[2])
    wait_for(heads.at[0:15], c_ssem)
    wait_for(half_send, d_ssem)
    wait_for(rows.at[0:15], e_ssem)
    wait_for(down_recv.at[0:31], g_ssem)


def body(tokens, mix_gain, w_query, w_key, w_value, w_outgate, w_gates, forget_bias, memory, normalizer, stabilizer,
         head_gain, w_out, mlp_gain, w_gate, w_up, w_down):
    args = (
        tokens, mix_gain.reshape(1, -1), w_query, w_key, w_value, w_outgate, w_gates, forget_bias.reshape(1, -1),
        memory, normalizer, stabilizer, head_gain, w_out, mlp_gain.reshape(1, -1), w_gate, w_up, w_down,
    )
    copies = [pltpu.VMEM(a.shape, a.dtype) for a in args]
    copies[6] = pltpu.VMEM((QK, 16), BF16)
    dma = pltpu.SemaphoreType.DMA
    return pl.pallas_call(
        layer,
        name="layer",
        out_shape=(
            jax.ShapeDtypeStruct((128, 64), BF16),
            jax.ShapeDtypeStruct(memory.shape, F32),
            jax.ShapeDtypeStruct(normalizer.shape, F32),
            jax.ShapeDtypeStruct(stabilizer.shape, F32),
        ),
        in_specs=[pl.BlockSpec(memory_space=pl.ANY)] * len(args),
        out_specs=[pl.BlockSpec(memory_space=pltpu.VMEM)] * 4,
        scratch_shapes=copies + [
            pltpu.VMEM(w_gate.shape, BF16),
            pltpu.VMEM(w_up.shape, BF16),
            pltpu.VMEM(w_down.shape, BF16),
            pltpu.VMEM((128, 128), F32),
            pltpu.VMEM((KV, SEQ, 1152), BF16),
            pltpu.VMEM((KV - 1, SEQ, 1152), BF16),
            pltpu.VMEM((KV, SEQ, 2048), BF16),
            pltpu.VMEM((KV - 1, SEQ, 2048), BF16),
            pltpu.VMEM((HEADS * SEQ, VD), F32),
            pltpu.VMEM((KV, SEQ, HEADS * VD), BF16),
            pltpu.VMEM((128, 128), BF16),
            pltpu.VMEM((128, 128), BF16),
            pltpu.VMEM((128, 128), F32),
            pltpu.VMEM((KV, 64, 128), BF16),
            pltpu.VMEM((ROW, ROW, 2, 32, 128), BF16),
            pltpu.VMEM((2 * KV, 32, 128), BF16),
            dma((len(args),)), dma((2,)), dma((2,)), dma((3,)), dma((3,)),
            dma, dma, dma, dma, dma, dma, dma, dma,
        ],
        compiler_params=pltpu.CompilerParams(
            collective_id=0, has_side_effects=True, vmem_limit_bytes=48 * 1024 * 1024
        ),
    )(*args)


def solution(mesh):
    in_specs = (
        P("dp", "kv"), P("kv"), P("kv", "tp"), P("kv", "tp"), P("kv", "tp"), P("kv", "tp"), P(), P("tp"),
        P(("dp", "kv"), "tp", None, None), P(("dp", "kv"), "tp", None), P(("dp", "kv"), "tp"), P("tp", None),
        P("tp", "kv"), P(), P(None, ("kv", "tp")), P(None, ("kv", "tp")), P(("kv", "tp"), None),
    )
    out_specs = (
        P("dp", ("kv", "tp")), P(("dp", "kv"), "tp", None, None), P(("dp", "kv"), "tp", None), P(("dp", "kv"), "tp"),
    )
    return jax.shard_map(body, mesh=mesh, in_specs=in_specs, out_specs=out_specs, check_vma=False)
```

```python
import jax
import jax.numpy as jnp
from jax import lax
from jax.experimental import pallas as pl
from jax.experimental.pallas import tpu as pltpu
from jax.sharding import PartitionSpec as P

QK = 128
VD = 256
EPSILON = 1e-06
ROW = 4
KV = 16
SEQ = 8
HEADS = 4
MESH = pl.DeviceIdType.MESH
F32 = jnp.float32
BF16 = jnp.bfloat16

FAR = sorted(
    [(a, b) for a in range(ROW) for b in range(ROW) if (a, b) != (0, 0)],
    key=lambda o: -(min(o[0], ROW - o[0]) + min(o[1], ROW - o[1])),
)


def dot(a, b):
    return jnp.dot(a, b, preferred_element_type=F32)


def dot_rows(a, b):
    return lax.dot_general(a, b, (((1,), (1,)), ((), ())), preferred_element_type=F32)


def layer(
    tok_h, gain_h, wq_h, wk_h, wv_h, wo_h, wgates_h, bias_h, mem_h, nrm_h, stab_h, hgain_h, wout_h, mgain_h,
    wg_h, wu_h, wd_h,
    out_ref, nmem_ref, nnrm_ref, nstab_ref,
    tok, gain, wq, wk, wv, wo, wgates, bias, mem, nrm, stab, hgain, wout, mgain, wg, wu, wd,
    pwg, pwu, pwd, ext, a1_send, a1_recv, a2_send, a2_recv, carried, heads, half_send, half_recv, resid, rows,
    down_send, down_recv,
    in_sem, a_ssem, a_rsem, w_ssem, w_rsem, c_ssem, c_rsem, d_ssem, d_rsem, e_ssem, e_rsem, g_ssem, g_rsem,
):
    me = lax.axis_index("kv")
    tp = lax.axis_index("tp")
    z, y = me // ROW, me % ROW
    other = 1 - tp

    def chip(dz, dy):
        return ((z + dz) % ROW) * ROW + (y + dy) % ROW

    barrier = pltpu.get_barrier_semaphore()
    for dz, dy in FAR:
        for core in (tp, other):
            pl.semaphore_signal(
                barrier, inc=1, device_id={"kv": chip(dz, dy), "tp": core}, device_id_type=MESH
            )
    pl.semaphore_signal(barrier, inc=1, device_id={"tp": other}, device_id_type=MESH)

    loads = {}

    def load(name, src, dst):
        loads[name] = pltpu.make_async_copy(src, dst, in_sem.at[len(loads)])
        loads[name].start()

    load("tok", tok_h, tok)
    load("gain", gain_h, gain)
    load("wq", wq_h, wq)
    load("wk", wk_h, wk)
    load("wgates", wgates_h.at[:, pl.ds(pl.multiple_of(me * QK, QK), QK)], wgates)
    load("wv", wv_h, wv)
    load("wo", wo_h, wo)
    load("mem", mem_h, mem)
    load("bias", bias_h, bias)
    load("nrm", nrm_h, nrm)
    load("stab", stab_h, stab)
    load("hgain", hgain_h, hgain)
    load("wout", wout_h, wout)
    load("mgain", mgain_h, mgain)
    load("wg", wg_h, wg)
    load("wu", wu_h, wu)
    load("wd", wd_h, wd)

    def ready(*names):
        for name in names:
            loads[name].wait()

    def send(src, dst, ssem, rsem, **device):
        pltpu.make_async_remote_copy(
            src_ref=src, dst_ref=dst, send_sem=ssem, recv_sem=rsem, device_id=device, device_id_type=MESH
        ).start()

    def wait_for(ref, sem):
        pltpu.make_async_copy(ref, ref, sem).wait()

    ready("tok", "gain")
    activations = tok[...].astype(F32)
    scaled = (activations * gain[...]).astype(BF16)
    square = jnp.sum(activations * activations, axis=1, keepdims=True)
    ext[...] = jnp.zeros_like(ext)
    ready("wq", "wk", "wgates")
    ext[:, 0:16] = dot_rows(scaled, wgates[...])
    lane = lax.broadcasted_iota(jnp.int32, (128, 128), 1)
    extra = jnp.where(lane == 16, square, ext[...])

    def put(dst, at, value):
        dst[:, :, at : at + value.shape[1]] = value.reshape(KV, SEQ, value.shape[1]).astype(BF16)

    put(a1_send, 0, dot(scaled, wq[...]))
    put(a1_send, 512, dot(scaled, wk[...]))
    put(a1_send, 1024, extra)
    pl.semaphore_wait(barrier, 2 * KV - 1)
    for slot, (dz, dy) in enumerate(FAR):
        to = chip(dz, dy)
        send(a1_send.at[to], a1_recv.at[slot], a_ssem.at[0], a_rsem.at[0], kv=to)
    ready("wv", "wo")
    put(a2_send, 0, dot(scaled, wv[...]))
    put(a2_send, 1024, dot(scaled, wo[...]))
    for slot, (dz, dy) in enumerate(FAR):
        to = chip(dz, dy)
        send(a2_send.at[to], a2_recv.at[slot], a_ssem.at[1], a_rsem.at[1], kv=to)
    for at, (src, dst) in enumerate(((wg_h, pwg), (wu_h, pwu), (wd_h, pwd))):
        send(src, dst, w_ssem.at[at], w_rsem.at[at], tp=other)

    def total_of(own, others):
        total = own[me].astype(F32)
        for slot in range(KV - 1):
            total = total + others[slot].astype(F32)
        return total

    def by_head(value, width):
        return jnp.concatenate([value[:, h * width : (h + 1) * width] for h in range(HEADS)], axis=0)

    wait_for(a1_recv, a_rsem.at[0])
    first = total_of(a1_send, a1_recv)
    inverse = lax.rsqrt(first[:, 1040:1041] * (1.0 / (KV * QK)) + EPSILON)
    query = (first[:, 0:512] * inverse).astype(BF16).astype(F32)
    key = (first[:, 512:1024] * (inverse * QK ** (-0.5))).astype(BF16).astype(F32)
    gate_pre = first[:, 1024:1152] * inverse
    low = tp == 0
    input_pre = jnp.where(low, gate_pre[:, 0:4], gate_pre[:, 4:8])
    forget_pre = jnp.where(low, gate_pre[:, 8:12], gate_pre[:, 12:16])
    ready("bias", "nrm", "stab", "hgain")
    raw = forget_pre + bias[...]
    log_forget = jnp.minimum(raw, 0.0) - jnp.log1p(jnp.exp(-jnp.abs(raw)))
    diagonal = lax.broadcasted_iota(jnp.int32, (SEQ, SEQ), 0) == lax.broadcasted_iota(jnp.int32, (SEQ, SEQ), 1)
    old_stab = jnp.concatenate(
        [
            jnp.sum(jnp.where(diagonal, stab[h : h + 1, :], 0.0), axis=1, keepdims=True)
            for h in range(HEADS)
        ],
        axis=1,
    )
    shifted = log_forget + old_stab
    new_stab = jnp.maximum(shifted, input_pre)
    for h in range(HEADS):
        nstab_ref[h : h + 1, :] = jnp.sum(
            jnp.where(diagonal, new_stab[:, h : h + 1], 0.0), axis=0, keepdims=True
        )
    forget_scale = by_head(jnp.exp(shifted - new_stab), 1)
    input_scale = by_head(jnp.exp(input_pre - new_stab), 1)
    query_heads = by_head(query, QK)
    key_heads = by_head(key, QK)
    old_normalizer = jnp.concatenate([nrm[:, h, :] for h in range(HEADS)], axis=0)
    new_normalizer = forget_scale * old_normalizer + input_scale * key_heads
    for h in range(HEADS):
        nnrm_ref[:, h, :] = new_normalizer[h * SEQ : (h + 1) * SEQ]
    denominator = jnp.sum(query_heads * new_normalizer, axis=1, keepdims=True)
    query_key = jnp.sum(query_heads * key_heads, axis=1, keepdims=True)
    query_cols = jnp.transpose(query_heads).astype(BF16)
    key_cols = jnp.transpose(key_heads).astype(BF16)
    pair_row = lax.broadcasted_iota(jnp.int32, (HEADS * SEQ, QK), 0)
    ready("mem")
    for pair in range(HEADS * SEQ):
        h, s = pair // SEQ, pair % SEQ
        spread = dot(query_cols, jnp.where(pair_row == pair, 1.0, 0.0).astype(BF16))
        old = mem[s, h]
        low_half = jnp.sum(old[:, 0:128] * spread, axis=0, keepdims=True)
        high_half = jnp.sum(old[:, 128:256] * spread, axis=0, keepdims=True)
        carried[pair : pair + 1, 0:128] = low_half
        carried[pair : pair + 1, 128:256] = high_half

    wait_for(a2_recv, a_rsem.at[1])
    second = total_of(a2_send, a2_recv) * inverse
    value_heads = by_head(second[:, 0:1024].astype(BF16).astype(F32), VD)
    outgate = by_head(second[:, 1024:2048].astype(BF16).astype(F32), VD)
    numerator = forget_scale * carried[...] + (input_scale * query_key) * value_heads
    head_out = numerator / jnp.maximum(jnp.abs(denominator), 1.0)
    gain_rows = jnp.concatenate(
        [jnp.broadcast_to(hgain[h : h + 1, :], (SEQ, VD)) for h in range(HEADS)], axis=0
    )
    normed = (
        head_out * lax.rsqrt(jnp.mean(head_out * head_out, axis=1, keepdims=True) + EPSILON) * gain_rows
    )
    mixed = normed * jax.nn.sigmoid(outgate)
    heads[me] = jnp.concatenate(
        [mixed[h * SEQ : (h + 1) * SEQ] for h in range(HEADS)], axis=1
    ).astype(BF16)

    for dz, dy in FAR:
        send(heads.at[me], heads.at[me], c_ssem, c_rsem, kv=chip(dz, dy))
    value_row = lax.broadcasted_iota(jnp.int32, (HEADS * SEQ, VD), 0)
    for pair in range(HEADS * SEQ):
        h, s = pair // SEQ, pair % SEQ
        outer = dot(key_cols, jnp.where(value_row == pair, value_heads, 0.0).astype(BF16))
        nmem_ref[s, h] = (
            forget_scale[pair : pair + 1, :] * mem[s, h] + input_scale[pair : pair + 1, :] * outer
        )
    ready("wout", "mgain")
    wait_for(heads.at[0:15], c_rsem)
    gathered = heads[...].astype(F32).reshape(KV * SEQ, HEADS * VD).astype(BF16)

    half_send[...] = dot(gathered, wout[...]).astype(BF16)
    send(half_send, half_recv, d_ssem, d_rsem, tp=other)
    wait_for(half_recv, d_rsem)
    branch = half_send[...].astype(F32) + half_recv[...].astype(F32)
    residual = (tok[...].astype(F32) + branch).astype(BF16)
    resid[...] = residual.astype(F32)
    rows[me] = jnp.where(low, resid[0:64, :], resid[64:128, :]).astype(BF16)

    for dz, dy in FAR:
        send(rows.at[me], rows.at[me], e_ssem, e_rsem, kv=chip(dz, dy))
    ready("wg", "wu", "wd")
    wait_for(pwg, w_rsem.at[0])
    wait_for(pwu, w_rsem.at[1])
    wait_for(pwd, w_rsem.at[2])
    wait_for(rows.at[0:15], e_rsem)
    whole = jnp.concatenate([rows[j].astype(F32) for j in range(KV)], axis=1)
    inverse_two = lax.rsqrt(jnp.mean(whole * whole, axis=1, keepdims=True) + EPSILON)
    mlp_in = (whole * inverse_two * mgain[...]).astype(BF16)

    def hidden_of(gate_w, up_w):
        return (jax.nn.silu(dot_rows(mlp_in, gate_w[...])) * dot_rows(mlp_in, up_w[...])).astype(BF16)

    hidden_own = hidden_of(wg, wu)
    hidden_other = hidden_of(pwg, pwu)

    lane_two = lax.broadcasted_iota(jnp.int32, (32, 128), 1)
    slot = me * 2 + tp
    for dz in (2, 1, 3, 0):
        cols = pl.ds(pl.multiple_of(((z + dz) % ROW) * 512, 512), 512)
        part = dot(hidden_own, wd[:, cols]) + dot(hidden_other, pwd[:, cols])
        for at in range(ROW):
            top = part[0:32, at * 128 : (at + 1) * 128]
            bottom = part[32:64, at * 128 : (at + 1) * 128]
            down_send[dz, at, 0] = jnp.where(lane_two < 64, top, pltpu.roll(bottom, 64, 1)).astype(BF16)
            down_send[dz, at, 1] = jnp.where(lane_two < 64, pltpu.roll(top, 64, 1), bottom).astype(BF16)
        for dy in (2, 1, 3, 0):
            column = (y + dy) % ROW
            for core in (tp, other):
                if (dz, dy) != (0, 0) or core is other:
                    send(
                        down_send.at[dz, column, core], down_recv.at[slot], g_ssem, g_rsem,
                        kv=chip(dz, dy), tp=core,
                    )
    down_recv[slot] = down_send[0, y, tp]
    wait_for(down_recv.at[0:31], g_rsem)
    pieces = []
    for core in range(2):
        total = down_recv[core].astype(F32)
        for j in range(1, KV):
            total = total + down_recv[2 * j + core].astype(F32)
        pieces += [total, pltpu.roll(total, 64, 1)]
    own = resid[...]
    own = jnp.where(low, own, pltpu.roll(own, 64, 1))
    summed = jnp.concatenate(pieces, axis=0) + own
    out_ref[...] = jnp.transpose(summed)[0:64, :].astype(BF16)

    wait_for(a1_recv, a_ssem.at[0])
    wait_for(a2_recv, a_ssem.at[1])
    wait_for(pwg, w_ssem.at[0])
    wait_for(pwu, w_ssem.at[1])
    wait_for(pwd, w_ssem.at[2])
    wait_for(heads.at[0:15], c_ssem)
    wait_for(half_send, d_ssem)
    wait_for(rows.at[0:15], e_ssem)
    wait_for(down_recv.at[0:31], g_ssem)


def finish(out, nmem, nnrm, nstab, out_h, nmem_h, nnrm_h, nstab_h, sem):
    copies = [(nmem.at[j], nmem_h.at[j]) for j in range(SEQ)]
    copies += [(nnrm, nnrm_h), (nstab, nstab_h), (out, out_h)]
    copies = [pltpu.make_async_copy(src, dst, sem.at[at]) for at, (src, dst) in enumerate(copies)]
    for copy in copies:
        copy.start()
    for copy in copies:
        copy.wait()


def body(tokens, mix_gain, w_query, w_key, w_value, w_outgate, w_gates, forget_bias, memory, normalizer, stabilizer,
         head_gain, w_out, mlp_gain, w_gate, w_up, w_down):
    args = (
        tokens, mix_gain.reshape(1, -1), w_query, w_key, w_value, w_outgate, w_gates.T, forget_bias.reshape(1, -1),
        memory, normalizer, stabilizer.T, head_gain, w_out, mlp_gain.reshape(1, -1), w_gate.T, w_up.T, w_down,
    )
    copies = [pltpu.VMEM(a.shape, a.dtype) for a in args]
    copies[6] = pltpu.VMEM((16, QK), BF16)
    dma = pltpu.SemaphoreType.DMA
    outs = (
        jax.ShapeDtypeStruct((64, 128), BF16),
        jax.ShapeDtypeStruct(memory.shape, F32),
        jax.ShapeDtypeStruct(normalizer.shape, F32),
        jax.ShapeDtypeStruct((HEADS, SEQ), F32),
    )
    results = pl.pallas_call(
        layer,
        name="layer",
        out_shape=tuple(pltpu.VMEM(o.shape, o.dtype) for o in outs),
        in_specs=[pl.BlockSpec(memory_space=pltpu.HBM)] * len(args),
        out_specs=[pl.BlockSpec(memory_space=pltpu.VMEM)] * 4,
        scratch_shapes=copies + [
            pltpu.VMEM(w_gate.shape[::-1], BF16),
            pltpu.VMEM(w_up.shape[::-1], BF16),
            pltpu.VMEM(w_down.shape, BF16),
            pltpu.VMEM((128, 128), F32),
            pltpu.VMEM((KV, SEQ, 1152), BF16),
            pltpu.VMEM((KV - 1, SEQ, 1152), BF16),
            pltpu.VMEM((KV, SEQ, 2048), BF16),
            pltpu.VMEM((KV - 1, SEQ, 2048), BF16),
            pltpu.VMEM((HEADS * SEQ, VD), F32),
            pltpu.VMEM((KV, SEQ, HEADS * VD), BF16),
            pltpu.VMEM((128, 128), BF16),
            pltpu.VMEM((128, 128), BF16),
            pltpu.VMEM((128, 128), F32),
            pltpu.VMEM((KV, 64, 128), BF16),
            pltpu.VMEM((ROW, ROW, 2, 32, 128), BF16),
            pltpu.VMEM((2 * KV, 32, 128), BF16),
            dma((len(args),)), dma((2,)), dma((2,)), dma((3,)), dma((3,)),
            dma, dma, dma, dma, dma, dma, dma, dma,
        ],
        compiler_params=pltpu.CompilerParams(
            collective_id=0, has_side_effects=True, vmem_limit_bytes=40 * 1024 * 1024
        ),
    )(*(pltpu.with_memory_space_constraint(a, pltpu.HBM) for a in args))
    out, new_memory, new_normalizer, new_stabilizer = pl.pallas_call(
        finish,
        name="finish",
        out_shape=outs,
        in_specs=[pl.BlockSpec(memory_space=pltpu.VMEM)] * 4,
        out_specs=[pl.BlockSpec(memory_space=pltpu.HBM)] * 4,
        scratch_shapes=[dma((SEQ + 3,))],
        compiler_params=pltpu.CompilerParams(vmem_limit_bytes=8 * 1024 * 1024),
    )(*results)
    return out.T, new_memory, new_normalizer, new_stabilizer.T


def solution(mesh):
    in_specs = (
        P("dp", "kv"), P("kv"), P("kv", "tp"), P("kv", "tp"), P("kv", "tp"), P("kv", "tp"), P(), P("tp"),
        P(("dp", "kv"), "tp", None, None), P(("dp", "kv"), "tp", None), P(("dp", "kv"), "tp"), P("tp", None),
        P("tp", "kv"), P(), P(None, ("kv", "tp")), P(None, ("kv", "tp")), P(("kv", "tp"), None),
    )
    out_specs = (
        P("dp", ("kv", "tp")), P(("dp", "kv"), "tp", None, None), P(("dp", "kv"), "tp", None), P(("dp", "kv"), "tp"),
    )
    return jax.shard_map(body, mesh=mesh, in_specs=in_specs, out_specs=out_specs, check_vma=False)
```

```python
import jax
import jax.numpy as jnp
from jax import lax
from jax.experimental import pallas as pl
from jax.experimental.pallas import tpu as pltpu
from jax.sharding import PartitionSpec as P

QK = 128
VD = 256
EPSILON = 1e-06
ROW = 4
KV = 16
SEQ = 8
HEADS = 4
MESH = pl.DeviceIdType.MESH
F32 = jnp.float32
BF16 = jnp.bfloat16

FAR = sorted(
    [(a, b) for a in range(ROW) for b in range(ROW) if (a, b) != (0, 0)],
    key=lambda o: -(min(o[0], ROW - o[0]) + min(o[1], ROW - o[1])),
)


def dot(a, b):
    return jnp.dot(a, b, preferred_element_type=F32)


def dot_rows(a, b):
    return lax.dot_general(a, b, (((1,), (1,)), ((), ())), preferred_element_type=F32)


def layer(
    tok_h, gain_h, wq_h, wk_h, wv_h, wo_h, wgates_h, bias_h, mem_h, nrm_h, stab_h, hgain_h, wout_h, mgain_h,
    wg_h, wu_h, wd_h,
    out_ref, nmem_ref, nnrm_ref, nstab_ref,
    tok, gain, wq, wk, wv, wo, wgates, bias, mem, nrm, stab, hgain, wout, mgain, wg, wu, wd,
    pwg, pwu, pwd, pwout, ext, a1_send, a1_recv, a2_send, a2_recv, carried, mixed_ref, heads, resid, rows,
    down_send, down_recv,
    in_sem, a_ssem, a_rsem, w_ssem, w_rsem, c_ssem, c_rsem, d_ssem, d_rsem, e_ssem, e_rsem, g_ssem, g_rsem,
):
    me = lax.axis_index("kv")
    tp = lax.axis_index("tp")
    z, y = me // ROW, me % ROW
    other = 1 - tp

    def chip(dz, dy):
        return ((z + dz) % ROW) * ROW + (y + dy) % ROW

    barrier = pltpu.get_barrier_semaphore()
    for dz, dy in FAR:
        for core in (tp, other):
            pl.semaphore_signal(
                barrier, inc=1, device_id={"kv": chip(dz, dy), "tp": core}, device_id_type=MESH
            )
    pl.semaphore_signal(barrier, inc=1, device_id={"tp": other}, device_id_type=MESH)

    loads = {}

    def load(name, src, dst):
        loads[name] = pltpu.make_async_copy(src, dst, in_sem.at[len(loads)])
        loads[name].start()

    load("tok", tok_h, tok)
    load("gain", gain_h, gain)
    load("wq", wq_h, wq)
    load("wk", wk_h, wk)
    load("wgates", wgates_h.at[:, pl.ds(pl.multiple_of(me * QK, QK), QK)], wgates)
    load("wv", wv_h, wv)
    load("wo", wo_h, wo)
    load("mem", mem_h, mem)
    load("bias", bias_h, bias)
    load("nrm", nrm_h, nrm)
    load("stab", stab_h, stab)
    load("hgain", hgain_h, hgain)
    load("wout", wout_h, wout)
    load("mgain", mgain_h, mgain)
    load("wg", wg_h, wg)
    load("wu", wu_h, wu)
    load("wd", wd_h, wd)

    def ready(*names):
        for name in names:
            loads[name].wait()

    def send(src, dst, ssem, rsem, **device):
        pltpu.make_async_remote_copy(
            src_ref=src, dst_ref=dst, send_sem=ssem, recv_sem=rsem, device_id=device, device_id_type=MESH
        ).start()

    def wait_for(ref, sem):
        pltpu.make_async_copy(ref, ref, sem).wait()

    ready("tok", "gain")
    activations = tok[...].astype(F32)
    scaled = (activations * gain[...]).astype(BF16)
    square = jnp.sum(activations * activations, axis=1, keepdims=True)
    ext[...] = jnp.zeros_like(ext)
    ready("wq", "wk", "wgates")
    ext[:, 0:16] = dot_rows(scaled, wgates[...])
    lane = lax.broadcasted_iota(jnp.int32, (128, 128), 1)
    extra = jnp.where(lane == 16, square, ext[...])

    def put(dst, at, value):
        dst[:, :, at : at + value.shape[1]] = value.reshape(KV, SEQ, value.shape[1]).astype(BF16)

    put(a1_send, 0, dot(scaled, wq[...]))
    put(a1_send, 512, dot(scaled, wk[...]))
    put(a1_send, 1024, extra)
    pl.semaphore_wait(barrier, 2 * KV - 1)
    for slot, (dz, dy) in enumerate(FAR):
        to = chip(dz, dy)
        send(a1_send.at[to], a1_recv.at[slot], a_ssem.at[0], a_rsem.at[0], kv=to)
    ready("wv", "wo")
    put(a2_send, 0, dot(scaled, wv[...]))
    put(a2_send, 1024, dot(scaled, wo[...]))
    for slot, (dz, dy) in enumerate(FAR):
        to = chip(dz, dy)
        send(a2_send.at[to], a2_recv.at[slot], a_ssem.at[1], a_rsem.at[1], kv=to)
    for at, (src, dst) in enumerate(((wout_h, pwout), (wg_h, pwg), (wu_h, pwu), (wd_h, pwd))):
        send(src, dst, w_ssem.at[at], w_rsem.at[at], tp=other)

    def total_of(own, others):
        total = own[me].astype(F32)
        for slot in range(KV - 1):
            total = total + others[slot].astype(F32)
        return total

    def by_head(value, width):
        return jnp.concatenate([value[:, h * width : (h + 1) * width] for h in range(HEADS)], axis=0)

    wait_for(a1_recv, a_rsem.at[0])
    first = total_of(a1_send, a1_recv)
    inverse = lax.rsqrt(first[:, 1040:1041] * (1.0 / (KV * QK)) + EPSILON)
    query = (first[:, 0:512] * inverse).astype(BF16).astype(F32)
    key = (first[:, 512:1024] * (inverse * QK ** (-0.5))).astype(BF16).astype(F32)
    gate_pre = first[:, 1024:1152] * inverse
    low = tp == 0
    input_pre = jnp.where(low, gate_pre[:, 0:4], gate_pre[:, 4:8])
    forget_pre = jnp.where(low, gate_pre[:, 8:12], gate_pre[:, 12:16])
    ready("bias", "nrm", "stab", "hgain")
    raw = forget_pre + bias[...]
    log_forget = jnp.minimum(raw, 0.0) - jnp.log1p(jnp.exp(-jnp.abs(raw)))
    diagonal = lax.broadcasted_iota(jnp.int32, (SEQ, SEQ), 0) == lax.broadcasted_iota(jnp.int32, (SEQ, SEQ), 1)
    old_stab = jnp.concatenate(
        [
            jnp.sum(jnp.where(diagonal, stab[h : h + 1, :], 0.0), axis=1, keepdims=True)
            for h in range(HEADS)
        ],
        axis=1,
    )
    shifted = log_forget + old_stab
    new_stab = jnp.maximum(shifted, input_pre)
    for h in range(HEADS):
        nstab_ref[h : h + 1, :] = jnp.sum(
            jnp.where(diagonal, new_stab[:, h : h + 1], 0.0), axis=0, keepdims=True
        )
    forget_scale = by_head(jnp.exp(shifted - new_stab), 1)
    input_scale = by_head(jnp.exp(input_pre - new_stab), 1)
    query_heads = by_head(query, QK)
    key_heads = by_head(key, QK)
    old_normalizer = jnp.concatenate([nrm[:, h, :] for h in range(HEADS)], axis=0)
    new_normalizer = forget_scale * old_normalizer + input_scale * key_heads
    for h in range(HEADS):
        nnrm_ref[:, h, :] = new_normalizer[h * SEQ : (h + 1) * SEQ]
    denominator = jnp.sum(query_heads * new_normalizer, axis=1, keepdims=True)
    query_key = jnp.sum(query_heads * key_heads, axis=1, keepdims=True)
    query_cols = jnp.transpose(query_heads).astype(BF16)
    key_cols = jnp.transpose(key_heads).astype(BF16)
    pair_row = lax.broadcasted_iota(jnp.int32, (HEADS * SEQ, QK), 0)
    ready("mem")
    for pair in range(HEADS * SEQ):
        h, s = pair // SEQ, pair % SEQ
        spread = dot(query_cols, jnp.where(pair_row == pair, 1.0, 0.0).astype(BF16))
        old = mem[s, h]
        low_half = jnp.sum(old[:, 0:128] * spread, axis=0, keepdims=True)
        high_half = jnp.sum(old[:, 128:256] * spread, axis=0, keepdims=True)
        carried[pair : pair + 1, 0:128] = low_half
        carried[pair : pair + 1, 128:256] = high_half

    wait_for(a2_recv, a_rsem.at[1])
    second = total_of(a2_send, a2_recv) * inverse
    value_heads = by_head(second[:, 0:1024].astype(BF16).astype(F32), VD)
    outgate = by_head(second[:, 1024:2048].astype(BF16).astype(F32), VD)
    numerator = forget_scale * carried[...] + (input_scale * query_key) * value_heads
    head_out = numerator / jnp.maximum(jnp.abs(denominator), 1.0)
    gain_rows = jnp.concatenate(
        [jnp.broadcast_to(hgain[h : h + 1, :], (SEQ, VD)) for h in range(HEADS)], axis=0
    )
    normed = (
        head_out * lax.rsqrt(jnp.mean(head_out * head_out, axis=1, keepdims=True) + EPSILON) * gain_rows
    )
    mixed = normed * jax.nn.sigmoid(outgate)
    mixed_ref[...] = jnp.concatenate(
        [mixed[h * SEQ : (h + 1) * SEQ] for h in range(HEADS)], axis=1
    ).astype(BF16)

    half, place = me // 8, me % 8
    for dz, dy in FAR:
        send(mixed_ref, heads.at[tp, place], c_ssem, c_rsem, kv=chip(dz, dy), tp=half)

    @pl.when(tp == half)
    def _():
        heads[tp, place] = mixed_ref[...]

    @pl.when(tp != half)
    def _():
        send(mixed_ref, heads.at[tp, place], c_ssem, c_rsem, tp=other)

    value_row = lax.broadcasted_iota(jnp.int32, (HEADS * SEQ, VD), 0)
    for pair in range(HEADS * SEQ):
        h, s = pair // SEQ, pair % SEQ
        outer = dot(key_cols, jnp.where(value_row == pair, value_heads, 0.0).astype(BF16))
        nmem_ref[s, h] = (
            forget_scale[pair : pair + 1, :] * mem[s, h] + input_scale[pair : pair + 1, :] * outer
        )
    ready("wout", "mgain")

    @pl.when(tp == half)
    def _():
        wait_for(a1_recv.at[:, :, 0:1024], c_rsem)

    @pl.when(tp != half)
    def _():
        wait_for(a1_send.at[:, :, 0:1024], c_rsem)

    def group(at, w):
        rows_of = heads[at].astype(F32).reshape(64, HEADS * VD).astype(BF16)
        return dot(rows_of, w[...]).astype(BF16).astype(F32)

    wait_for(pwout, w_rsem.at[0])
    branch = group(tp, wout) + group(other, pwout)
    own_rows = pl.ds(pl.multiple_of(tp * 64, 64), 64)
    residual = (tok[own_rows, :].astype(F32) + branch).astype(BF16)
    rows[me] = residual
    resid[tp] = residual

    for dz, dy in FAR:
        send(rows.at[me], rows.at[me], e_ssem, e_rsem, kv=chip(dz, dy))
    send(resid.at[tp], resid.at[tp], d_ssem, d_rsem, tp=other)
    ready("wg", "wu", "wd")
    wait_for(pwg, w_rsem.at[1])
    wait_for(pwu, w_rsem.at[2])
    wait_for(pwd, w_rsem.at[3])
    wait_for(rows.at[0:15], e_rsem)
    whole = jnp.concatenate([rows[j].astype(F32) for j in range(KV)], axis=1)
    inverse_two = lax.rsqrt(jnp.mean(whole * whole, axis=1, keepdims=True) + EPSILON)
    mlp_in = (whole * inverse_two * mgain[...]).astype(BF16)

    def hidden_of(gate_w, up_w):
        return (jax.nn.silu(dot_rows(mlp_in, gate_w[...])) * dot_rows(mlp_in, up_w[...])).astype(BF16)

    hidden_own = hidden_of(wg, wu)
    hidden_other = hidden_of(pwg, pwu)

    lane_two = lax.broadcasted_iota(jnp.int32, (32, 128), 1)
    slot = me * 2 + tp
    for dz in (2, 1, 3, 0):
        cols = pl.ds(pl.multiple_of(((z + dz) % ROW) * 512, 512), 512)
        part = dot(hidden_own, wd[:, cols]) + dot(hidden_other, pwd[:, cols])
        for at in range(ROW):
            top = part[0:32, at * 128 : (at + 1) * 128]
            bottom = part[32:64, at * 128 : (at + 1) * 128]
            down_send[dz, at, 0] = jnp.where(lane_two < 64, top, pltpu.roll(bottom, 64, 1)).astype(BF16)
            down_send[dz, at, 1] = jnp.where(lane_two < 64, pltpu.roll(top, 64, 1), bottom).astype(BF16)
        for dy in (2, 1, 3, 0):
            column = (y + dy) % ROW
            for core in (tp, other):
                if (dz, dy) != (0, 0) or core is other:
                    send(
                        down_send.at[dz, column, core], down_recv.at[slot], g_ssem, g_rsem,
                        kv=chip(dz, dy), tp=core,
                    )
    down_recv[slot] = down_send[0, y, tp]
    wait_for(down_recv.at[0:31], g_rsem)
    pieces = []
    for core in range(2):
        total = down_recv[core].astype(F32)
        for j in range(1, KV):
            total = total + down_recv[2 * j + core].astype(F32)
        pieces += [total, pltpu.roll(total, 64, 1)]
    wait_for(resid.at[0], d_rsem)
    own = resid[...].astype(F32).reshape(128, 128)
    own = jnp.where(low, own, pltpu.roll(own, 64, 1))
    summed = jnp.concatenate(pieces, axis=0) + own
    out_ref[...] = jnp.transpose(summed)[0:64, :].astype(BF16)

    wait_for(a1_recv, a_ssem.at[0])
    wait_for(a2_recv, a_ssem.at[1])
    wait_for(pwout, w_ssem.at[0])
    wait_for(pwg, w_ssem.at[1])
    wait_for(pwu, w_ssem.at[2])
    wait_for(pwd, w_ssem.at[3])

    @pl.when(tp == half)
    def _():
        wait_for(a1_recv.at[:, :, 0:1024], c_ssem)

    @pl.when(tp != half)
    def _():
        wait_for(a1_send.at[:, :, 0:1024], c_ssem)

    wait_for(resid.at[0], d_ssem)
    wait_for(rows.at[0:15], e_ssem)
    wait_for(down_recv.at[0:31], g_ssem)


def finish(out, nmem, nnrm, nstab, out_h, nmem_h, nnrm_h, nstab_h, sem):
    copies = [(nmem.at[j], nmem_h.at[j]) for j in range(SEQ)]
    copies += [(nnrm, nnrm_h), (nstab, nstab_h), (out, out_h)]
    copies = [pltpu.make_async_copy(src, dst, sem.at[at]) for at, (src, dst) in enumerate(copies)]
    for copy in copies:
        copy.start()
    for copy in copies:
        copy.wait()


def body(tokens, mix_gain, w_query, w_key, w_value, w_outgate, w_gates, forget_bias, memory, normalizer, stabilizer,
         head_gain, w_out, mlp_gain, w_gate, w_up, w_down):
    args = (
        tokens, mix_gain.reshape(1, -1), w_query, w_key, w_value, w_outgate, w_gates.T, forget_bias.reshape(1, -1),
        memory, normalizer, stabilizer.T, head_gain, w_out, mlp_gain.reshape(1, -1), w_gate.T, w_up.T, w_down,
    )
    copies = [pltpu.VMEM(a.shape, a.dtype) for a in args]
    copies[6] = pltpu.VMEM((16, QK), BF16)
    dma = pltpu.SemaphoreType.DMA
    outs = (
        jax.ShapeDtypeStruct((64, 128), BF16),
        jax.ShapeDtypeStruct(memory.shape, F32),
        jax.ShapeDtypeStruct(normalizer.shape, F32),
        jax.ShapeDtypeStruct((HEADS, SEQ), F32),
    )
    results = pl.pallas_call(
        layer,
        name="layer",
        out_shape=tuple(pltpu.VMEM(o.shape, o.dtype) for o in outs),
        in_specs=[pl.BlockSpec(memory_space=pltpu.HBM)] * len(args),
        out_specs=[pl.BlockSpec(memory_space=pltpu.VMEM)] * 4,
        scratch_shapes=copies + [
            pltpu.VMEM(w_gate.shape[::-1], BF16),
            pltpu.VMEM(w_up.shape[::-1], BF16),
            pltpu.VMEM(w_down.shape, BF16),
            pltpu.VMEM(w_out.shape, BF16),
            pltpu.VMEM((128, 128), F32),
            pltpu.VMEM((KV, SEQ, 1152), BF16),
            pltpu.VMEM((KV - 1, SEQ, 1152), BF16),
            pltpu.VMEM((KV, SEQ, 2048), BF16),
            pltpu.VMEM((KV - 1, SEQ, 2048), BF16),
            pltpu.VMEM((HEADS * SEQ, VD), F32),
            pltpu.VMEM((SEQ, HEADS * VD), BF16),
            pltpu.VMEM((2, KV // 2, SEQ, HEADS * VD), BF16),
            pltpu.VMEM((2, 64, 128), BF16),
            pltpu.VMEM((KV, 64, 128), BF16),
            pltpu.VMEM((ROW, ROW, 2, 32, 128), BF16),
            pltpu.VMEM((2 * KV, 32, 128), BF16),
            dma((len(args),)), dma((2,)), dma((2,)), dma((4,)), dma((4,)),
            dma, dma, dma, dma, dma, dma, dma, dma,
        ],
        compiler_params=pltpu.CompilerParams(
            collective_id=0, has_side_effects=True, vmem_limit_bytes=40 * 1024 * 1024
        ),
    )(*(pltpu.with_memory_space_constraint(a, pltpu.HBM) for a in args))
    out, new_memory, new_normalizer, new_stabilizer = pl.pallas_call(
        finish,
        name="finish",
        out_shape=outs,
        in_specs=[pl.BlockSpec(memory_space=pltpu.VMEM)] * 4,
        out_specs=[pl.BlockSpec(memory_space=pltpu.HBM)] * 4,
        scratch_shapes=[dma((SEQ + 3,))],
        compiler_params=pltpu.CompilerParams(vmem_limit_bytes=8 * 1024 * 1024),
    )(*results)
    return out.T, new_memory, new_normalizer, new_stabilizer.T


def solution(mesh):
    in_specs = (
        P("dp", "kv"), P("kv"), P("kv", "tp"), P("kv", "tp"), P("kv", "tp"), P("kv", "tp"), P(), P("tp"),
        P(("dp", "kv"), "tp", None, None), P(("dp", "kv"), "tp", None), P(("dp", "kv"), "tp"), P("tp", None),
        P("tp", "kv"), P(), P(None, ("kv", "tp")), P(None, ("kv", "tp")), P(("kv", "tp"), None),
    )
    out_specs = (
        P("dp", ("kv", "tp")), P(("dp", "kv"), "tp", None, None), P(("dp", "kv"), "tp", None), P(("dp", "kv"), "tp"),
    )
    return jax.shard_map(body, mesh=mesh, in_specs=in_specs, out_specs=out_specs, check_vma=False)
```

```python
import jax
import jax.numpy as jnp
from jax import lax
from jax.experimental import pallas as pl
from jax.experimental.pallas import tpu as pltpu
from jax.sharding import PartitionSpec as P

QK = 128
VD = 256
EPSILON = 1e-06
ROW = 4
KV = 16
SEQ = 8
HEADS = 4
MESH = pl.DeviceIdType.MESH
F32 = jnp.float32
BF16 = jnp.bfloat16

FAR = sorted(
    [(a, b) for a in range(ROW) for b in range(ROW) if (a, b) != (0, 0)],
    key=lambda o: -(min(o[0], ROW - o[0]) + min(o[1], ROW - o[1])),
)


def dot(a, b):
    return jnp.dot(a, b, preferred_element_type=F32)


def dot_rows(a, b):
    return lax.dot_general(a, b, (((1,), (1,)), ((), ())), preferred_element_type=F32)


def layer(
    tok_h, gain_h, wq_h, wk_h, wv_h, wo_h, wgates_h, bias_h, mem_h, nrm_h, stab_h, hgain_h, wout_h, mgain_h,
    wg_h, wu_h, wd_h,
    out_ref, nmem_ref, nnrm_ref, nstab_ref,
    tok, gain, wq, wk, wv, wo, wgates, bias, mem, nrm, stab, hgain, wout, mgain, wg, wu, wd,
    pwg, pwu, pwd, pwout, ext, y1_send, y1_recv, z1_send, z1_recv, y2_send, y2_recv, z2_send, z2_recv, o_send, o_recv, carried, mixed_ref, heads, resid, rows,
    down_send, down_recv,
    in_sem, a_ssem, a_rsem, b_ssem, b_rsem, o_ssem, o_rsem, w_ssem, w_rsem, c_ssem, c_rsem, d_ssem, d_rsem, e_ssem, e_rsem, g_ssem, g_rsem,
):
    me = lax.axis_index("kv")
    tp = lax.axis_index("tp")
    z, y = me // ROW, me % ROW
    other = 1 - tp

    def chip(dz, dy):
        return ((z + dz) % ROW) * ROW + (y + dy) % ROW

    barrier = pltpu.get_barrier_semaphore()
    for dz, dy in FAR:
        for core in (tp, other):
            pl.semaphore_signal(
                barrier, inc=1, device_id={"kv": chip(dz, dy), "tp": core}, device_id_type=MESH
            )
    pl.semaphore_signal(barrier, inc=1, device_id={"tp": other}, device_id_type=MESH)

    loads = {}

    def load(name, src, dst):
        loads[name] = pltpu.make_async_copy(src, dst, in_sem.at[len(loads)])
        loads[name].start()

    load("tok", tok_h, tok)
    load("gain", gain_h, gain)
    load("wq", wq_h, wq)
    load("wk", wk_h, wk)
    load("wgates", wgates_h.at[:, pl.ds(pl.multiple_of(me * QK, QK), QK)], wgates)
    load("wv", wv_h, wv)
    load("wo", wo_h, wo)
    load("mem", mem_h, mem)
    load("bias", bias_h, bias)
    load("nrm", nrm_h, nrm)
    load("stab", stab_h, stab)
    load("hgain", hgain_h, hgain)
    load("wout", wout_h, wout)
    load("mgain", mgain_h, mgain)
    load("wg", wg_h, wg)
    load("wu", wu_h, wu)
    load("wd", wd_h, wd)

    def ready(*names):
        for name in names:
            loads[name].wait()

    def send(src, dst, ssem, rsem, **device):
        pltpu.make_async_remote_copy(
            src_ref=src, dst_ref=dst, send_sem=ssem, recv_sem=rsem, device_id=device, device_id_type=MESH
        ).start()

    def wait_for(ref, sem):
        pltpu.make_async_copy(ref, ref, sem).wait()

    ready("tok", "gain")
    activations = tok[...].astype(F32)
    scaled = (activations * gain[...]).astype(BF16)
    square = jnp.sum(activations * activations, axis=1, keepdims=True)
    ext[...] = jnp.zeros_like(ext)
    ready("wq", "wk", "wgates")
    ext[:, 0:16] = dot_rows(scaled, wgates[...])
    lane = lax.broadcasted_iota(jnp.int32, (128, 128), 1)
    extra = jnp.where(lane == 16, square, ext[...])

    def put(dst, at, value):
        dst[..., at : at + value.shape[1]] = value.reshape(*dst.shape[:-1], value.shape[1]).astype(BF16)

    def first_step(at, ycols, zcols):
        for step in (2, 1, 3):
            column = (y + step) % ROW
            send(
                y1_send.at[:, column, :, ycols], y1_recv.at[step - 1, :, :, ycols], a_ssem.at[at], a_rsem.at[at],
                kv=chip(0, step),
            )
            row = (z + step) % ROW
            send(
                z1_send.at[row, :, :, zcols], z1_recv.at[step - 1, :, :, zcols], a_ssem.at[at + 2], a_rsem.at[at + 2],
                kv=chip(step, 0),
            )

    def second_step(at, ycols, zcols):
        wait_for(y1_recv.at[:, :, :, ycols], a_rsem.at[at])
        total = y1_send[:, y, :, ycols].astype(F32)
        for slot in range(ROW - 1):
            total = total + y1_recv[slot, :, :, ycols].astype(F32)
        y2_send[:, :, ycols] = total.astype(BF16)
        for step in (2, 1, 3):
            row = (z + step) % ROW
            send(
                y2_send.at[row, :, ycols], y2_recv.at[step - 1, :, ycols], b_ssem.at[at], b_rsem.at[at],
                kv=chip(step, 0),
            )
        wait_for(z1_recv.at[:, :, :, zcols], a_rsem.at[at + 2])
        total = z1_send[z, :, :, zcols].astype(F32)
        for slot in range(ROW - 1):
            total = total + z1_recv[slot, :, :, zcols].astype(F32)
        z2_send[:, :, zcols] = total.astype(BF16)
        for step in (2, 1, 3):
            column = (y + step) % ROW
            send(
                z2_send.at[column, :, zcols], z2_recv.at[step - 1, :, zcols], b_ssem.at[at + 2], b_rsem.at[at + 2],
                kv=chip(0, step),
            )

    def arrived(at, send_buf, recv_buf, mine, cols):
        wait_for(recv_buf.at[:, :, cols], b_rsem.at[at])
        total = send_buf[mine, :, cols].astype(F32)
        for slot in range(ROW - 1):
            total = total + recv_buf[slot, :, cols].astype(F32)
        return total

    put(y1_send, 0, dot(scaled, wq[...]))
    put(y1_send, 512, extra)
    put(z1_send, 0, dot(scaled, wk[...]))
    pl.semaphore_wait(barrier, 2 * KV - 1)
    early_y, early_z, late_y, late_z = pl.ds(0, 640), pl.ds(0, 512), pl.ds(640, 512), pl.ds(512, 512)
    first_step(0, early_y, early_z)
    ready("wv")
    put(y1_send, 640, dot(scaled, wv[:, 0:512]))
    put(z1_send, 512, dot(scaled, wv[:, 512:1024]))
    first_step(1, late_y, late_z)
    ready("wo")
    put(o_send, 0, dot(scaled, wo[...]))
    for slot, (dz, dy) in enumerate(FAR):
        to = chip(dz, dy)
        send(o_send.at[to // ROW, to % ROW], o_recv.at[slot], o_ssem, o_rsem, kv=to)
    second_step(0, early_y, early_z)
    second_step(1, late_y, late_z)
    for at, (src, dst) in enumerate(((wout_h, pwout), (wg_h, pwg), (wu_h, pwu), (wd_h, pwd))):
        send(src, dst, w_ssem.at[at], w_rsem.at[at], tp=other)

    def by_head(value, width):
        return jnp.concatenate([value[:, h * width : (h + 1) * width] for h in range(HEADS)], axis=0)

    first = arrived(0, y2_send, y2_recv, z, early_y)
    inverse = lax.rsqrt(first[:, 528:529] * (1.0 / (KV * QK)) + EPSILON)
    query = (first[:, 0:512] * inverse).astype(BF16).astype(F32)
    key_sum = arrived(2, z2_send, z2_recv, y, early_z)
    key = (key_sum * (inverse * QK ** (-0.5))).astype(BF16).astype(F32)
    gate_pre = first[:, 512:640] * inverse
    low = tp == 0
    input_pre = jnp.where(low, gate_pre[:, 0:4], gate_pre[:, 4:8])
    forget_pre = jnp.where(low, gate_pre[:, 8:12], gate_pre[:, 12:16])
    ready("bias", "nrm", "stab", "hgain")
    raw = forget_pre + bias[...]
    log_forget = jnp.minimum(raw, 0.0) - jnp.log1p(jnp.exp(-jnp.abs(raw)))
    diagonal = lax.broadcasted_iota(jnp.int32, (SEQ, SEQ), 0) == lax.broadcasted_iota(jnp.int32, (SEQ, SEQ), 1)
    old_stab = jnp.concatenate(
        [
            jnp.sum(jnp.where(diagonal, stab[h : h + 1, :], 0.0), axis=1, keepdims=True)
            for h in range(HEADS)
        ],
        axis=1,
    )
    shifted = log_forget + old_stab
    new_stab = jnp.maximum(shifted, input_pre)
    for h in range(HEADS):
        nstab_ref[h : h + 1, :] = jnp.sum(
            jnp.where(diagonal, new_stab[:, h : h + 1], 0.0), axis=0, keepdims=True
        )
    forget_scale = by_head(jnp.exp(shifted - new_stab), 1)
    input_scale = by_head(jnp.exp(input_pre - new_stab), 1)
    query_heads = by_head(query, QK)
    key_heads = by_head(key, QK)
    old_normalizer = jnp.concatenate([nrm[:, h, :] for h in range(HEADS)], axis=0)
    new_normalizer = forget_scale * old_normalizer + input_scale * key_heads
    for h in range(HEADS):
        nnrm_ref[:, h, :] = new_normalizer[h * SEQ : (h + 1) * SEQ]
    denominator = jnp.sum(query_heads * new_normalizer, axis=1, keepdims=True)
    query_key = jnp.sum(query_heads * key_heads, axis=1, keepdims=True)
    query_cols = jnp.transpose(query_heads).astype(BF16)
    key_cols = jnp.transpose(key_heads).astype(BF16)
    pair_row = lax.broadcasted_iota(jnp.int32, (HEADS * SEQ, QK), 0)
    ready("mem")
    for pair in range(HEADS * SEQ):
        h, s = pair // SEQ, pair % SEQ
        spread = dot(query_cols, jnp.where(pair_row == pair, 1.0, 0.0).astype(BF16))
        old = mem[s, h]
        low_half = jnp.sum(old[:, 0:128] * spread, axis=0, keepdims=True)
        high_half = jnp.sum(old[:, 128:256] * spread, axis=0, keepdims=True)
        carried[pair : pair + 1, 0:128] = low_half
        carried[pair : pair + 1, 128:256] = high_half

    value_sum = jnp.concatenate(
        [arrived(1, y2_send, y2_recv, z, late_y), arrived(3, z2_send, z2_recv, y, late_z)], axis=1
    )
    value_heads = by_head((value_sum * inverse).astype(BF16).astype(F32), VD)
    numerator = forget_scale * carried[...] + (input_scale * query_key) * value_heads
    head_out = numerator / jnp.maximum(jnp.abs(denominator), 1.0)
    gain_rows = jnp.concatenate(
        [jnp.broadcast_to(hgain[h : h + 1, :], (SEQ, VD)) for h in range(HEADS)], axis=0
    )
    normed = (
        head_out * lax.rsqrt(jnp.mean(head_out * head_out, axis=1, keepdims=True) + EPSILON) * gain_rows
    )
    wait_for(o_recv, o_rsem)
    outgate_sum = o_send[z, y].astype(F32)
    for slot in range(KV - 1):
        outgate_sum = outgate_sum + o_recv[slot].astype(F32)
    outgate = by_head((outgate_sum * inverse).astype(BF16).astype(F32), VD)
    mixed = normed * jax.nn.sigmoid(outgate)
    mixed_ref[...] = jnp.concatenate(
        [mixed[h * SEQ : (h + 1) * SEQ] for h in range(HEADS)], axis=1
    ).astype(BF16)

    half, place = me // 8, me % 8
    for dz, dy in FAR:
        send(mixed_ref, heads.at[tp, place], c_ssem, c_rsem, kv=chip(dz, dy), tp=half)

    @pl.when(tp == half)
    def _():
        heads[tp, place] = mixed_ref[...]

    @pl.when(tp != half)
    def _():
        send(mixed_ref, heads.at[tp, place], c_ssem, c_rsem, tp=other)

    value_row = lax.broadcasted_iota(jnp.int32, (HEADS * SEQ, VD), 0)
    for pair in range(HEADS * SEQ):
        h, s = pair // SEQ, pair % SEQ
        outer = dot(key_cols, jnp.where(value_row == pair, value_heads, 0.0).astype(BF16))
        nmem_ref[s, h] = (
            forget_scale[pair : pair + 1, :] * mem[s, h] + input_scale[pair : pair + 1, :] * outer
        )
    ready("wout", "mgain")

    @pl.when(tp == half)
    def _():
        wait_for(o_recv, c_rsem)

    @pl.when(tp != half)
    def _():
        wait_for(o_send, c_rsem)

    def group(at, w):
        rows_of = heads[at].astype(F32).reshape(64, HEADS * VD).astype(BF16)
        return dot(rows_of, w[...]).astype(BF16).astype(F32)

    wait_for(pwout, w_rsem.at[0])
    branch = group(tp, wout) + group(other, pwout)
    own_rows = pl.ds(pl.multiple_of(tp * 64, 64), 64)
    residual = (tok[own_rows, :].astype(F32) + branch).astype(BF16)
    rows[me] = residual
    resid[tp] = residual

    for dz, dy in FAR:
        send(rows.at[me], rows.at[me], e_ssem, e_rsem, kv=chip(dz, dy))
    send(resid.at[tp], resid.at[tp], d_ssem, d_rsem, tp=other)
    ready("wg", "wu", "wd")
    wait_for(pwg, w_rsem.at[1])
    wait_for(pwu, w_rsem.at[2])
    wait_for(pwd, w_rsem.at[3])
    wait_for(rows.at[0:15], e_rsem)
    whole = jnp.concatenate([rows[j].astype(F32) for j in range(KV)], axis=1)
    inverse_two = lax.rsqrt(jnp.mean(whole * whole, axis=1, keepdims=True) + EPSILON)
    mlp_in = (whole * inverse_two * mgain[...]).astype(BF16)

    def hidden_of(gate_w, up_w):
        return (jax.nn.silu(dot_rows(mlp_in, gate_w[...])) * dot_rows(mlp_in, up_w[...])).astype(BF16)

    hidden_own = hidden_of(wg, wu)
    hidden_other = hidden_of(pwg, pwu)

    lane_two = lax.broadcasted_iota(jnp.int32, (32, 128), 1)
    slot = me * 2 + tp
    for dz in (2, 1, 3, 0):
        cols = pl.ds(pl.multiple_of(((z + dz) % ROW) * 512, 512), 512)
        part = dot(hidden_own, wd[:, cols]) + dot(hidden_other, pwd[:, cols])
        for at in range(ROW):
            top = part[0:32, at * 128 : (at + 1) * 128]
            bottom = part[32:64, at * 128 : (at + 1) * 128]
            down_send[dz, at, 0] = jnp.where(lane_two < 64, top, pltpu.roll(bottom, 64, 1)).astype(BF16)
            down_send[dz, at, 1] = jnp.where(lane_two < 64, pltpu.roll(top, 64, 1), bottom).astype(BF16)
        for dy in (2, 1, 3, 0):
            column = (y + dy) % ROW
            for core in (tp, other):
                if (dz, dy) != (0, 0) or core is other:
                    send(
                        down_send.at[dz, column, core], down_recv.at[slot], g_ssem, g_rsem,
                        kv=chip(dz, dy), tp=core,
                    )
    down_recv[slot] = down_send[0, y, tp]
    wait_for(down_recv.at[0:31], g_rsem)
    pieces = []
    for core in range(2):
        total = down_recv[core].astype(F32)
        for j in range(1, KV):
            total = total + down_recv[2 * j + core].astype(F32)
        pieces += [total, pltpu.roll(total, 64, 1)]
    wait_for(resid.at[0], d_rsem)
    own = resid[...].astype(F32).reshape(128, 128)
    own = jnp.where(low, own, pltpu.roll(own, 64, 1))
    summed = jnp.concatenate(pieces, axis=0) + own
    out_ref[...] = jnp.transpose(summed)[0:64, :].astype(BF16)

    for at, ycols, zcols in ((0, early_y, early_z), (1, late_y, late_z)):
        wait_for(y1_recv.at[:, :, :, ycols], a_ssem.at[at])
        wait_for(z1_recv.at[:, :, :, zcols], a_ssem.at[at + 2])
        wait_for(y2_recv.at[:, :, ycols], b_ssem.at[at])
        wait_for(z2_recv.at[:, :, zcols], b_ssem.at[at + 2])
    wait_for(o_recv, o_ssem)
    wait_for(pwout, w_ssem.at[0])
    wait_for(pwg, w_ssem.at[1])
    wait_for(pwu, w_ssem.at[2])
    wait_for(pwd, w_ssem.at[3])

    @pl.when(tp == half)
    def _():
        wait_for(o_recv, c_ssem)

    @pl.when(tp != half)
    def _():
        wait_for(o_send, c_ssem)

    wait_for(resid.at[0], d_ssem)
    wait_for(rows.at[0:15], e_ssem)
    wait_for(down_recv.at[0:31], g_ssem)


def finish(out, nmem, nnrm, nstab, out_h, nmem_h, nnrm_h, nstab_h, sem):
    copies = [(nmem.at[j], nmem_h.at[j]) for j in range(SEQ)]
    copies += [(nnrm, nnrm_h), (nstab, nstab_h), (out, out_h)]
    copies = [pltpu.make_async_copy(src, dst, sem.at[at]) for at, (src, dst) in enumerate(copies)]
    for copy in copies:
        copy.start()
    for copy in copies:
        copy.wait()


def body(tokens, mix_gain, w_query, w_key, w_value, w_outgate, w_gates, forget_bias, memory, normalizer, stabilizer,
         head_gain, w_out, mlp_gain, w_gate, w_up, w_down):
    args = (
        tokens, mix_gain.reshape(1, -1), w_query, w_key, w_value, w_outgate, w_gates.T, forget_bias.reshape(1, -1),
        memory, normalizer, stabilizer.T, head_gain, w_out, mlp_gain.reshape(1, -1), w_gate.T, w_up.T, w_down,
    )
    copies = [pltpu.VMEM(a.shape, a.dtype) for a in args]
    copies[6] = pltpu.VMEM((16, QK), BF16)
    dma = pltpu.SemaphoreType.DMA
    outs = (
        jax.ShapeDtypeStruct((64, 128), BF16),
        jax.ShapeDtypeStruct(memory.shape, F32),
        jax.ShapeDtypeStruct(normalizer.shape, F32),
        jax.ShapeDtypeStruct((HEADS, SEQ), F32),
    )
    results = pl.pallas_call(
        layer,
        name="layer",
        out_shape=tuple(pltpu.VMEM(o.shape, o.dtype) for o in outs),
        in_specs=[pl.BlockSpec(memory_space=pltpu.HBM)] * len(args),
        out_specs=[pl.BlockSpec(memory_space=pltpu.VMEM)] * 4,
        scratch_shapes=copies + [
            pltpu.VMEM(w_gate.shape[::-1], BF16),
            pltpu.VMEM(w_up.shape[::-1], BF16),
            pltpu.VMEM(w_down.shape, BF16),
            pltpu.VMEM(w_out.shape, BF16),
            pltpu.VMEM((128, 128), F32),
            pltpu.VMEM((ROW, ROW, SEQ, 1152), BF16),
            pltpu.VMEM((ROW - 1, ROW, SEQ, 1152), BF16),
            pltpu.VMEM((ROW, ROW, SEQ, 1024), BF16),
            pltpu.VMEM((ROW - 1, ROW, SEQ, 1024), BF16),
            pltpu.VMEM((ROW, SEQ, 1152), BF16),
            pltpu.VMEM((ROW - 1, SEQ, 1152), BF16),
            pltpu.VMEM((ROW, SEQ, 1024), BF16),
            pltpu.VMEM((ROW - 1, SEQ, 1024), BF16),
            pltpu.VMEM((ROW, ROW, SEQ, 1024), BF16),
            pltpu.VMEM((KV - 1, SEQ, 1024), BF16),
            pltpu.VMEM((HEADS * SEQ, VD), F32),
            pltpu.VMEM((SEQ, HEADS * VD), BF16),
            pltpu.VMEM((2, KV // 2, SEQ, HEADS * VD), BF16),
            pltpu.VMEM((2, 64, 128), BF16),
            pltpu.VMEM((KV, 64, 128), BF16),
            pltpu.VMEM((ROW, ROW, 2, 32, 128), BF16),
            pltpu.VMEM((2 * KV, 32, 128), BF16),
            dma((len(args),)), dma((4,)), dma((4,)), dma((4,)), dma((4,)), dma, dma, dma((4,)), dma((4,)),
            dma, dma, dma, dma, dma, dma, dma, dma,
        ],
        compiler_params=pltpu.CompilerParams(
            collective_id=0, has_side_effects=True, vmem_limit_bytes=40 * 1024 * 1024
        ),
    )(*(pltpu.with_memory_space_constraint(a, pltpu.HBM) for a in args))
    out, new_memory, new_normalizer, new_stabilizer = pl.pallas_call(
        finish,
        name="finish",
        out_shape=outs,
        in_specs=[pl.BlockSpec(memory_space=pltpu.VMEM)] * 4,
        out_specs=[pl.BlockSpec(memory_space=pltpu.HBM)] * 4,
        scratch_shapes=[dma((SEQ + 3,))],
        compiler_params=pltpu.CompilerParams(vmem_limit_bytes=8 * 1024 * 1024),
    )(*results)
    return out.T, new_memory, new_normalizer, new_stabilizer.T


def solution(mesh):
    in_specs = (
        P("dp", "kv"), P("kv"), P("kv", "tp"), P("kv", "tp"), P("kv", "tp"), P("kv", "tp"), P(), P("tp"),
        P(("dp", "kv"), "tp", None, None), P(("dp", "kv"), "tp", None), P(("dp", "kv"), "tp"), P("tp", None),
        P("tp", "kv"), P(), P(None, ("kv", "tp")), P(None, ("kv", "tp")), P(("kv", "tp"), None),
    )
    out_specs = (
        P("dp", ("kv", "tp")), P(("dp", "kv"), "tp", None, None), P(("dp", "kv"), "tp", None), P(("dp", "kv"), "tp"),
    )
    return jax.shard_map(body, mesh=mesh, in_specs=in_specs, out_specs=out_specs, check_vma=False)
```

```python
import jax
import jax.numpy as jnp
from jax import lax
from jax.experimental import pallas as pl
from jax.experimental.pallas import tpu as pltpu
from jax.sharding import PartitionSpec as P

QK = 128
VD = 256
EPSILON = 1e-06
ROW = 4
KV = 16
SEQ = 8
HEADS = 4
MESH = pl.DeviceIdType.MESH
F32 = jnp.float32
BF16 = jnp.bfloat16

FAR = sorted(
    [(a, b) for a in range(ROW) for b in range(ROW) if (a, b) != (0, 0)],
    key=lambda o: -(min(o[0], ROW - o[0]) + min(o[1], ROW - o[1])),
)


def dot(a, b):
    return jnp.dot(a, b, preferred_element_type=F32)


def dot_rows(a, b):
    return lax.dot_general(a, b, (((1,), (1,)), ((), ())), preferred_element_type=F32)


def layer(
    tok_h, gain_h, wq_h, wk_h, wv_h, wo_h, wgates_h, bias_h, mem_h, nrm_h, stab_h, hgain_h, wout_h, mgain_h,
    wg_h, wu_h, wd_h,
    out_ref, nmem_ref, nnrm_ref, nstab_ref,
    tok, gain, wq, wk, wv, wo, wgates, bias, mem, nrm, stab, hgain, wout, mgain, wg, wu, wd,
    pwg, pwu, pwd, pwout, ext, y1_send, y1_recv, z1_send, z1_recv, y2_send, y2_recv, z2_send, z2_recv, o_send, o_recv, carried, mixed_ref, heads, resid, rows,
    down_send, down_recv,
    plane_sem, in_sem, a_ssem, a_rsem, b_ssem, b_rsem, o_ssem, o_rsem, w_ssem, w_rsem, c_ssem, c_rsem, d_ssem, d_rsem, e_ssem, e_rsem, g_ssem, g_rsem,
):
    me = lax.axis_index("kv")
    tp = lax.axis_index("tp")
    z, y = me // ROW, me % ROW
    other = 1 - tp

    def chip(dz, dy):
        return ((z + dz) % ROW) * ROW + (y + dy) % ROW

    barrier = pltpu.get_barrier_semaphore()
    for step in (2, 1, 3):
        pl.semaphore_signal(barrier, inc=1, device_id={"kv": chip(step, 0)}, device_id_type=MESH)
        pl.semaphore_signal(barrier, inc=1, device_id={"kv": chip(0, step)}, device_id_type=MESH)
    pl.semaphore_signal(barrier, inc=1, device_id={"tp": other}, device_id_type=MESH)

    loads = {}

    def load(name, src, dst):
        loads[name] = pltpu.make_async_copy(src, dst, in_sem.at[len(loads)])
        loads[name].start()

    load("tok", tok_h, tok)
    load("gain", gain_h, gain)
    load("wq", wq_h, wq)
    load("wk", wk_h, wk)
    load("wgates", wgates_h.at[:, pl.ds(pl.multiple_of(me * QK, QK), QK)], wgates)
    load("wv", wv_h, wv)
    load("wo", wo_h, wo)
    load("mem", mem_h, mem)
    load("bias", bias_h, bias)
    load("nrm", nrm_h, nrm)
    load("stab", stab_h, stab)
    load("hgain", hgain_h, hgain)
    load("wout", wout_h, wout)
    load("mgain", mgain_h, mgain)
    load("wg", wg_h, wg)
    load("wu", wu_h, wu)
    load("wd", wd_h, wd)

    def ready(*names):
        for name in names:
            loads[name].wait()

    def send(src, dst, ssem, rsem, **device):
        pltpu.make_async_remote_copy(
            src_ref=src, dst_ref=dst, send_sem=ssem, recv_sem=rsem, device_id=device, device_id_type=MESH
        ).start()

    def wait_for(ref, sem):
        pltpu.make_async_copy(ref, ref, sem).wait()

    ready("tok", "gain")
    activations = tok[...].astype(F32)
    scaled = (activations * gain[...]).astype(BF16)
    square = jnp.sum(activations * activations, axis=1, keepdims=True)
    ext[...] = jnp.zeros_like(ext)
    ready("wq", "wk", "wgates")
    ext[:, 0:16] = dot_rows(scaled, wgates[...])
    lane = lax.broadcasted_iota(jnp.int32, (128, 128), 1)
    extra = jnp.where(lane == 16, square, ext[...])

    def put(dst, at, value):
        dst[..., at : at + value.shape[1]] = value.reshape(*dst.shape[:-1], value.shape[1]).astype(BF16)

    def first_step(at, ycols, zcols):
        for step in (2, 1, 3):
            column = (y + step) % ROW
            send(
                y1_send.at[:, column, :, ycols], y1_recv.at[step - 1, :, :, ycols], a_ssem.at[at], a_rsem.at[at],
                kv=chip(0, step),
            )
            row = (z + step) % ROW
            send(
                z1_send.at[row, :, :, zcols], z1_recv.at[step - 1, :, :, zcols], a_ssem.at[at + 2], a_rsem.at[at + 2],
                kv=chip(step, 0),
            )

    def second_step(at, ycols, zcols):
        wait_for(y1_recv.at[:, :, :, ycols], a_rsem.at[at])
        total = y1_send[:, y, :, ycols].astype(F32)
        for slot in range(ROW - 1):
            total = total + y1_recv[slot, :, :, ycols].astype(F32)
        y2_send[:, :, ycols] = total.astype(BF16)
        for step in (2, 1, 3):
            row = (z + step) % ROW
            send(
                y2_send.at[row, :, ycols], y2_recv.at[step - 1, :, ycols], b_ssem.at[at], b_rsem.at[at],
                kv=chip(step, 0),
            )
        wait_for(z1_recv.at[:, :, :, zcols], a_rsem.at[at + 2])
        total = z1_send[z, :, :, zcols].astype(F32)
        for slot in range(ROW - 1):
            total = total + z1_recv[slot, :, :, zcols].astype(F32)
        z2_send[:, :, zcols] = total.astype(BF16)
        for step in (2, 1, 3):
            column = (y + step) % ROW
            send(
                z2_send.at[column, :, zcols], z2_recv.at[step - 1, :, zcols], b_ssem.at[at + 2], b_rsem.at[at + 2],
                kv=chip(0, step),
            )

    def arrived(at, send_buf, recv_buf, mine, cols):
        wait_for(recv_buf.at[:, :, cols], b_rsem.at[at])
        total = send_buf[mine, :, cols].astype(F32)
        for slot in range(ROW - 1):
            total = total + recv_buf[slot, :, cols].astype(F32)
        return total

    put(y1_send, 0, dot(scaled, wq[...]))
    put(y1_send, 512, extra)
    put(z1_send, 0, dot(scaled, wk[...]))
    pl.semaphore_wait(barrier, 2 * ROW - 1)
    for step in (2, 1, 3):
        pl.semaphore_signal(plane_sem, inc=1, device_id={"kv": chip(step, 0)}, device_id_type=MESH)
    early_y, early_z, late_y, late_z = pl.ds(0, 640), pl.ds(0, 512), pl.ds(640, 512), pl.ds(512, 512)
    first_step(0, early_y, early_z)
    ready("wv")
    put(y1_send, 640, dot(scaled, wv[:, 0:512]))
    put(z1_send, 512, dot(scaled, wv[:, 512:1024]))
    first_step(1, late_y, late_z)
    ready("wo")
    put(o_send, 0, dot(scaled, wo[...]))
    pl.semaphore_wait(plane_sem, ROW - 1)
    for slot, (dz, dy) in enumerate(FAR):
        to = chip(dz, dy)
        send(o_send.at[to // ROW, to % ROW], o_recv.at[slot], o_ssem, o_rsem, kv=to)
    second_step(0, early_y, early_z)
    second_step(1, late_y, late_z)
    for at, (src, dst) in enumerate(((wout_h, pwout), (wg_h, pwg), (wu_h, pwu), (wd_h, pwd))):
        send(src, dst, w_ssem.at[at], w_rsem.at[at], tp=other)

    def by_head(value, width):
        return jnp.concatenate([value[:, h * width : (h + 1) * width] for h in range(HEADS)], axis=0)

    first = arrived(0, y2_send, y2_recv, z, early_y)
    inverse = lax.rsqrt(first[:, 528:529] * (1.0 / (KV * QK)) + EPSILON)
    query = (first[:, 0:512] * inverse).astype(BF16).astype(F32)
    key_sum = arrived(2, z2_send, z2_recv, y, early_z)
    key = (key_sum * (inverse * QK ** (-0.5))).astype(BF16).astype(F32)
    gate_pre = first[:, 512:640] * inverse
    low = tp == 0
    input_pre = jnp.where(low, gate_pre[:, 0:4], gate_pre[:, 4:8])
    forget_pre = jnp.where(low, gate_pre[:, 8:12], gate_pre[:, 12:16])
    ready("bias", "nrm", "stab", "hgain")
    raw = forget_pre + bias[...]
    log_forget = jnp.minimum(raw, 0.0) - jnp.log1p(jnp.exp(-jnp.abs(raw)))
    diagonal = lax.broadcasted_iota(jnp.int32, (SEQ, SEQ), 0) == lax.broadcasted_iota(jnp.int32, (SEQ, SEQ), 1)
    old_stab = jnp.concatenate(
        [
            jnp.sum(jnp.where(diagonal, stab[h : h + 1, :], 0.0), axis=1, keepdims=True)
            for h in range(HEADS)
        ],
        axis=1,
    )
    shifted = log_forget + old_stab
    new_stab = jnp.maximum(shifted, input_pre)
    for h in range(HEADS):
        nstab_ref[h : h + 1, :] = jnp.sum(
            jnp.where(diagonal, new_stab[:, h : h + 1], 0.0), axis=0, keepdims=True
        )
    forget_scale = by_head(jnp.exp(shifted - new_stab), 1)
    input_scale = by_head(jnp.exp(input_pre - new_stab), 1)
    query_heads = by_head(query, QK)
    key_heads = by_head(key, QK)
    old_normalizer = jnp.concatenate([nrm[:, h, :] for h in range(HEADS)], axis=0)
    new_normalizer = forget_scale * old_normalizer + input_scale * key_heads
    for h in range(HEADS):
        nnrm_ref[:, h, :] = new_normalizer[h * SEQ : (h + 1) * SEQ]
    denominator = jnp.sum(query_heads * new_normalizer, axis=1, keepdims=True)
    query_key = jnp.sum(query_heads * key_heads, axis=1, keepdims=True)
    query_cols = jnp.transpose(query_heads).astype(BF16)
    key_cols = jnp.transpose(key_heads).astype(BF16)
    pair_row = lax.broadcasted_iota(jnp.int32, (HEADS * SEQ, QK), 0)
    ready("mem")
    for pair in range(HEADS * SEQ):
        h, s = pair // SEQ, pair % SEQ
        spread = dot(query_cols, jnp.where(pair_row == pair, 1.0, 0.0).astype(BF16))
        old = mem[s, h]
        low_half = jnp.sum(old[:, 0:128] * spread, axis=0, keepdims=True)
        high_half = jnp.sum(old[:, 128:256] * spread, axis=0, keepdims=True)
        carried[pair : pair + 1, 0:128] = low_half
        carried[pair : pair + 1, 128:256] = high_half

    value_sum = jnp.concatenate(
        [arrived(1, y2_send, y2_recv, z, late_y), arrived(3, z2_send, z2_recv, y, late_z)], axis=1
    )
    value_heads = by_head((value_sum * inverse).astype(BF16).astype(F32), VD)
    numerator = forget_scale * carried[...] + (input_scale * query_key) * value_heads
    head_out = numerator / jnp.maximum(jnp.abs(denominator), 1.0)
    gain_rows = jnp.concatenate(
        [jnp.broadcast_to(hgain[h : h + 1, :], (SEQ, VD)) for h in range(HEADS)], axis=0
    )
    normed = (
        head_out * lax.rsqrt(jnp.mean(head_out * head_out, axis=1, keepdims=True) + EPSILON) * gain_rows
    )
    wait_for(o_recv, o_rsem)
    outgate_sum = o_send[z, y].astype(F32)
    for slot in range(KV - 1):
        outgate_sum = outgate_sum + o_recv[slot].astype(F32)
    outgate = by_head((outgate_sum * inverse).astype(BF16).astype(F32), VD)
    mixed = normed * jax.nn.sigmoid(outgate)
    mixed_ref[...] = jnp.concatenate(
        [mixed[h * SEQ : (h + 1) * SEQ] for h in range(HEADS)], axis=1
    ).astype(BF16)

    half, place = me // 8, me % 8
    for dz, dy in FAR:
        send(mixed_ref, heads.at[tp, place], c_ssem, c_rsem, kv=chip(dz, dy), tp=half)

    @pl.when(tp == half)
    def _():
        heads[tp, place] = mixed_ref[...]

    @pl.when(tp != half)
    def _():
        send(mixed_ref, heads.at[tp, place], c_ssem, c_rsem, tp=other)

    value_row = lax.broadcasted_iota(jnp.int32, (HEADS * SEQ, VD), 0)
    for pair in range(HEADS * SEQ):
        h, s = pair // SEQ, pair % SEQ
        outer = dot(key_cols, jnp.where(value_row == pair, value_heads, 0.0).astype(BF16))
        nmem_ref[s, h] = (
            forget_scale[pair : pair + 1, :] * mem[s, h] + input_scale[pair : pair + 1, :] * outer
        )
    ready("wout", "mgain")

    @pl.when(tp == half)
    def _():
        wait_for(o_recv, c_rsem)

    @pl.when(tp != half)
    def _():
        wait_for(o_send, c_rsem)

    def group(at, w):
        rows_of = heads[at].astype(F32).reshape(64, HEADS * VD).astype(BF16)
        return dot(rows_of, w[...]).astype(BF16).astype(F32)

    wait_for(pwout, w_rsem.at[0])
    branch = group(tp, wout) + group(other, pwout)
    own_rows = pl.ds(pl.multiple_of(tp * 64, 64), 64)
    residual = (tok[own_rows, :].astype(F32) + branch).astype(BF16)
    rows[me] = residual
    resid[tp] = residual

    for dz, dy in FAR:
        send(rows.at[me], rows.at[me], e_ssem, e_rsem, kv=chip(dz, dy))
    send(resid.at[tp], resid.at[tp], d_ssem, d_rsem, tp=other)
    ready("wg", "wu", "wd")
    wait_for(pwg, w_rsem.at[1])
    wait_for(pwu, w_rsem.at[2])
    wait_for(pwd, w_rsem.at[3])
    wait_for(rows.at[0:15], e_rsem)
    whole = jnp.concatenate([rows[j].astype(F32) for j in range(KV)], axis=1)
    inverse_two = lax.rsqrt(jnp.mean(whole * whole, axis=1, keepdims=True) + EPSILON)
    mlp_in = (whole * inverse_two * mgain[...]).astype(BF16)

    def hidden_of(gate_w, up_w):
        return (jax.nn.silu(dot_rows(mlp_in, gate_w[...])) * dot_rows(mlp_in, up_w[...])).astype(BF16)

    hidden_own = hidden_of(wg, wu)
    hidden_other = hidden_of(pwg, pwu)

    lane_two = lax.broadcasted_iota(jnp.int32, (32, 128), 1)
    slot = me * 2 + tp
    for dz in (2, 1, 3, 0):
        cols = pl.ds(pl.multiple_of(((z + dz) % ROW) * 512, 512), 512)
        part = dot(hidden_own, wd[:, cols]) + dot(hidden_other, pwd[:, cols])
        for at in range(ROW):
            top = part[0:32, at * 128 : (at + 1) * 128]
            bottom = part[32:64, at * 128 : (at + 1) * 128]
            down_send[dz, at, 0] = jnp.where(lane_two < 64, top, pltpu.roll(bottom, 64, 1)).astype(BF16)
            down_send[dz, at, 1] = jnp.where(lane_two < 64, pltpu.roll(top, 64, 1), bottom).astype(BF16)
        for dy in (2, 1, 3, 0):
            column = (y + dy) % ROW
            for core in (tp, other):
                if (dz, dy) != (0, 0) or core is other:
                    send(
                        down_send.at[dz, column, core], down_recv.at[slot], g_ssem, g_rsem,
                        kv=chip(dz, dy), tp=core,
                    )
    down_recv[slot] = down_send[0, y, tp]
    wait_for(down_recv.at[0:31], g_rsem)
    pieces = []
    for core in range(2):
        total = down_recv[core].astype(F32)
        for j in range(1, KV):
            total = total + down_recv[2 * j + core].astype(F32)
        pieces += [total, pltpu.roll(total, 64, 1)]
    wait_for(resid.at[0], d_rsem)
    own = resid[...].astype(F32).reshape(128, 128)
    own = jnp.where(low, own, pltpu.roll(own, 64, 1))
    summed = jnp.concatenate(pieces, axis=0) + own
    out_ref[...] = jnp.transpose(summed)[0:64, :].astype(BF16)

    for at, ycols, zcols in ((0, early_y, early_z), (1, late_y, late_z)):
        wait_for(y1_recv.at[:, :, :, ycols], a_ssem.at[at])
        wait_for(z1_recv.at[:, :, :, zcols], a_ssem.at[at + 2])
        wait_for(y2_recv.at[:, :, ycols], b_ssem.at[at])
        wait_for(z2_recv.at[:, :, zcols], b_ssem.at[at + 2])
    wait_for(o_recv, o_ssem)
    wait_for(pwout, w_ssem.at[0])
    wait_for(pwg, w_ssem.at[1])
    wait_for(pwu, w_ssem.at[2])
    wait_for(pwd, w_ssem.at[3])

    @pl.when(tp == half)
    def _():
        wait_for(o_recv, c_ssem)

    @pl.when(tp != half)
    def _():
        wait_for(o_send, c_ssem)

    wait_for(resid.at[0], d_ssem)
    wait_for(rows.at[0:15], e_ssem)
    wait_for(down_recv.at[0:31], g_ssem)


def finish(out, nmem, nnrm, nstab, out_h, nmem_h, nnrm_h, nstab_h, sem):
    copies = [(nmem.at[j], nmem_h.at[j]) for j in range(SEQ)]
    copies += [(nnrm, nnrm_h), (nstab, nstab_h), (out, out_h)]
    copies = [pltpu.make_async_copy(src, dst, sem.at[at]) for at, (src, dst) in enumerate(copies)]
    for copy in copies:
        copy.start()
    for copy in copies:
        copy.wait()


def body(tokens, mix_gain, w_query, w_key, w_value, w_outgate, w_gates, forget_bias, memory, normalizer, stabilizer,
         head_gain, w_out, mlp_gain, w_gate, w_up, w_down):
    args = (
        tokens, mix_gain.reshape(1, -1), w_query, w_key, w_value, w_outgate, w_gates.T, forget_bias.reshape(1, -1),
        memory, normalizer, stabilizer.T, head_gain, w_out, mlp_gain.reshape(1, -1), w_gate.T, w_up.T, w_down,
    )
    copies = [pltpu.VMEM(a.shape, a.dtype) for a in args]
    copies[6] = pltpu.VMEM((16, QK), BF16)
    dma = pltpu.SemaphoreType.DMA
    outs = (
        jax.ShapeDtypeStruct((64, 128), BF16),
        jax.ShapeDtypeStruct(memory.shape, F32),
        jax.ShapeDtypeStruct(normalizer.shape, F32),
        jax.ShapeDtypeStruct((HEADS, SEQ), F32),
    )
    results = pl.pallas_call(
        layer,
        name="layer",
        out_shape=tuple(pltpu.VMEM(o.shape, o.dtype) for o in outs),
        in_specs=[pl.BlockSpec(memory_space=pltpu.HBM)] * len(args),
        out_specs=[pl.BlockSpec(memory_space=pltpu.VMEM)] * 4,
        scratch_shapes=copies + [
            pltpu.VMEM(w_gate.shape[::-1], BF16),
            pltpu.VMEM(w_up.shape[::-1], BF16),
            pltpu.VMEM(w_down.shape, BF16),
            pltpu.VMEM(w_out.shape, BF16),
            pltpu.VMEM((128, 128), F32),
            pltpu.VMEM((ROW, ROW, SEQ, 1152), BF16),
            pltpu.VMEM((ROW - 1, ROW, SEQ, 1152), BF16),
            pltpu.VMEM((ROW, ROW, SEQ, 1024), BF16),
            pltpu.VMEM((ROW - 1, ROW, SEQ, 1024), BF16),
            pltpu.VMEM((ROW, SEQ, 1152), BF16),
            pltpu.VMEM((ROW - 1, SEQ, 1152), BF16),
            pltpu.VMEM((ROW, SEQ, 1024), BF16),
            pltpu.VMEM((ROW - 1, SEQ, 1024), BF16),
            pltpu.VMEM((ROW, ROW, SEQ, 1024), BF16),
            pltpu.VMEM((KV - 1, SEQ, 1024), BF16),
            pltpu.VMEM((HEADS * SEQ, VD), F32),
            pltpu.VMEM((SEQ, HEADS * VD), BF16),
            pltpu.VMEM((2, KV // 2, SEQ, HEADS * VD), BF16),
            pltpu.VMEM((2, 64, 128), BF16),
            pltpu.VMEM((KV, 64, 128), BF16),
            pltpu.VMEM((ROW, ROW, 2, 32, 128), BF16),
            pltpu.VMEM((2 * KV, 32, 128), BF16),
            pltpu.SemaphoreType.REGULAR, dma((len(args),)), dma((4,)), dma((4,)), dma((4,)), dma((4,)), dma, dma, dma((4,)), dma((4,)),
            dma, dma, dma, dma, dma, dma, dma, dma,
        ],
        compiler_params=pltpu.CompilerParams(
            collective_id=0, has_side_effects=True, vmem_limit_bytes=40 * 1024 * 1024
        ),
    )(*(pltpu.with_memory_space_constraint(a, pltpu.HBM) for a in args))
    out, new_memory, new_normalizer, new_stabilizer = pl.pallas_call(
        finish,
        name="finish",
        out_shape=outs,
        in_specs=[pl.BlockSpec(memory_space=pltpu.VMEM)] * 4,
        out_specs=[pl.BlockSpec(memory_space=pltpu.HBM)] * 4,
        scratch_shapes=[dma((SEQ + 3,))],
        compiler_params=pltpu.CompilerParams(vmem_limit_bytes=8 * 1024 * 1024),
    )(*results)
    return out.T, new_memory, new_normalizer, new_stabilizer.T


def solution(mesh):
    in_specs = (
        P("dp", "kv"), P("kv"), P("kv", "tp"), P("kv", "tp"), P("kv", "tp"), P("kv", "tp"), P(), P("tp"),
        P(("dp", "kv"), "tp", None, None), P(("dp", "kv"), "tp", None), P(("dp", "kv"), "tp"), P("tp", None),
        P("tp", "kv"), P(), P(None, ("kv", "tp")), P(None, ("kv", "tp")), P(("kv", "tp"), None),
    )
    out_specs = (
        P("dp", ("kv", "tp")), P(("dp", "kv"), "tp", None, None), P(("dp", "kv"), "tp", None), P(("dp", "kv"), "tp"),
    )
    return jax.shard_map(body, mesh=mesh, in_specs=in_specs, out_specs=out_specs, check_vma=False)
```

```python
import jax
import jax.numpy as jnp
from jax import lax
from jax.experimental import pallas as pl
from jax.experimental.pallas import tpu as pltpu
from jax.sharding import PartitionSpec as P

QK = 128
VD = 256
EPSILON = 1e-06
ROW = 4
KV = 16
SEQ = 8
HEADS = 4
MESH = pl.DeviceIdType.MESH
F32 = jnp.float32
BF16 = jnp.bfloat16

FAR = sorted(
    [(a, b) for a in range(ROW) for b in range(ROW) if (a, b) != (0, 0)],
    key=lambda o: -(min(o[0], ROW - o[0]) + min(o[1], ROW - o[1])),
)


def dot(a, b):
    return jnp.dot(a, b, preferred_element_type=F32)


def dot_rows(a, b):
    return lax.dot_general(a, b, (((1,), (1,)), ((), ())), preferred_element_type=F32)


def layer(
    tok_h, gain_h, wq_h, wk_h, wv_h, wo_h, wgates_h, bias_h, mem_h, nrm_h, stab_h, hgain_h, wout_h, mgain_h,
    wg_h, wu_h, wd_h,
    out_ref, nmem_ref, nnrm_ref, nstab_ref,
    tok, gain, wq, wk, wv, wo, wgates, bias, mem, nrm, stab, hgain, wout, mgain, wg, wu, wd,
    pwg, pwu, pwd, pwout, ext, y1_send, y1_recv, z1_send, z1_recv, y2_send, y2_recv, z2_send, z2_recv, o_send, o_recv, carried, mixed_ref, heads, resid, rows,
    down_send, down_recv,
    plane_sem, in_sem, a_ssem, a_rsem, b_ssem, b_rsem, o_ssem, o_rsem, w_ssem, w_rsem, c_ssem, c_rsem, d_ssem, d_rsem, e_ssem, e_rsem, g_ssem, g_rsem,
):
    me = lax.axis_index("kv")
    tp = lax.axis_index("tp")
    z, y = me // ROW, me % ROW
    other = 1 - tp

    def chip(dz, dy):
        return ((z + dz) % ROW) * ROW + (y + dy) % ROW

    barrier = pltpu.get_barrier_semaphore()
    for step in (2, 1, 3):
        pl.semaphore_signal(barrier, inc=1, device_id={"kv": chip(step, 0)}, device_id_type=MESH)
        pl.semaphore_signal(barrier, inc=1, device_id={"kv": chip(0, step)}, device_id_type=MESH)
    pl.semaphore_signal(barrier, inc=1, device_id={"tp": other}, device_id_type=MESH)

    loads = {}

    def load(name, src, dst):
        loads[name] = pltpu.make_async_copy(src, dst, in_sem.at[len(loads)])
        loads[name].start()

    load("tok", tok_h, tok)
    load("gain", gain_h, gain)
    load("wq", wq_h, wq)
    load("wk", wk_h, wk)
    load("wgates", wgates_h.at[:, pl.ds(pl.multiple_of(me * QK, QK), QK)], wgates)
    load("wv", wv_h, wv)
    load("wo", wo_h, wo)
    load("mem", mem_h, mem)
    load("bias", bias_h, bias)
    load("nrm", nrm_h, nrm)
    load("stab", stab_h, stab)
    load("hgain", hgain_h, hgain)
    load("wout", wout_h, wout)
    load("mgain", mgain_h, mgain)
    load("wg", wg_h, wg)
    load("wu", wu_h, wu)
    load("wd", wd_h, wd)

    def ready(*names):
        for name in names:
            loads[name].wait()

    def send(src, dst, ssem, rsem, **device):
        pltpu.make_async_remote_copy(
            src_ref=src, dst_ref=dst, send_sem=ssem, recv_sem=rsem, device_id=device, device_id_type=MESH
        ).start()

    def wait_for(ref, sem):
        pltpu.make_async_copy(ref, ref, sem).wait()

    ready("tok", "gain")
    activations = tok[...].astype(F32)
    scaled = (activations * gain[...]).astype(BF16)
    square = jnp.sum(activations * activations, axis=1, keepdims=True)
    ext[...] = jnp.zeros_like(ext)
    ready("wq", "wk", "wgates")
    ext[:, 0:16] = dot_rows(scaled, wgates[...])
    lane = lax.broadcasted_iota(jnp.int32, (128, 128), 1)
    extra = jnp.where(lane == 16, square, ext[...])

    def put(dst, at, value):
        dst[..., at : at + value.shape[1]] = value.reshape(*dst.shape[:-1], value.shape[1]).astype(BF16)

    def first_step(at, ycols, zcols):
        for step in (2, 1, 3):
            column = (y + step) % ROW
            send(
                y1_send.at[:, column, :, ycols], y1_recv.at[step - 1, :, :, ycols], a_ssem.at[at], a_rsem.at[at],
                kv=chip(0, step),
            )
            row = (z + step) % ROW
            send(
                z1_send.at[row, :, :, zcols], z1_recv.at[step - 1, :, :, zcols], a_ssem.at[at + 2], a_rsem.at[at + 2],
                kv=chip(step, 0),
            )

    def second_step(at, ycols, zcols):
        wait_for(y1_recv.at[:, :, :, ycols], a_rsem.at[at])
        total = y1_send[:, y, :, ycols].astype(F32)
        for slot in range(ROW - 1):
            total = total + y1_recv[slot, :, :, ycols].astype(F32)
        y2_send[:, :, ycols] = total.astype(BF16)
        for step in (2, 1, 3):
            row = (z + step) % ROW
            send(
                y2_send.at[row, :, ycols], y2_recv.at[step - 1, :, ycols], b_ssem.at[at], b_rsem.at[at],
                kv=chip(step, 0),
            )
        wait_for(z1_recv.at[:, :, :, zcols], a_rsem.at[at + 2])
        total = z1_send[z, :, :, zcols].astype(F32)
        for slot in range(ROW - 1):
            total = total + z1_recv[slot, :, :, zcols].astype(F32)
        z2_send[:, :, zcols] = total.astype(BF16)
        for step in (2, 1, 3):
            column = (y + step) % ROW
            send(
                z2_send.at[column, :, zcols], z2_recv.at[step - 1, :, zcols], b_ssem.at[at + 2], b_rsem.at[at + 2],
                kv=chip(0, step),
            )

    def arrived(at, send_buf, recv_buf, mine, cols):
        wait_for(recv_buf.at[:, :, cols], b_rsem.at[at])
        total = send_buf[mine, :, cols].astype(F32)
        for slot in range(ROW - 1):
            total = total + recv_buf[slot, :, cols].astype(F32)
        return total

    put(y1_send, 0, dot(scaled, wq[...]))
    put(y1_send, 512, extra)
    put(z1_send, 0, dot(scaled, wk[...]))
    pl.semaphore_wait(barrier, 2 * ROW - 1)
    for step in (2, 1, 3):
        pl.semaphore_signal(plane_sem, inc=1, device_id={"kv": chip(step, 0)}, device_id_type=MESH)
    early_y, early_z, late_y, late_z = pl.ds(0, 640), pl.ds(0, 512), pl.ds(640, 512), pl.ds(512, 512)
    first_step(0, early_y, early_z)
    ready("wv")
    put(y1_send, 640, dot(scaled, wv[:, 0:512]))
    put(z1_send, 512, dot(scaled, wv[:, 512:1024]))
    first_step(1, late_y, late_z)
    ready("wo")
    put(o_send, 0, dot(scaled, wo[...]))
    pl.semaphore_wait(plane_sem, ROW - 1)
    for slot, (dz, dy) in enumerate(FAR):
        to = chip(dz, dy)
        send(o_send.at[to // ROW, to % ROW], o_recv.at[slot], o_ssem, o_rsem, kv=to)
    second_step(0, early_y, early_z)
    second_step(1, late_y, late_z)
    for at, (src, dst) in enumerate(((wout_h, pwout), (wg_h, pwg), (wu_h, pwu), (wd_h, pwd))):
        send(src, dst, w_ssem.at[at], w_rsem.at[at], tp=other)

    def by_head(value, width):
        return jnp.concatenate([value[:, h * width : (h + 1) * width] for h in range(HEADS)], axis=0)

    first = arrived(0, y2_send, y2_recv, z, early_y)
    inverse = lax.rsqrt(first[:, 528:529] * (1.0 / (KV * QK)) + EPSILON)
    query = (first[:, 0:512] * inverse).astype(BF16).astype(F32)
    key_sum = arrived(2, z2_send, z2_recv, y, early_z)
    key = (key_sum * (inverse * QK ** (-0.5))).astype(BF16).astype(F32)
    gate_pre = first[:, 512:640] * inverse
    low = tp == 0
    input_pre = jnp.where(low, gate_pre[:, 0:4], gate_pre[:, 4:8])
    forget_pre = jnp.where(low, gate_pre[:, 8:12], gate_pre[:, 12:16])
    ready("bias", "nrm", "stab", "hgain")
    raw = forget_pre + bias[...]
    log_forget = jnp.minimum(raw, 0.0) - jnp.log1p(jnp.exp(-jnp.abs(raw)))
    diagonal = lax.broadcasted_iota(jnp.int32, (SEQ, SEQ), 0) == lax.broadcasted_iota(jnp.int32, (SEQ, SEQ), 1)
    old_stab = jnp.concatenate(
        [
            jnp.sum(jnp.where(diagonal, stab[h : h + 1, :], 0.0), axis=1, keepdims=True)
            for h in range(HEADS)
        ],
        axis=1,
    )
    shifted = log_forget + old_stab
    new_stab = jnp.maximum(shifted, input_pre)
    for h in range(HEADS):
        nstab_ref[h : h + 1, :] = jnp.sum(
            jnp.where(diagonal, new_stab[:, h : h + 1], 0.0), axis=0, keepdims=True
        )
    forget_scale = by_head(jnp.exp(shifted - new_stab), 1)
    input_scale = by_head(jnp.exp(input_pre - new_stab), 1)
    query_heads = by_head(query, QK)
    key_heads = by_head(key, QK)
    old_normalizer = jnp.concatenate([nrm[:, h, :] for h in range(HEADS)], axis=0)
    new_normalizer = forget_scale * old_normalizer + input_scale * key_heads
    for h in range(HEADS):
        nnrm_ref[:, h, :] = new_normalizer[h * SEQ : (h + 1) * SEQ]
    denominator = jnp.sum(query_heads * new_normalizer, axis=1, keepdims=True)
    query_key = jnp.sum(query_heads * key_heads, axis=1, keepdims=True)
    query_cols = jnp.transpose(query_heads).astype(BF16)
    key_cols = jnp.transpose(key_heads).astype(BF16)
    pair_row = lax.broadcasted_iota(jnp.int32, (HEADS * SEQ, QK), 0)
    ready("mem")
    for pair in range(HEADS * SEQ):
        h, s = pair // SEQ, pair % SEQ
        spread = dot(query_cols, jnp.where(pair_row == pair, 1.0, 0.0).astype(BF16))
        old = mem[s, h]
        low_half = jnp.sum(old[:, 0:128] * spread, axis=0, keepdims=True)
        high_half = jnp.sum(old[:, 128:256] * spread, axis=0, keepdims=True)
        carried[pair : pair + 1, 0:128] = low_half
        carried[pair : pair + 1, 128:256] = high_half

    value_sum = jnp.concatenate(
        [arrived(1, y2_send, y2_recv, z, late_y), arrived(3, z2_send, z2_recv, y, late_z)], axis=1
    )
    value_heads = by_head((value_sum * inverse).astype(BF16).astype(F32), VD)
    numerator = forget_scale * carried[...] + (input_scale * query_key) * value_heads
    head_out = numerator / jnp.maximum(jnp.abs(denominator), 1.0)
    gain_rows = jnp.concatenate(
        [jnp.broadcast_to(hgain[h : h + 1, :], (SEQ, VD)) for h in range(HEADS)], axis=0
    )
    normed = (
        head_out * lax.rsqrt(jnp.mean(head_out * head_out, axis=1, keepdims=True) + EPSILON) * gain_rows
    )
    wait_for(o_recv, o_rsem)
    outgate_sum = o_send[z, y].astype(F32)
    for slot in range(KV - 1):
        outgate_sum = outgate_sum + o_recv[slot].astype(F32)
    outgate = by_head((outgate_sum * inverse).astype(BF16).astype(F32), VD)
    mixed = normed * jax.nn.sigmoid(outgate)
    mixed_ref[...] = jnp.concatenate(
        [mixed[h * SEQ : (h + 1) * SEQ] for h in range(HEADS)], axis=1
    ).astype(BF16)

    half, place = me // 8, me % 8
    for dz, dy in FAR:
        send(mixed_ref, heads.at[tp, place], c_ssem, c_rsem, kv=chip(dz, dy), tp=half)

    @pl.when(tp == half)
    def _():
        heads[tp, place] = mixed_ref[...]

    @pl.when(tp != half)
    def _():
        send(mixed_ref, heads.at[tp, place], c_ssem, c_rsem, tp=other)

    value_row = lax.broadcasted_iota(jnp.int32, (HEADS * SEQ, VD), 0)
    for pair in range(HEADS * SEQ):
        h, s = pair // SEQ, pair % SEQ
        outer = dot(key_cols, jnp.where(value_row == pair, value_heads, 0.0).astype(BF16))
        nmem_ref[s, h] = (
            forget_scale[pair : pair + 1, :] * mem[s, h] + input_scale[pair : pair + 1, :] * outer
        )
    ready("wout", "mgain")

    @pl.when(tp == half)
    def _():
        wait_for(o_recv, c_rsem)

    @pl.when(tp != half)
    def _():
        wait_for(o_send, c_rsem)

    def group(at, w):
        rows_of = heads[at].astype(F32).reshape(64, HEADS * VD).astype(BF16)
        return dot(rows_of, w[...]).astype(BF16).astype(F32)

    wait_for(pwout, w_rsem.at[0])
    branch = group(tp, wout) + group(other, pwout)
    own_rows = pl.ds(pl.multiple_of(tp * 64, 64), 64)
    residual = (tok[own_rows, :].astype(F32) + branch).astype(BF16)
    rows[z, y] = residual
    resid[tp] = residual

    for dz in (2, 1, 3, 0):
        for dy in (2, 1, 3, 0):
            if (dz, dy) != (0, 0):
                send(rows.at[z, y], rows.at[z, y], e_ssem, e_rsem.at[dz], kv=chip(dz, dy))
    send(resid.at[tp], resid.at[tp], d_ssem, d_rsem, tp=other)
    ready("wg", "wu", "wd")
    wait_for(pwg, w_rsem.at[1])
    wait_for(pwu, w_rsem.at[2])
    wait_for(pwd, w_rsem.at[3])

    square_two, sums = None, None
    for steps in ((0,), (1,), (3,), (2,)):
        for dz in steps:
            wait_for(rows.at[0, 0 : ROW - (dz == 0)], e_rsem.at[dz])
        for dz in steps:
            row = (z + ROW - dz) % ROW
            span = pl.ds(pl.multiple_of(row * 512, 512), 512)
            block = jnp.concatenate([rows[row, column].astype(F32) for column in range(ROW)], axis=1)
            square = jnp.sum(block * block, axis=1, keepdims=True)
            block = (block * mgain[:, span]).astype(BF16)
            parts = [dot_rows(block, w[:, span]) for w in (wg, wu, pwg, pwu)]
            if sums is None:
                square_two, sums = square, parts
            else:
                square_two, sums = square_two + square, [a + b for a, b in zip(sums, parts)]
    inverse_two = lax.rsqrt(square_two * (1.0 / (KV * QK)) + EPSILON)
    gate_own, up_own, gate_other, up_other = [total * inverse_two for total in sums]
    hidden_own = (jax.nn.silu(gate_own) * up_own).astype(BF16)
    hidden_other = (jax.nn.silu(gate_other) * up_other).astype(BF16)

    lane_two = lax.broadcasted_iota(jnp.int32, (32, 128), 1)
    slot = me * 2 + tp
    for dz in (2, 1, 3, 0):
        cols = pl.ds(pl.multiple_of(((z + dz) % ROW) * 512, 512), 512)
        part = dot(hidden_own, wd[:, cols]) + dot(hidden_other, pwd[:, cols])
        for at in range(ROW):
            top = part[0:32, at * 128 : (at + 1) * 128]
            bottom = part[32:64, at * 128 : (at + 1) * 128]
            down_send[dz, at, 0] = jnp.where(lane_two < 64, top, pltpu.roll(bottom, 64, 1)).astype(BF16)
            down_send[dz, at, 1] = jnp.where(lane_two < 64, pltpu.roll(top, 64, 1), bottom).astype(BF16)
        for dy in (2, 1, 3, 0):
            column = (y + dy) % ROW
            for core in (tp, other):
                if (dz, dy) != (0, 0) or core is other:
                    send(
                        down_send.at[dz, column, core], down_recv.at[slot], g_ssem, g_rsem,
                        kv=chip(dz, dy), tp=core,
                    )
    down_recv[slot] = down_send[0, y, tp]
    wait_for(down_recv.at[0:31], g_rsem)
    pieces = []
    for core in range(2):
        total = down_recv[core].astype(F32)
        for j in range(1, KV):
            total = total + down_recv[2 * j + core].astype(F32)
        pieces += [total, pltpu.roll(total, 64, 1)]
    wait_for(resid.at[0], d_rsem)
    own = resid[...].astype(F32).reshape(128, 128)
    own = jnp.where(low, own, pltpu.roll(own, 64, 1))
    summed = jnp.concatenate(pieces, axis=0) + own
    out_ref[...] = jnp.transpose(summed)[0:64, :].astype(BF16)

    for at, ycols, zcols in ((0, early_y, early_z), (1, late_y, late_z)):
        wait_for(y1_recv.at[:, :, :, ycols], a_ssem.at[at])
        wait_for(z1_recv.at[:, :, :, zcols], a_ssem.at[at + 2])
        wait_for(y2_recv.at[:, :, ycols], b_ssem.at[at])
        wait_for(z2_recv.at[:, :, zcols], b_ssem.at[at + 2])
    wait_for(o_recv, o_ssem)
    wait_for(pwout, w_ssem.at[0])
    wait_for(pwg, w_ssem.at[1])
    wait_for(pwu, w_ssem.at[2])
    wait_for(pwd, w_ssem.at[3])

    @pl.when(tp == half)
    def _():
        wait_for(o_recv, c_ssem)

    @pl.when(tp != half)
    def _():
        wait_for(o_send, c_ssem)

    wait_for(resid.at[0], d_ssem)
    wait_for(rows.at[0:3], e_ssem)
    wait_for(rows.at[0, 0:3], e_ssem)
    wait_for(down_recv.at[0:31], g_ssem)


def finish(out, nmem, nnrm, nstab, out_h, nmem_h, nnrm_h, nstab_h, sem):
    copies = [(nmem.at[j], nmem_h.at[j]) for j in range(SEQ)]
    copies += [(nnrm, nnrm_h), (nstab, nstab_h), (out, out_h)]
    copies = [pltpu.make_async_copy(src, dst, sem.at[at]) for at, (src, dst) in enumerate(copies)]
    for copy in copies:
        copy.start()
    for copy in copies:
        copy.wait()


def body(tokens, mix_gain, w_query, w_key, w_value, w_outgate, w_gates, forget_bias, memory, normalizer, stabilizer,
         head_gain, w_out, mlp_gain, w_gate, w_up, w_down):
    args = (
        tokens, mix_gain.reshape(1, -1), w_query, w_key, w_value, w_outgate, w_gates.T, forget_bias.reshape(1, -1),
        memory, normalizer, stabilizer.T, head_gain, w_out, mlp_gain.reshape(1, -1), w_gate.T, w_up.T, w_down,
    )
    copies = [pltpu.VMEM(a.shape, a.dtype) for a in args]
    copies[6] = pltpu.VMEM((16, QK), BF16)
    dma = pltpu.SemaphoreType.DMA
    outs = (
        jax.ShapeDtypeStruct((64, 128), BF16),
        jax.ShapeDtypeStruct(memory.shape, F32),
        jax.ShapeDtypeStruct(normalizer.shape, F32),
        jax.ShapeDtypeStruct((HEADS, SEQ), F32),
    )
    results = pl.pallas_call(
        layer,
        name="layer",
        out_shape=tuple(pltpu.VMEM(o.shape, o.dtype) for o in outs),
        in_specs=[pl.BlockSpec(memory_space=pltpu.HBM)] * len(args),
        out_specs=[pl.BlockSpec(memory_space=pltpu.VMEM)] * 4,
        scratch_shapes=copies + [
            pltpu.VMEM(w_gate.shape[::-1], BF16),
            pltpu.VMEM(w_up.shape[::-1], BF16),
            pltpu.VMEM(w_down.shape, BF16),
            pltpu.VMEM(w_out.shape, BF16),
            pltpu.VMEM((128, 128), F32),
            pltpu.VMEM((ROW, ROW, SEQ, 1152), BF16),
            pltpu.VMEM((ROW - 1, ROW, SEQ, 1152), BF16),
            pltpu.VMEM((ROW, ROW, SEQ, 1024), BF16),
            pltpu.VMEM((ROW - 1, ROW, SEQ, 1024), BF16),
            pltpu.VMEM((ROW, SEQ, 1152), BF16),
            pltpu.VMEM((ROW - 1, SEQ, 1152), BF16),
            pltpu.VMEM((ROW, SEQ, 1024), BF16),
            pltpu.VMEM((ROW - 1, SEQ, 1024), BF16),
            pltpu.VMEM((ROW, ROW, SEQ, 1024), BF16),
            pltpu.VMEM((KV - 1, SEQ, 1024), BF16),
            pltpu.VMEM((HEADS * SEQ, VD), F32),
            pltpu.VMEM((SEQ, HEADS * VD), BF16),
            pltpu.VMEM((2, KV // 2, SEQ, HEADS * VD), BF16),
            pltpu.VMEM((2, 64, 128), BF16),
            pltpu.VMEM((ROW, ROW, 64, 128), BF16),
            pltpu.VMEM((ROW, ROW, 2, 32, 128), BF16),
            pltpu.VMEM((2 * KV, 32, 128), BF16),
            pltpu.SemaphoreType.REGULAR, dma((len(args),)), dma((4,)), dma((4,)), dma((4,)), dma((4,)), dma, dma, dma((4,)), dma((4,)),
            dma, dma, dma, dma, dma, dma((4,)), dma, dma,
        ],
        compiler_params=pltpu.CompilerParams(
            collective_id=0, has_side_effects=True, vmem_limit_bytes=40 * 1024 * 1024
        ),
    )(*(pltpu.with_memory_space_constraint(a, pltpu.HBM) for a in args))
    out, new_memory, new_normalizer, new_stabilizer = pl.pallas_call(
        finish,
        name="finish",
        out_shape=outs,
        in_specs=[pl.BlockSpec(memory_space=pltpu.VMEM)] * 4,
        out_specs=[pl.BlockSpec(memory_space=pltpu.HBM)] * 4,
        scratch_shapes=[dma((SEQ + 3,))],
        compiler_params=pltpu.CompilerParams(vmem_limit_bytes=8 * 1024 * 1024),
    )(*results)
    return out.T, new_memory, new_normalizer, new_stabilizer.T


def solution(mesh):
    in_specs = (
        P("dp", "kv"), P("kv"), P("kv", "tp"), P("kv", "tp"), P("kv", "tp"), P("kv", "tp"), P(), P("tp"),
        P(("dp", "kv"), "tp", None, None), P(("dp", "kv"), "tp", None), P(("dp", "kv"), "tp"), P("tp", None),
        P("tp", "kv"), P(), P(None, ("kv", "tp")), P(None, ("kv", "tp")), P(("kv", "tp"), None),
    )
    out_specs = (
        P("dp", ("kv", "tp")), P(("dp", "kv"), "tp", None, None), P(("dp", "kv"), "tp", None), P(("dp", "kv"), "tp"),
    )
    return jax.shard_map(body, mesh=mesh, in_specs=in_specs, out_specs=out_specs, check_vma=False)
```

```python
import jax
import jax.numpy as jnp
from jax import lax
from jax.experimental import pallas as pl
from jax.experimental.pallas import tpu as pltpu
from jax.sharding import PartitionSpec as P

QK = 128
VD = 256
EPSILON = 1e-06
ROW = 4
KV = 16
SEQ = 8
HEADS = 4
MESH = pl.DeviceIdType.MESH
F32 = jnp.float32
BF16 = jnp.bfloat16

FAR = sorted(
    [(a, b) for a in range(ROW) for b in range(ROW) if (a, b) != (0, 0)],
    key=lambda o: -(min(o[0], ROW - o[0]) + min(o[1], ROW - o[1])),
)


def dot(a, b):
    return jnp.dot(a, b, preferred_element_type=F32)


def dot_rows(a, b):
    return lax.dot_general(a, b, (((1,), (1,)), ((), ())), preferred_element_type=F32)


def layer(
    tok_h, gain_h, wq_h, wk_h, wv_h, wo_h, wgates_h, bias_h, mem_h, nrm_h, stab_h, hgain_h, wout_h, mgain_h,
    wg_h, wu_h, wd_h,
    down_recv, resid, nmem_ref, nnrm_ref, nstab_ref,
    tok, gain, wq, wk, wv, wo, wgates, bias, mem, nrm, stab, hgain, wout, mgain, wg, wu, wd,
    pwg, pwu, pwd, pwout, ext, y1_send, y1_recv, z1_send, z1_recv, y2_send, y2_recv, z2_send, z2_recv, o_send, o_recv, carried, mixed_ref, heads, rows, down_send,
    plane_sem, in_sem, a_ssem, a_rsem, b_ssem, b_rsem, o_ssem, o_rsem, w_ssem, w_rsem, c_ssem, c_rsem, d_ssem, d_rsem, e_ssem, e_rsem, g_ssem, g_rsem,
):
    me = lax.axis_index("kv")
    tp = lax.axis_index("tp")
    z, y = me // ROW, me % ROW
    other = 1 - tp

    def chip(dz, dy):
        return ((z + dz) % ROW) * ROW + (y + dy) % ROW

    barrier = pltpu.get_barrier_semaphore()
    for step in (2, 1, 3):
        pl.semaphore_signal(barrier, inc=1, device_id={"kv": chip(step, 0)}, device_id_type=MESH)
        pl.semaphore_signal(barrier, inc=1, device_id={"kv": chip(0, step)}, device_id_type=MESH)
    pl.semaphore_signal(barrier, inc=1, device_id={"tp": other}, device_id_type=MESH)

    loads = {}

    def load(name, src, dst):
        loads[name] = pltpu.make_async_copy(src, dst, in_sem.at[len(loads)])
        loads[name].start()

    load("tok", tok_h, tok)
    load("gain", gain_h, gain)
    load("wq", wq_h, wq)
    load("wk", wk_h, wk)
    load("wgates", wgates_h.at[:, pl.ds(pl.multiple_of(me * QK, QK), QK)], wgates)
    load("wv", wv_h, wv)
    load("wo", wo_h, wo)
    load("mem", mem_h, mem)
    load("bias", bias_h, bias)
    load("nrm", nrm_h, nrm)
    load("stab", stab_h, stab)
    load("hgain", hgain_h, hgain)
    load("wout", wout_h, wout)
    load("mgain", mgain_h, mgain)
    load("wg", wg_h, wg)
    load("wu", wu_h, wu)
    load("wd", wd_h, wd)

    def ready(*names):
        for name in names:
            loads[name].wait()

    def send(src, dst, ssem, rsem, **device):
        pltpu.make_async_remote_copy(
            src_ref=src, dst_ref=dst, send_sem=ssem, recv_sem=rsem, device_id=device, device_id_type=MESH
        ).start()

    def wait_for(ref, sem):
        pltpu.make_async_copy(ref, ref, sem).wait()

    ready("tok", "gain")
    activations = tok[...].astype(F32)
    scaled = (activations * gain[...]).astype(BF16)
    square = jnp.sum(activations * activations, axis=1, keepdims=True)
    ext[...] = jnp.zeros_like(ext)
    ready("wq", "wk", "wgates")
    ext[:, 0:16] = dot_rows(scaled, wgates[...])
    lane = lax.broadcasted_iota(jnp.int32, (128, 128), 1)
    extra = jnp.where(lane == 16, square, ext[...])

    def put(dst, at, value):
        dst[..., at : at + value.shape[1]] = value.reshape(*dst.shape[:-1], value.shape[1]).astype(BF16)

    def first_step(at, ycols, zcols):
        for step in (2, 1, 3):
            column = (y + step) % ROW
            send(
                y1_send.at[:, column, :, ycols], y1_recv.at[step - 1, :, :, ycols], a_ssem.at[at], a_rsem.at[at],
                kv=chip(0, step),
            )
            row = (z + step) % ROW
            send(
                z1_send.at[row, :, :, zcols], z1_recv.at[step - 1, :, :, zcols], a_ssem.at[at + 2], a_rsem.at[at + 2],
                kv=chip(step, 0),
            )

    def second_step(at, ycols, zcols):
        wait_for(y1_recv.at[:, :, :, ycols], a_rsem.at[at])
        total = y1_send[:, y, :, ycols].astype(F32)
        for slot in range(ROW - 1):
            total = total + y1_recv[slot, :, :, ycols].astype(F32)
        y2_send[:, :, ycols] = total.astype(BF16)
        for step in (2, 1, 3):
            row = (z + step) % ROW
            send(
                y2_send.at[row, :, ycols], y2_recv.at[step - 1, :, ycols], b_ssem.at[at], b_rsem.at[at],
                kv=chip(step, 0),
            )
        wait_for(z1_recv.at[:, :, :, zcols], a_rsem.at[at + 2])
        total = z1_send[z, :, :, zcols].astype(F32)
        for slot in range(ROW - 1):
            total = total + z1_recv[slot, :, :, zcols].astype(F32)
        z2_send[:, :, zcols] = total.astype(BF16)
        for step in (2, 1, 3):
            column = (y + step) % ROW
            send(
                z2_send.at[column, :, zcols], z2_recv.at[step - 1, :, zcols], b_ssem.at[at + 2], b_rsem.at[at + 2],
                kv=chip(0, step),
            )

    def arrived(at, send_buf, recv_buf, mine, cols):
        wait_for(recv_buf.at[:, :, cols], b_rsem.at[at])
        total = send_buf[mine, :, cols].astype(F32)
        for slot in range(ROW - 1):
            total = total + recv_buf[slot, :, cols].astype(F32)
        return total

    put(y1_send, 0, dot(scaled, wq[...]))
    put(y1_send, 512, extra)
    put(z1_send, 0, dot(scaled, wk[...]))
    pl.semaphore_wait(barrier, 2 * ROW - 1)
    for step in (2, 1, 3):
        pl.semaphore_signal(plane_sem, inc=1, device_id={"kv": chip(step, 0)}, device_id_type=MESH)
    early_y, early_z, late_y, late_z = pl.ds(0, 640), pl.ds(0, 512), pl.ds(640, 512), pl.ds(512, 512)
    first_step(0, early_y, early_z)
    ready("wv")
    put(y1_send, 640, dot(scaled, wv[:, 0:512]))
    put(z1_send, 512, dot(scaled, wv[:, 512:1024]))
    first_step(1, late_y, late_z)
    ready("wo")
    put(o_send, 0, dot(scaled, wo[...]))
    pl.semaphore_wait(plane_sem, ROW - 1)
    for slot, (dz, dy) in enumerate(FAR):
        to = chip(dz, dy)
        send(o_send.at[to // ROW, to % ROW], o_recv.at[slot], o_ssem, o_rsem, kv=to)
    second_step(0, early_y, early_z)
    second_step(1, late_y, late_z)
    for at, (src, dst) in enumerate(((wout_h, pwout), (wg_h, pwg), (wu_h, pwu), (wd_h, pwd))):
        send(src, dst, w_ssem.at[at], w_rsem.at[at], tp=other)

    def by_head(value, width):
        return jnp.concatenate([value[:, h * width : (h + 1) * width] for h in range(HEADS)], axis=0)

    first = arrived(0, y2_send, y2_recv, z, early_y)
    inverse = lax.rsqrt(first[:, 528:529] * (1.0 / (KV * QK)) + EPSILON)
    query = (first[:, 0:512] * inverse).astype(BF16).astype(F32)
    key_sum = arrived(2, z2_send, z2_recv, y, early_z)
    key = (key_sum * (inverse * QK ** (-0.5))).astype(BF16).astype(F32)
    gate_pre = first[:, 512:640] * inverse
    low = tp == 0
    input_pre = jnp.where(low, gate_pre[:, 0:4], gate_pre[:, 4:8])
    forget_pre = jnp.where(low, gate_pre[:, 8:12], gate_pre[:, 12:16])
    ready("bias", "nrm", "stab", "hgain")
    raw = forget_pre + bias[...]
    log_forget = jnp.minimum(raw, 0.0) - jnp.log1p(jnp.exp(-jnp.abs(raw)))
    diagonal = lax.broadcasted_iota(jnp.int32, (SEQ, SEQ), 0) == lax.broadcasted_iota(jnp.int32, (SEQ, SEQ), 1)
    old_stab = jnp.concatenate(
        [
            jnp.sum(jnp.where(diagonal, stab[h : h + 1, :], 0.0), axis=1, keepdims=True)
            for h in range(HEADS)
        ],
        axis=1,
    )
    shifted = log_forget + old_stab
    new_stab = jnp.maximum(shifted, input_pre)
    for h in range(HEADS):
        nstab_ref[h : h + 1, :] = jnp.sum(
            jnp.where(diagonal, new_stab[:, h : h + 1], 0.0), axis=0, keepdims=True
        )
    forget_scale = by_head(jnp.exp(shifted - new_stab), 1)
    input_scale = by_head(jnp.exp(input_pre - new_stab), 1)
    query_heads = by_head(query, QK)
    key_heads = by_head(key, QK)
    old_normalizer = jnp.concatenate([nrm[:, h, :] for h in range(HEADS)], axis=0)
    new_normalizer = forget_scale * old_normalizer + input_scale * key_heads
    for h in range(HEADS):
        nnrm_ref[:, h, :] = new_normalizer[h * SEQ : (h + 1) * SEQ]
    denominator = jnp.sum(query_heads * new_normalizer, axis=1, keepdims=True)
    query_key = jnp.sum(query_heads * key_heads, axis=1, keepdims=True)
    query_cols = jnp.transpose(query_heads).astype(BF16)
    key_cols = jnp.transpose(key_heads).astype(BF16)
    pair_row = lax.broadcasted_iota(jnp.int32, (HEADS * SEQ, QK), 0)
    ready("mem")
    for pair in range(HEADS * SEQ):
        h, s = pair // SEQ, pair % SEQ
        spread = dot(query_cols, jnp.where(pair_row == pair, 1.0, 0.0).astype(BF16))
        old = mem[s, h]
        low_half = jnp.sum(old[:, 0:128] * spread, axis=0, keepdims=True)
        high_half = jnp.sum(old[:, 128:256] * spread, axis=0, keepdims=True)
        carried[pair : pair + 1, 0:128] = low_half
        carried[pair : pair + 1, 128:256] = high_half

    value_sum = jnp.concatenate(
        [arrived(1, y2_send, y2_recv, z, late_y), arrived(3, z2_send, z2_recv, y, late_z)], axis=1
    )
    value_heads = by_head((value_sum * inverse).astype(BF16).astype(F32), VD)
    numerator = forget_scale * carried[...] + (input_scale * query_key) * value_heads
    head_out = numerator / jnp.maximum(jnp.abs(denominator), 1.0)
    gain_rows = jnp.concatenate(
        [jnp.broadcast_to(hgain[h : h + 1, :], (SEQ, VD)) for h in range(HEADS)], axis=0
    )
    normed = (
        head_out * lax.rsqrt(jnp.mean(head_out * head_out, axis=1, keepdims=True) + EPSILON) * gain_rows
    )
    wait_for(o_recv, o_rsem)
    outgate_sum = o_send[z, y].astype(F32)
    for slot in range(KV - 1):
        outgate_sum = outgate_sum + o_recv[slot].astype(F32)
    outgate = by_head((outgate_sum * inverse).astype(BF16).astype(F32), VD)
    mixed = normed * jax.nn.sigmoid(outgate)
    mixed_ref[...] = jnp.concatenate(
        [mixed[h * SEQ : (h + 1) * SEQ] for h in range(HEADS)], axis=1
    ).astype(BF16)

    half, place = me // 8, me % 8
    for dz, dy in FAR:
        send(mixed_ref, heads.at[tp, place], c_ssem, c_rsem, kv=chip(dz, dy), tp=half)

    @pl.when(tp == half)
    def _():
        heads[tp, place] = mixed_ref[...]

    @pl.when(tp != half)
    def _():
        send(mixed_ref, heads.at[tp, place], c_ssem, c_rsem, tp=other)

    value_row = lax.broadcasted_iota(jnp.int32, (HEADS * SEQ, VD), 0)
    for pair in range(HEADS * SEQ):
        h, s = pair // SEQ, pair % SEQ
        outer = dot(key_cols, jnp.where(value_row == pair, value_heads, 0.0).astype(BF16))
        nmem_ref[s, h] = (
            forget_scale[pair : pair + 1, :] * mem[s, h] + input_scale[pair : pair + 1, :] * outer
        )
    ready("wout", "mgain")

    @pl.when(tp == half)
    def _():
        wait_for(o_recv, c_rsem)

    @pl.when(tp != half)
    def _():
        wait_for(o_send, c_rsem)

    def group(at, w):
        rows_of = heads[at].astype(F32).reshape(64, HEADS * VD).astype(BF16)
        return dot(rows_of, w[...]).astype(BF16).astype(F32)

    wait_for(pwout, w_rsem.at[0])
    branch = group(tp, wout) + group(other, pwout)
    own_rows = pl.ds(pl.multiple_of(tp * 64, 64), 64)
    residual = (tok[own_rows, :].astype(F32) + branch).astype(BF16)
    rows[z, y] = residual
    resid[tp] = residual

    for dz in (2, 1, 3, 0):
        for dy in (2, 1, 3, 0):
            if (dz, dy) != (0, 0):
                send(rows.at[z, y], rows.at[z, y], e_ssem, e_rsem.at[dz], kv=chip(dz, dy))
    send(resid.at[tp], resid.at[tp], d_ssem, d_rsem, tp=other)
    ready("wg", "wu", "wd")
    wait_for(pwg, w_rsem.at[1])
    wait_for(pwu, w_rsem.at[2])
    wait_for(pwd, w_rsem.at[3])

    square_two, sums = None, None
    for steps in ((0,), (1,), (3,), (2,)):
        for dz in steps:
            wait_for(rows.at[0, 0 : ROW - (dz == 0)], e_rsem.at[dz])
        for dz in steps:
            row = (z + ROW - dz) % ROW
            span = pl.ds(pl.multiple_of(row * 512, 512), 512)
            block = jnp.concatenate([rows[row, column].astype(F32) for column in range(ROW)], axis=1)
            square = jnp.sum(block * block, axis=1, keepdims=True)
            block = (block * mgain[:, span]).astype(BF16)
            parts = [dot_rows(block, w[:, span]) for w in (wg, wu, pwg, pwu)]
            if sums is None:
                square_two, sums = square, parts
            else:
                square_two, sums = square_two + square, [a + b for a, b in zip(sums, parts)]
    inverse_two = lax.rsqrt(square_two * (1.0 / (KV * QK)) + EPSILON)
    gate_own, up_own, gate_other, up_other = [total * inverse_two for total in sums]
    hidden_own = (jax.nn.silu(gate_own) * up_own).astype(BF16)
    hidden_other = (jax.nn.silu(gate_other) * up_other).astype(BF16)

    lane_two = lax.broadcasted_iota(jnp.int32, (32, 128), 1)
    slot = me * 2 + tp
    for dz in (2, 1, 3, 0):
        cols = pl.ds(pl.multiple_of(((z + dz) % ROW) * 512, 512), 512)
        part = dot(hidden_own, wd[:, cols]) + dot(hidden_other, pwd[:, cols])
        for at in range(ROW):
            top = part[0:32, at * 128 : (at + 1) * 128]
            bottom = part[32:64, at * 128 : (at + 1) * 128]
            down_send[dz, at, 0] = jnp.where(lane_two < 64, top, pltpu.roll(bottom, 64, 1)).astype(BF16)
            down_send[dz, at, 1] = jnp.where(lane_two < 64, pltpu.roll(top, 64, 1), bottom).astype(BF16)
        for dy in (2, 1, 3, 0):
            column = (y + dy) % ROW
            for core in (tp, other):
                if (dz, dy) != (0, 0) or core is other:
                    send(
                        down_send.at[dz, column, core], down_recv.at[slot], g_ssem, g_rsem,
                        kv=chip(dz, dy), tp=core,
                    )
    down_recv[slot] = down_send[0, y, tp]
    wait_for(down_recv.at[0:31], g_rsem)
    wait_for(resid.at[0], d_rsem)

    for at, ycols, zcols in ((0, early_y, early_z), (1, late_y, late_z)):
        wait_for(y1_recv.at[:, :, :, ycols], a_ssem.at[at])
        wait_for(z1_recv.at[:, :, :, zcols], a_ssem.at[at + 2])
        wait_for(y2_recv.at[:, :, ycols], b_ssem.at[at])
        wait_for(z2_recv.at[:, :, zcols], b_ssem.at[at + 2])
    wait_for(o_recv, o_ssem)
    wait_for(pwout, w_ssem.at[0])
    wait_for(pwg, w_ssem.at[1])
    wait_for(pwu, w_ssem.at[2])
    wait_for(pwd, w_ssem.at[3])

    @pl.when(tp == half)
    def _():
        wait_for(o_recv, c_ssem)

    @pl.when(tp != half)
    def _():
        wait_for(o_send, c_ssem)

    wait_for(resid.at[0], d_ssem)
    wait_for(rows.at[0:3], e_ssem)
    wait_for(rows.at[0, 0:3], e_ssem)
    wait_for(down_recv.at[0:31], g_ssem)


def finish(down_recv, resid, nmem, nnrm, nstab, out_h, nmem_h, nnrm_h, nstab_h, out, sem):
    copies = [(nmem.at[j], nmem_h.at[j]) for j in range(SEQ)]
    copies += [(nnrm, nnrm_h), (nstab, nstab_h), (out, out_h)]
    copies = [pltpu.make_async_copy(src, dst, sem.at[at]) for at, (src, dst) in enumerate(copies)]
    for copy in copies[:-1]:
        copy.start()
    pieces = []
    for core in range(2):
        total = down_recv[core].astype(F32)
        for j in range(1, KV):
            total = total + down_recv[2 * j + core].astype(F32)
        pieces += [total, pltpu.roll(total, 64, 1)]
    own = resid[...].astype(F32).reshape(128, 128)
    own = jnp.where(lax.axis_index("tp") == 0, own, pltpu.roll(own, 64, 1))
    summed = jnp.concatenate(pieces, axis=0) + own
    out[...] = jnp.transpose(summed)[0:64, :].astype(BF16)
    copies[-1].start()
    for copy in copies:
        copy.wait()


def body(tokens, mix_gain, w_query, w_key, w_value, w_outgate, w_gates, forget_bias, memory, normalizer, stabilizer,
         head_gain, w_out, mlp_gain, w_gate, w_up, w_down):
    args = (
        tokens, mix_gain.reshape(1, -1), w_query, w_key, w_value, w_outgate, w_gates.T, forget_bias.reshape(1, -1),
        memory, normalizer, stabilizer.T, head_gain, w_out, mlp_gain.reshape(1, -1), w_gate.T, w_up.T, w_down,
    )
    copies = [pltpu.VMEM(a.shape, a.dtype) for a in args]
    copies[6] = pltpu.VMEM((16, QK), BF16)
    dma = pltpu.SemaphoreType.DMA
    outs = (
        jax.ShapeDtypeStruct((64, 128), BF16),
        jax.ShapeDtypeStruct(memory.shape, F32),
        jax.ShapeDtypeStruct(normalizer.shape, F32),
        jax.ShapeDtypeStruct((HEADS, SEQ), F32),
    )
    parts = (jax.ShapeDtypeStruct((2 * KV, 32, 128), BF16), jax.ShapeDtypeStruct((2, 64, 128), BF16))
    results = pl.pallas_call(
        layer,
        name="layer",
        out_shape=tuple(pltpu.VMEM(o.shape, o.dtype) for o in parts + outs[1:]),
        in_specs=[pl.BlockSpec(memory_space=pltpu.HBM)] * len(args),
        out_specs=[pl.BlockSpec(memory_space=pltpu.VMEM)] * 5,
        scratch_shapes=copies + [
            pltpu.VMEM(w_gate.shape[::-1], BF16),
            pltpu.VMEM(w_up.shape[::-1], BF16),
            pltpu.VMEM(w_down.shape, BF16),
            pltpu.VMEM(w_out.shape, BF16),
            pltpu.VMEM((128, 128), F32),
            pltpu.VMEM((ROW, ROW, SEQ, 1152), BF16),
            pltpu.VMEM((ROW - 1, ROW, SEQ, 1152), BF16),
            pltpu.VMEM((ROW, ROW, SEQ, 1024), BF16),
            pltpu.VMEM((ROW - 1, ROW, SEQ, 1024), BF16),
            pltpu.VMEM((ROW, SEQ, 1152), BF16),
            pltpu.VMEM((ROW - 1, SEQ, 1152), BF16),
            pltpu.VMEM((ROW, SEQ, 1024), BF16),
            pltpu.VMEM((ROW - 1, SEQ, 1024), BF16),
            pltpu.VMEM((ROW, ROW, SEQ, 1024), BF16),
            pltpu.VMEM((KV - 1, SEQ, 1024), BF16),
            pltpu.VMEM((HEADS * SEQ, VD), F32),
            pltpu.VMEM((SEQ, HEADS * VD), BF16),
            pltpu.VMEM((2, KV // 2, SEQ, HEADS * VD), BF16),
            pltpu.VMEM((ROW, ROW, 64, 128), BF16),
            pltpu.VMEM((ROW, ROW, 2, 32, 128), BF16),
            pltpu.SemaphoreType.REGULAR, dma((len(args),)), dma((4,)), dma((4,)), dma((4,)), dma((4,)), dma, dma, dma((4,)), dma((4,)),
            dma, dma, dma, dma, dma, dma((4,)), dma, dma,
        ],
        compiler_params=pltpu.CompilerParams(
            collective_id=0, has_side_effects=True, vmem_limit_bytes=40 * 1024 * 1024
        ),
    )(*(pltpu.with_memory_space_constraint(a, pltpu.HBM) for a in args))
    out, new_memory, new_normalizer, new_stabilizer = pl.pallas_call(
        finish,
        name="finish",
        out_shape=outs,
        in_specs=[pl.BlockSpec(memory_space=pltpu.VMEM)] * 5,
        out_specs=[pl.BlockSpec(memory_space=pltpu.HBM)] * 4,
        scratch_shapes=[pltpu.VMEM((64, 128), BF16), dma((SEQ + 3,))],
        compiler_params=pltpu.CompilerParams(vmem_limit_bytes=8 * 1024 * 1024),
    )(*results)
    return out.T, new_memory, new_normalizer, new_stabilizer.T


def solution(mesh):
    in_specs = (
        P("dp", "kv"), P("kv"), P("kv", "tp"), P("kv", "tp"), P("kv", "tp"), P("kv", "tp"), P(), P("tp"),
        P(("dp", "kv"), "tp", None, None), P(("dp", "kv"), "tp", None), P(("dp", "kv"), "tp"), P("tp", None),
        P("tp", "kv"), P(), P(None, ("kv", "tp")), P(None, ("kv", "tp")), P(("kv", "tp"), None),
    )
    out_specs = (
        P("dp", ("kv", "tp")), P(("dp", "kv"), "tp", None, None), P(("dp", "kv"), "tp", None), P(("dp", "kv"), "tp"),
    )
    return jax.shard_map(body, mesh=mesh, in_specs=in_specs, out_specs=out_specs, check_vma=False)
```

```python
import jax
import jax.numpy as jnp
from jax import lax
from jax.experimental import pallas as pl
from jax.experimental.pallas import tpu as pltpu
from jax.sharding import PartitionSpec as P

QK = 128
VD = 256
EPSILON = 1e-06
ROW = 4
KV = 16
SEQ = 8
HEADS = 4
MESH = pl.DeviceIdType.MESH
F32 = jnp.float32
BF16 = jnp.bfloat16

FAR = sorted(
    [(a, b) for a in range(ROW) for b in range(ROW) if (a, b) != (0, 0)],
    key=lambda o: -(min(o[0], ROW - o[0]) + min(o[1], ROW - o[1])),
)


def dot(a, b):
    return jnp.dot(a, b, preferred_element_type=F32)


def dot_rows(a, b):
    return lax.dot_general(a, b, (((1,), (1,)), ((), ())), preferred_element_type=F32)


def layer(
    tok_h, gain_h, wq_h, wk_h, wv_h, wo_h, wgates_h, bias_h, mem_h, nrm_h, stab_h, hgain_h, wout_h, mgain_h,
    wg_h, wu_h, wd_h,
    down_recv, resid, nmem_ref, nnrm_ref, nstab_ref,
    tok, gain, wq, wk, wv, wo, wgates, bias, mem, nrm, stab, hgain, wout, mgain, wg, wu, wd,
    pwg, pwu, pwd, pwout, ext, y1_send, y1_recv, z1_send, z1_recv, y2_send, y2_recv, z2_send, z2_recv, o_send, o_recv, carried, mixed_ref, heads, rows, down_send,
    plane_sem, in_sem, a_ssem, a_rsem, b_ssem, b_rsem, o_ssem, o_rsem, w_ssem, w_rsem, c_ssem, c_rsem, d_ssem, d_rsem, e_ssem, e_rsem, g_ssem, g_rsem,
):
    me = lax.axis_index("kv")
    tp = lax.axis_index("tp")
    z, y = lax.div(me, ROW), lax.rem(me, ROW)
    other = 1 - tp

    def chip(dz, dy):
        return lax.rem(z + dz, ROW) * ROW + lax.rem(y + dy, ROW)

    barrier = pltpu.get_barrier_semaphore()
    for step in (2, 1, 3):
        pl.semaphore_signal(barrier, inc=1, device_id={"kv": chip(step, 0)}, device_id_type=MESH)
        pl.semaphore_signal(barrier, inc=1, device_id={"kv": chip(0, step)}, device_id_type=MESH)
    pl.semaphore_signal(barrier, inc=1, device_id={"tp": other}, device_id_type=MESH)

    loads = {}

    def load(name, src, dst):
        loads[name] = pltpu.make_async_copy(src, dst, in_sem.at[len(loads)])
        loads[name].start()

    load("tok", tok_h, tok)
    load("gain", gain_h, gain)
    load("wq", wq_h, wq)
    load("wk", wk_h, wk)
    load("wgates", wgates_h.at[:, pl.ds(pl.multiple_of(me * QK, QK), QK)], wgates)
    load("wv", wv_h, wv)
    load("wo", wo_h, wo)
    load("mem", mem_h, mem)
    load("bias", bias_h, bias)
    load("nrm", nrm_h, nrm)
    load("stab", stab_h, stab)
    load("hgain", hgain_h, hgain)
    load("wout", wout_h, wout)
    load("mgain", mgain_h, mgain)
    load("wg", wg_h, wg)
    load("wu", wu_h, wu)
    load("wd", wd_h, wd)

    def ready(*names):
        for name in names:
            loads[name].wait()

    def send(src, dst, ssem, rsem, **device):
        pltpu.make_async_remote_copy(
            src_ref=src, dst_ref=dst, send_sem=ssem, recv_sem=rsem, device_id=device, device_id_type=MESH
        ).start()

    def wait_for(ref, sem):
        pltpu.make_async_copy(ref, ref, sem).wait()

    ready("tok", "gain")
    activations = tok[...].astype(F32)
    scaled = (activations * gain[...]).astype(BF16)
    square = jnp.sum(activations * activations, axis=1, keepdims=True)
    ext[...] = jnp.zeros_like(ext)
    ready("wq", "wk", "wgates")
    ext[:, 0:16] = dot_rows(scaled, wgates[...])
    lane = lax.broadcasted_iota(jnp.int32, (128, 128), 1)
    extra = jnp.where(lane == 16, square, ext[...])

    def put(dst, at, value):
        dst[..., at : at + value.shape[1]] = value.reshape(*dst.shape[:-1], value.shape[1]).astype(BF16)

    def first_step(at, ycols, zcols):
        for step in (2, 1, 3):
            column = lax.rem(y + step, ROW)
            send(
                y1_send.at[:, column, :, ycols], y1_recv.at[step - 1, :, :, ycols], a_ssem.at[at], a_rsem.at[at],
                kv=chip(0, step),
            )
            row = lax.rem(z + step, ROW)
            send(
                z1_send.at[row, :, :, zcols], z1_recv.at[step - 1, :, :, zcols], a_ssem.at[at + 2], a_rsem.at[at + 2],
                kv=chip(step, 0),
            )

    def second_step(at, ycols, zcols):
        wait_for(y1_recv.at[:, :, :, ycols], a_rsem.at[at])
        total = y1_send[:, y, :, ycols].astype(F32)
        for slot in range(ROW - 1):
            total = total + y1_recv[slot, :, :, ycols].astype(F32)
        y2_send[:, :, ycols] = total.astype(BF16)
        for step in (2, 1, 3):
            row = lax.rem(z + step, ROW)
            send(
                y2_send.at[row, :, ycols], y2_recv.at[step - 1, :, ycols], b_ssem.at[at], b_rsem.at[at],
                kv=chip(step, 0),
            )
        wait_for(z1_recv.at[:, :, :, zcols], a_rsem.at[at + 2])
        total = z1_send[z, :, :, zcols].astype(F32)
        for slot in range(ROW - 1):
            total = total + z1_recv[slot, :, :, zcols].astype(F32)
        z2_send[:, :, zcols] = total.astype(BF16)
        for step in (2, 1, 3):
            column = lax.rem(y + step, ROW)
            send(
                z2_send.at[column, :, zcols], z2_recv.at[step - 1, :, zcols], b_ssem.at[at + 2], b_rsem.at[at + 2],
                kv=chip(0, step),
            )

    def arrived(at, send_buf, recv_buf, mine, cols):
        wait_for(recv_buf.at[:, :, cols], b_rsem.at[at])
        total = send_buf[mine, :, cols].astype(F32)
        for slot in range(ROW - 1):
            total = total + recv_buf[slot, :, cols].astype(F32)
        return total

    put(y1_send, 0, dot(scaled, wq[...]))
    put(y1_send, 512, extra)
    put(z1_send, 0, dot(scaled, wk[...]))
    pl.semaphore_wait(barrier, 2 * ROW - 1)
    for step in (2, 1, 3):
        pl.semaphore_signal(plane_sem, inc=1, device_id={"kv": chip(step, 0)}, device_id_type=MESH)
    early_y, early_z, late_y, late_z = pl.ds(0, 640), pl.ds(0, 512), pl.ds(640, 512), pl.ds(512, 512)
    first_step(0, early_y, early_z)
    ready("wv")
    put(y1_send, 640, dot(scaled, wv[:, 0:512]))
    put(z1_send, 512, dot(scaled, wv[:, 512:1024]))
    first_step(1, late_y, late_z)
    ready("wo")
    put(o_send, 0, dot(scaled, wo[...]))
    pl.semaphore_wait(plane_sem, ROW - 1)
    for slot, (dz, dy) in enumerate([(a, b) for a in (2, 1, 3, 0) for b in (2, 1, 3, 0) if (a, b) != (0, 0)]):
        to = chip(dz, dy)
        send(o_send.at[lax.div(to, ROW), lax.rem(to, ROW)], o_recv.at[slot], o_ssem, o_rsem, kv=to)
    second_step(0, early_y, early_z)
    second_step(1, late_y, late_z)
    for at, (src, dst) in enumerate(((wout_h, pwout), (wg_h, pwg), (wu_h, pwu), (wd_h, pwd))):
        send(src, dst, w_ssem.at[at], w_rsem.at[at], tp=other)

    def by_head(value, width):
        return jnp.concatenate([value[:, h * width : (h + 1) * width] for h in range(HEADS)], axis=0)

    first = arrived(0, y2_send, y2_recv, z, early_y)
    inverse = lax.rsqrt(first[:, 528:529] * (1.0 / (KV * QK)) + EPSILON)
    query = (first[:, 0:512] * inverse).astype(BF16).astype(F32)
    key_sum = arrived(2, z2_send, z2_recv, y, early_z)
    key = (key_sum * (inverse * QK ** (-0.5))).astype(BF16).astype(F32)
    gate_pre = first[:, 512:640] * inverse
    low = tp == 0
    input_pre = jnp.where(low, gate_pre[:, 0:4], gate_pre[:, 4:8])
    forget_pre = jnp.where(low, gate_pre[:, 8:12], gate_pre[:, 12:16])
    ready("bias", "nrm", "stab", "hgain")
    raw = forget_pre + bias[...]
    log_forget = jnp.minimum(raw, 0.0) - jnp.log1p(jnp.exp(-jnp.abs(raw)))
    diagonal = lax.broadcasted_iota(jnp.int32, (SEQ, SEQ), 0) == lax.broadcasted_iota(jnp.int32, (SEQ, SEQ), 1)
    old_stab = jnp.concatenate(
        [
            jnp.sum(jnp.where(diagonal, stab[h : h + 1, :], 0.0), axis=1, keepdims=True)
            for h in range(HEADS)
        ],
        axis=1,
    )
    shifted = log_forget + old_stab
    new_stab = jnp.maximum(shifted, input_pre)
    for h in range(HEADS):
        nstab_ref[h : h + 1, :] = jnp.sum(
            jnp.where(diagonal, new_stab[:, h : h + 1], 0.0), axis=0, keepdims=True
        )
    forget_scale = by_head(jnp.exp(shifted - new_stab), 1)
    input_scale = by_head(jnp.exp(input_pre - new_stab), 1)
    query_heads = by_head(query, QK)
    key_heads = by_head(key, QK)
    old_normalizer = jnp.concatenate([nrm[:, h, :] for h in range(HEADS)], axis=0)
    new_normalizer = forget_scale * old_normalizer + input_scale * key_heads
    for h in range(HEADS):
        nnrm_ref[:, h, :] = new_normalizer[h * SEQ : (h + 1) * SEQ]
    denominator = jnp.sum(query_heads * new_normalizer, axis=1, keepdims=True)
    query_key = jnp.sum(query_heads * key_heads, axis=1, keepdims=True)
    query_cols = jnp.transpose(query_heads).astype(BF16)
    key_cols = jnp.transpose(key_heads).astype(BF16)
    pair_row = lax.broadcasted_iota(jnp.int32, (HEADS * SEQ, QK), 0)
    ready("mem")
    for pair in range(HEADS * SEQ):
        h, s = pair // SEQ, pair % SEQ
        spread = dot(query_cols, jnp.where(pair_row == pair, 1.0, 0.0).astype(BF16))
        old = mem[s, h]
        low_half = jnp.sum(old[:, 0:128] * spread, axis=0, keepdims=True)
        high_half = jnp.sum(old[:, 128:256] * spread, axis=0, keepdims=True)
        carried[pair : pair + 1, 0:128] = low_half
        carried[pair : pair + 1, 128:256] = high_half

    value_sum = jnp.concatenate(
        [arrived(1, y2_send, y2_recv, z, late_y), arrived(3, z2_send, z2_recv, y, late_z)], axis=1
    )
    value_heads = by_head((value_sum * inverse).astype(BF16).astype(F32), VD)
    numerator = forget_scale * carried[...] + (input_scale * query_key) * value_heads
    head_out = numerator / jnp.maximum(jnp.abs(denominator), 1.0)
    gain_rows = jnp.concatenate(
        [jnp.broadcast_to(hgain[h : h + 1, :], (SEQ, VD)) for h in range(HEADS)], axis=0
    )
    normed = (
        head_out * lax.rsqrt(jnp.mean(head_out * head_out, axis=1, keepdims=True) + EPSILON) * gain_rows
    )
    wait_for(o_recv, o_rsem)
    outgate_sum = o_send[z, y].astype(F32)
    for slot in range(KV - 1):
        outgate_sum = outgate_sum + o_recv[slot].astype(F32)
    outgate = by_head((outgate_sum * inverse).astype(BF16).astype(F32), VD)
    mixed = normed * jax.nn.sigmoid(outgate)
    mixed_ref[...] = jnp.concatenate(
        [mixed[h * SEQ : (h + 1) * SEQ] for h in range(HEADS)], axis=1
    ).astype(BF16)

    half, place = lax.div(me, 8), lax.rem(me, 8)
    for dz, dy in [(a, b) for a in (2, 1, 3, 0) for b in (2, 1, 3, 0) if (a, b) != (0, 0)]:
        send(mixed_ref, heads.at[tp, place], c_ssem, c_rsem, kv=chip(dz, dy), tp=half)

    @pl.when(tp == half)
    def _():
        heads[tp, place] = mixed_ref[...]

    @pl.when(tp != half)
    def _():
        send(mixed_ref, heads.at[tp, place], c_ssem, c_rsem, tp=other)

    value_row = lax.broadcasted_iota(jnp.int32, (HEADS * SEQ, VD), 0)
    for pair in range(HEADS * SEQ):
        h, s = pair // SEQ, pair % SEQ
        outer = dot(key_cols, jnp.where(value_row == pair, value_heads, 0.0).astype(BF16))
        nmem_ref[s, h] = (
            forget_scale[pair : pair + 1, :] * mem[s, h] + input_scale[pair : pair + 1, :] * outer
        )
    ready("wout", "mgain")

    @pl.when(tp == half)
    def _():
        wait_for(o_recv, c_rsem)

    @pl.when(tp != half)
    def _():
        wait_for(o_send, c_rsem)

    def group(at, w):
        rows_of = heads[at].astype(F32).reshape(64, HEADS * VD).astype(BF16)
        return dot(rows_of, w[...]).astype(BF16).astype(F32)

    wait_for(pwout, w_rsem.at[0])
    branch = group(tp, wout) + group(other, pwout)
    own_rows = pl.ds(pl.multiple_of(tp * 64, 64), 64)
    residual = (tok[own_rows, :].astype(F32) + branch).astype(BF16)
    rows[z, y] = residual
    resid[tp] = residual

    for dz in (2, 1, 3, 0):
        for dy in (2, 1, 3, 0):
            if (dz, dy) != (0, 0):
                send(rows.at[z, y], rows.at[z, y], e_ssem, e_rsem.at[dz], kv=chip(dz, dy))
    send(resid.at[tp], resid.at[tp], d_ssem, d_rsem, tp=other)
    ready("wg", "wu", "wd")
    wait_for(pwg, w_rsem.at[1])
    wait_for(pwu, w_rsem.at[2])
    wait_for(pwd, w_rsem.at[3])

    square_two, sums = None, None
    for steps in ((0,), (1,), (3,), (2,)):
        for dz in steps:
            wait_for(rows.at[0, 0 : ROW - (dz == 0)], e_rsem.at[dz])
        for dz in steps:
            row = lax.rem(z + ROW - dz, ROW)
            span = pl.ds(pl.multiple_of(row * 512, 512), 512)
            block = jnp.concatenate([rows[row, column].astype(F32) for column in range(ROW)], axis=1)
            square = jnp.sum(block * block, axis=1, keepdims=True)
            block = (block * mgain[:, span]).astype(BF16)
            parts = [dot_rows(block, w[:, span]) for w in (wg, wu, pwg, pwu)]
            if sums is None:
                square_two, sums = square, parts
            else:
                square_two, sums = square_two + square, [a + b for a, b in zip(sums, parts)]
    inverse_two = lax.rsqrt(square_two * (1.0 / (KV * QK)) + EPSILON)
    gate_own, up_own, gate_other, up_other = [total * inverse_two for total in sums]
    hidden_own = (jax.nn.silu(gate_own) * up_own).astype(BF16)
    hidden_other = (jax.nn.silu(gate_other) * up_other).astype(BF16)

    lane_two = lax.broadcasted_iota(jnp.int32, (32, 128), 1)
    slot = me * 2 + tp
    for dz in (2, 1, 3, 0):
        cols = pl.ds(pl.multiple_of(lax.rem(z + dz, ROW) * 512, 512), 512)
        part = dot(hidden_own, wd[:, cols]) + dot(hidden_other, pwd[:, cols])
        for at in range(ROW):
            top = part[0:32, at * 128 : (at + 1) * 128]
            bottom = part[32:64, at * 128 : (at + 1) * 128]
            down_send[dz, at, 0] = jnp.where(lane_two < 64, top, pltpu.roll(bottom, 64, 1)).astype(BF16)
            down_send[dz, at, 1] = jnp.where(lane_two < 64, pltpu.roll(top, 64, 1), bottom).astype(BF16)
        for dy in (2, 1, 3, 0):
            column = lax.rem(y + dy, ROW)
            for core in (tp, other):
                if (dz, dy) != (0, 0) or core is other:
                    send(
                        down_send.at[dz, column, core], down_recv.at[slot], g_ssem, g_rsem,
                        kv=chip(dz, dy), tp=core,
                    )
    down_recv[slot] = down_send[0, y, tp]
    wait_for(down_recv.at[0:31], g_rsem)
    wait_for(resid.at[0], d_rsem)

    for at, ycols, zcols in ((0, early_y, early_z), (1, late_y, late_z)):
        wait_for(y1_recv.at[:, :, :, ycols], a_ssem.at[at])
        wait_for(z1_recv.at[:, :, :, zcols], a_ssem.at[at + 2])
        wait_for(y2_recv.at[:, :, ycols], b_ssem.at[at])
        wait_for(z2_recv.at[:, :, zcols], b_ssem.at[at + 2])
    wait_for(o_recv, o_ssem)
    wait_for(pwout, w_ssem.at[0])
    wait_for(pwg, w_ssem.at[1])
    wait_for(pwu, w_ssem.at[2])
    wait_for(pwd, w_ssem.at[3])

    @pl.when(tp == half)
    def _():
        wait_for(o_recv, c_ssem)

    @pl.when(tp != half)
    def _():
        wait_for(o_send, c_ssem)

    wait_for(resid.at[0], d_ssem)
    wait_for(rows.at[0:3], e_ssem)
    wait_for(rows.at[0, 0:3], e_ssem)
    wait_for(down_recv.at[0:31], g_ssem)


def finish(down_recv, resid, nmem, nnrm, nstab, out_h, nmem_h, nnrm_h, nstab_h, out, sem):
    copies = [(nmem.at[j], nmem_h.at[j]) for j in range(SEQ)]
    copies += [(nnrm, nnrm_h), (nstab, nstab_h), (out, out_h)]
    copies = [pltpu.make_async_copy(src, dst, sem.at[at]) for at, (src, dst) in enumerate(copies)]
    for copy in copies[:-1]:
        copy.start()
    pieces = []
    for core in range(2):
        total = down_recv[core].astype(F32)
        for j in range(1, KV):
            total = total + down_recv[2 * j + core].astype(F32)
        pieces += [total, pltpu.roll(total, 64, 1)]
    own = resid[...].astype(F32).reshape(128, 128)
    own = jnp.where(lax.axis_index("tp") == 0, own, pltpu.roll(own, 64, 1))
    summed = jnp.concatenate(pieces, axis=0) + own
    out[...] = jnp.transpose(summed)[0:64, :].astype(BF16)
    copies[-1].start()
    for copy in copies:
        copy.wait()


def body(tokens, mix_gain, w_query, w_key, w_value, w_outgate, w_gates, forget_bias, memory, normalizer, stabilizer,
         head_gain, w_out, mlp_gain, w_gate, w_up, w_down):
    args = (
        tokens, mix_gain.reshape(1, -1), w_query, w_key, w_value, w_outgate, w_gates.T, forget_bias.reshape(1, -1),
        memory, normalizer, stabilizer.T, head_gain, w_out, mlp_gain.reshape(1, -1), w_gate.T, w_up.T, w_down,
    )
    copies = [pltpu.VMEM(a.shape, a.dtype) for a in args]
    copies[6] = pltpu.VMEM((16, QK), BF16)
    dma = pltpu.SemaphoreType.DMA
    outs = (
        jax.ShapeDtypeStruct((64, 128), BF16),
        jax.ShapeDtypeStruct(memory.shape, F32),
        jax.ShapeDtypeStruct(normalizer.shape, F32),
        jax.ShapeDtypeStruct((HEADS, SEQ), F32),
    )
    parts = (jax.ShapeDtypeStruct((2 * KV, 32, 128), BF16), jax.ShapeDtypeStruct((2, 64, 128), BF16))
    results = pl.pallas_call(
        layer,
        name="layer",
        out_shape=tuple(pltpu.VMEM(o.shape, o.dtype) for o in parts + outs[1:]),
        in_specs=[pl.BlockSpec(memory_space=pltpu.HBM)] * len(args),
        out_specs=[pl.BlockSpec(memory_space=pltpu.VMEM)] * 5,
        scratch_shapes=copies + [
            pltpu.VMEM(w_gate.shape[::-1], BF16),
            pltpu.VMEM(w_up.shape[::-1], BF16),
            pltpu.VMEM(w_down.shape, BF16),
            pltpu.VMEM(w_out.shape, BF16),
            pltpu.VMEM((128, 128), F32),
            pltpu.VMEM((ROW, ROW, SEQ, 1152), BF16),
            pltpu.VMEM((ROW - 1, ROW, SEQ, 1152), BF16),
            pltpu.VMEM((ROW, ROW, SEQ, 1024), BF16),
            pltpu.VMEM((ROW - 1, ROW, SEQ, 1024), BF16),
            pltpu.VMEM((ROW, SEQ, 1152), BF16),
            pltpu.VMEM((ROW - 1, SEQ, 1152), BF16),
            pltpu.VMEM((ROW, SEQ, 1024), BF16),
            pltpu.VMEM((ROW - 1, SEQ, 1024), BF16),
            pltpu.VMEM((ROW, ROW, SEQ, 1024), BF16),
            pltpu.VMEM((KV - 1, SEQ, 1024), BF16),
            pltpu.VMEM((HEADS * SEQ, VD), F32),
            pltpu.VMEM((SEQ, HEADS * VD), BF16),
            pltpu.VMEM((2, KV // 2, SEQ, HEADS * VD), BF16),
            pltpu.VMEM((ROW, ROW, 64, 128), BF16),
            pltpu.VMEM((ROW, ROW, 2, 32, 128), BF16),
            pltpu.SemaphoreType.REGULAR, dma((len(args),)), dma((4,)), dma((4,)), dma((4,)), dma((4,)), dma, dma, dma((4,)), dma((4,)),
            dma, dma, dma, dma, dma, dma((4,)), dma, dma,
        ],
        compiler_params=pltpu.CompilerParams(
            collective_id=0, has_side_effects=True, vmem_limit_bytes=40 * 1024 * 1024
        ),
    )(*(pltpu.with_memory_space_constraint(a, pltpu.HBM) for a in args))
    out, new_memory, new_normalizer, new_stabilizer = pl.pallas_call(
        finish,
        name="finish",
        out_shape=outs,
        in_specs=[pl.BlockSpec(memory_space=pltpu.VMEM)] * 5,
        out_specs=[pl.BlockSpec(memory_space=pltpu.HBM)] * 4,
        scratch_shapes=[pltpu.VMEM((64, 128), BF16), dma((SEQ + 3,))],
        compiler_params=pltpu.CompilerParams(vmem_limit_bytes=8 * 1024 * 1024),
    )(*results)
    return out.T, new_memory, new_normalizer, new_stabilizer.T


def solution(mesh):
    in_specs = (
        P("dp", "kv"), P("kv"), P("kv", "tp"), P("kv", "tp"), P("kv", "tp"), P("kv", "tp"), P(), P("tp"),
        P(("dp", "kv"), "tp", None, None), P(("dp", "kv"), "tp", None), P(("dp", "kv"), "tp"), P("tp", None),
        P("tp", "kv"), P(), P(None, ("kv", "tp")), P(None, ("kv", "tp")), P(("kv", "tp"), None),
    )
    out_specs = (
        P("dp", ("kv", "tp")), P(("dp", "kv"), "tp", None, None), P(("dp", "kv"), "tp", None), P(("dp", "kv"), "tp"),
    )
    return jax.shard_map(body, mesh=mesh, in_specs=in_specs, out_specs=out_specs, check_vma=False)
```

```python
import jax
import jax.numpy as jnp
from jax import lax
from jax.experimental import pallas as pl
from jax.experimental.pallas import tpu as pltpu
from jax.sharding import PartitionSpec as P

QK = 128
VD = 256
EPSILON = 1e-06
ROW = 4
KV = 16
SEQ = 8
HEADS = 4
MESH = pl.DeviceIdType.MESH
F32 = jnp.float32
BF16 = jnp.bfloat16

FAR = sorted(
    [(a, b) for a in range(ROW) for b in range(ROW) if (a, b) != (0, 0)],
    key=lambda o: -(min(o[0], ROW - o[0]) + min(o[1], ROW - o[1])),
)


def dot(a, b):
    return jnp.dot(a, b, preferred_element_type=F32)


def dot_rows(a, b):
    return lax.dot_general(a, b, (((1,), (1,)), ((), ())), preferred_element_type=F32)


def layer(
    tok_h, gain_h, wq_h, wk_h, wv_h, wo_h, wgates_h, bias_h, mem_h, nrm_h, stab_h, hgain_h, wout_h, mgain_h,
    wg_h, wu_h, wd_h,
    down_recv, resid, nmem_ref, nnrm_ref, nstab_ref,
    tok, gain, wq, wk, wv, wo, wgates, bias, mem, nrm, stab, hgain, wout, mgain, wg, wu, wd,
    pwg, pwu, pwd, pwout, ext, y1_send, y1_recv, z1_send, z1_recv, y2_send, y2_recv, z2_send, z2_recv, o_send, o_recv, carried, mixed_ref, heads, rows, down_send,
    plane_sem, in_sem, a_ssem, a_rsem, b_ssem, b_rsem, o_ssem, o_rsem, w_ssem, w_rsem, c_ssem, c_rsem, d_ssem, d_rsem, e_ssem, e_rsem, g_ssem, g_rsem,
):
    me = lax.axis_index("kv")
    tp = lax.axis_index("tp")
    z, y = lax.div(me, ROW), lax.rem(me, ROW)
    other = 1 - tp

    def chip(dz, dy):
        return lax.rem(z + dz, ROW) * ROW + lax.rem(y + dy, ROW)

    barrier = pltpu.get_barrier_semaphore()
    for step in (2, 1, 3):
        pl.semaphore_signal(barrier, inc=1, device_id={"kv": chip(step, 0)}, device_id_type=MESH)
        pl.semaphore_signal(barrier, inc=1, device_id={"kv": chip(0, step)}, device_id_type=MESH)
    pl.semaphore_signal(barrier, inc=1, device_id={"tp": other}, device_id_type=MESH)

    loads = {}

    def load(name, src, dst):
        loads[name] = pltpu.make_async_copy(src, dst, in_sem.at[len(loads)])
        loads[name].start()

    load("tok", tok_h, tok)
    load("gain", gain_h, gain)
    load("wq", wq_h, wq)
    load("wk", wk_h, wk)
    load("wgates", wgates_h.at[:, pl.ds(pl.multiple_of(me * QK, QK), QK)], wgates)
    load("wv", wv_h, wv)
    load("wo", wo_h, wo)
    load("mem", mem_h, mem)
    load("bias", bias_h, bias)
    load("nrm", nrm_h, nrm)
    load("stab", stab_h, stab)
    load("hgain", hgain_h, hgain)
    load("wout", wout_h, wout)
    load("mgain", mgain_h, mgain)
    load("wg", wg_h, wg)
    load("wu", wu_h, wu)
    load("wd", wd_h, wd)

    def ready(*names):
        for name in names:
            loads[name].wait()

    def send(src, dst, ssem, rsem, **device):
        pltpu.make_async_remote_copy(
            src_ref=src, dst_ref=dst, send_sem=ssem, recv_sem=rsem, device_id=device, device_id_type=MESH
        ).start()

    def wait_for(ref, sem):
        pltpu.make_async_copy(ref, ref, sem).wait()

    ready("tok", "gain")
    activations = tok[...].astype(F32)
    scaled = (activations * gain[...]).astype(BF16)
    square = jnp.sum(activations * activations, axis=1, keepdims=True)
    ext[...] = jnp.zeros_like(ext)
    ready("wq", "wk", "wgates")
    ext[:, 0:16] = dot_rows(scaled, wgates[...])
    lane = lax.broadcasted_iota(jnp.int32, (128, 128), 1)
    extra = jnp.where(lane == 16, square, ext[...])

    def put(dst, at, value):
        dst[..., at : at + value.shape[1]] = value.reshape(*dst.shape[:-1], value.shape[1]).astype(BF16)

    def first_step(at, ycols, zcols):
        for step in (2, 1, 3):
            column = lax.rem(y + step, ROW)
            send(
                y1_send.at[:, column, :, ycols], y1_recv.at[step - 1, :, :, ycols], a_ssem.at[at], a_rsem.at[at],
                kv=chip(0, step),
            )
            row = lax.rem(z + step, ROW)
            send(
                z1_send.at[row, :, :, zcols], z1_recv.at[step - 1, :, :, zcols], a_ssem.at[at + 2], a_rsem.at[at + 2],
                kv=chip(step, 0),
            )

    def second_step(at, ycols, zcols):
        wait_for(y1_recv.at[:, :, :, ycols], a_rsem.at[at])
        total = y1_send[:, y, :, ycols].astype(F32)
        for slot in range(ROW - 1):
            total = total + y1_recv[slot, :, :, ycols].astype(F32)
        y2_send[:, :, ycols] = total.astype(BF16)
        for step in (2, 1, 3):
            row = lax.rem(z + step, ROW)
            send(
                y2_send.at[row, :, ycols], y2_recv.at[step - 1, :, ycols], b_ssem.at[at], b_rsem.at[at],
                kv=chip(step, 0),
            )
        wait_for(z1_recv.at[:, :, :, zcols], a_rsem.at[at + 2])
        total = z1_send[z, :, :, zcols].astype(F32)
        for slot in range(ROW - 1):
            total = total + z1_recv[slot, :, :, zcols].astype(F32)
        z2_send[:, :, zcols] = total.astype(BF16)
        for step in (2, 1, 3):
            column = lax.rem(y + step, ROW)
            send(
                z2_send.at[column, :, zcols], z2_recv.at[step - 1, :, zcols], b_ssem.at[at + 2], b_rsem.at[at + 2],
                kv=chip(0, step),
            )

    def arrived(at, send_buf, recv_buf, mine, cols):
        wait_for(recv_buf.at[:, :, cols], b_rsem.at[at])
        total = send_buf[mine, :, cols].astype(F32)
        for slot in range(ROW - 1):
            total = total + recv_buf[slot, :, cols].astype(F32)
        return total

    put(y1_send, 0, dot(scaled, wq[...]))
    put(y1_send, 512, extra)
    put(z1_send, 0, dot(scaled, wk[...]))
    pl.semaphore_wait(barrier, 2 * ROW - 1)
    for step in (2, 1, 3):
        pl.semaphore_signal(plane_sem, inc=1, device_id={"kv": chip(step, 0)}, device_id_type=MESH)
    early_y, early_z, late_y, late_z = pl.ds(0, 640), pl.ds(0, 512), pl.ds(640, 512), pl.ds(512, 512)
    first_step(0, early_y, early_z)
    ready("wv")
    put(y1_send, 640, dot(scaled, wv[:, 0:512]))
    put(z1_send, 512, dot(scaled, wv[:, 512:1024]))
    first_step(1, late_y, late_z)
    ready("wo")
    put(o_send, 0, dot(scaled, wo[...]))
    pl.semaphore_wait(plane_sem, ROW - 1)
    for slot, (dz, dy) in enumerate([(a, b) for a in (2, 1, 3, 0) for b in (2, 1, 3, 0) if (a, b) != (0, 0)]):
        to = chip(dz, dy)
        send(o_send.at[lax.div(to, ROW), lax.rem(to, ROW)], o_recv.at[slot], o_ssem, o_rsem, kv=to)
    second_step(0, early_y, early_z)
    second_step(1, late_y, late_z)
    for at, (src, dst) in enumerate(((wout_h, pwout), (wg_h, pwg), (wu_h, pwu), (wd_h, pwd))):
        send(src, dst, w_ssem.at[at], w_rsem.at[at], tp=other)

    def by_head(value, width):
        return jnp.concatenate([value[:, h * width : (h + 1) * width] for h in range(HEADS)], axis=0)

    first = arrived(0, y2_send, y2_recv, z, early_y)
    inverse = lax.rsqrt(first[:, 528:529] * (1.0 / (KV * QK)) + EPSILON)
    query = (first[:, 0:512] * inverse).astype(BF16).astype(F32)
    key_sum = arrived(2, z2_send, z2_recv, y, early_z)
    key = (key_sum * (inverse * QK ** (-0.5))).astype(BF16).astype(F32)
    gate_pre = first[:, 512:640] * inverse
    low = tp == 0
    input_pre = jnp.where(low, gate_pre[:, 0:4], gate_pre[:, 4:8])
    forget_pre = jnp.where(low, gate_pre[:, 8:12], gate_pre[:, 12:16])
    ready("bias", "nrm", "stab", "hgain")
    raw = forget_pre + bias[...]
    log_forget = jnp.minimum(raw, 0.0) - jnp.log1p(jnp.exp(-jnp.abs(raw)))
    diagonal = lax.broadcasted_iota(jnp.int32, (SEQ, SEQ), 0) == lax.broadcasted_iota(jnp.int32, (SEQ, SEQ), 1)
    old_stab = jnp.concatenate(
        [
            jnp.sum(jnp.where(diagonal, stab[h : h + 1, :], 0.0), axis=1, keepdims=True)
            for h in range(HEADS)
        ],
        axis=1,
    )
    shifted = log_forget + old_stab
    new_stab = jnp.maximum(shifted, input_pre)
    for h in range(HEADS):
        nstab_ref[h : h + 1, :] = jnp.sum(
            jnp.where(diagonal, new_stab[:, h : h + 1], 0.0), axis=0, keepdims=True
        )
    forget_scale = by_head(jnp.exp(shifted - new_stab), 1)
    input_scale = by_head(jnp.exp(input_pre - new_stab), 1)
    query_heads = by_head(query, QK)
    key_heads = by_head(key, QK)
    old_normalizer = jnp.concatenate([nrm[:, h, :] for h in range(HEADS)], axis=0)
    new_normalizer = forget_scale * old_normalizer + input_scale * key_heads
    for h in range(HEADS):
        nnrm_ref[:, h, :] = new_normalizer[h * SEQ : (h + 1) * SEQ]
    denominator = jnp.sum(query_heads * new_normalizer, axis=1, keepdims=True)
    query_key = jnp.sum(query_heads * key_heads, axis=1, keepdims=True)
    query_cols = jnp.transpose(query_heads).astype(BF16)
    key_cols = jnp.transpose(key_heads).astype(BF16)
    pair_row = lax.broadcasted_iota(jnp.int32, (HEADS * SEQ, QK), 0)
    ready("mem")
    for pair in range(HEADS * SEQ):
        h, s = pair // SEQ, pair % SEQ
        spread = dot(query_cols, jnp.where(pair_row == pair, 1.0, 0.0).astype(BF16))
        old = mem[s, h]
        low_half = jnp.sum(old[:, 0:128] * spread, axis=0, keepdims=True)
        high_half = jnp.sum(old[:, 128:256] * spread, axis=0, keepdims=True)
        carried[pair : pair + 1, 0:128] = low_half
        carried[pair : pair + 1, 128:256] = high_half

    value_sum = jnp.concatenate(
        [arrived(1, y2_send, y2_recv, z, late_y), arrived(3, z2_send, z2_recv, y, late_z)], axis=1
    )
    value_heads = by_head((value_sum * inverse).astype(BF16).astype(F32), VD)
    numerator = forget_scale * carried[...] + (input_scale * query_key) * value_heads
    head_out = numerator / jnp.maximum(jnp.abs(denominator), 1.0)
    gain_rows = jnp.concatenate(
        [jnp.broadcast_to(hgain[h : h + 1, :], (SEQ, VD)) for h in range(HEADS)], axis=0
    )
    normed = (
        head_out * lax.rsqrt(jnp.mean(head_out * head_out, axis=1, keepdims=True) + EPSILON) * gain_rows
    )
    wait_for(o_recv, o_rsem)
    outgate_sum = o_send[z, y].astype(F32)
    for slot in range(KV - 1):
        outgate_sum = outgate_sum + o_recv[slot].astype(F32)
    outgate = by_head((outgate_sum * inverse).astype(BF16).astype(F32), VD)
    mixed = normed * jax.nn.sigmoid(outgate)
    mixed_ref[...] = jnp.concatenate(
        [mixed[h * SEQ : (h + 1) * SEQ] for h in range(HEADS)], axis=1
    ).astype(BF16)

    half, place = lax.div(me, 8), lax.rem(me, 8)
    for dz, dy in [(a, b) for a in (2, 1, 3, 0) for b in (2, 1, 3, 0) if (a, b) != (0, 0)]:
        send(mixed_ref, heads.at[tp, place], c_ssem, c_rsem, kv=chip(dz, dy), tp=half)

    @pl.when(tp == half)
    def _():
        heads[tp, place] = mixed_ref[...]

    @pl.when(tp != half)
    def _():
        send(mixed_ref, heads.at[tp, place], c_ssem, c_rsem, tp=other)

    value_row = lax.broadcasted_iota(jnp.int32, (HEADS * SEQ, VD), 0)
    for pair in range(HEADS * SEQ):
        h, s = pair // SEQ, pair % SEQ
        outer = dot(key_cols, jnp.where(value_row == pair, value_heads, 0.0).astype(BF16))
        nmem_ref[s, h] = (
            forget_scale[pair : pair + 1, :] * mem[s, h] + input_scale[pair : pair + 1, :] * outer
        )
    ready("wout", "mgain")

    @pl.when(tp == half)
    def _():
        wait_for(o_recv, c_rsem)

    @pl.when(tp != half)
    def _():
        wait_for(o_send, c_rsem)

    def group(at, w):
        rows_of = heads[at].astype(F32).reshape(64, HEADS * VD).astype(BF16)
        return dot(rows_of, w[...]).astype(BF16).astype(F32)

    wait_for(pwout, w_rsem.at[0])
    branch = group(tp, wout) + group(other, pwout)
    own_rows = pl.ds(pl.multiple_of(tp * 64, 64), 64)
    residual = (tok[own_rows, :].astype(F32) + branch).astype(BF16)
    rows[z, y] = residual
    resid[tp] = residual

    for dz in (2, 1, 3, 0):
        for dy in (2, 1, 3, 0):
            if (dz, dy) != (0, 0):
                send(rows.at[z, y], rows.at[z, y], e_ssem, e_rsem.at[dz], kv=chip(dz, dy))
    send(resid.at[tp], resid.at[tp], d_ssem, d_rsem, tp=other)
    ready("wg", "wu", "wd")
    wait_for(pwg, w_rsem.at[1])
    wait_for(pwu, w_rsem.at[2])
    wait_for(pwd, w_rsem.at[3])

    square_two, sums = None, None
    for steps in ((0,), (1,), (3,), (2,)):
        for dz in steps:
            wait_for(rows.at[0, 0 : ROW - (dz == 0)], e_rsem.at[dz])
        for dz in steps:
            row = lax.rem(z + ROW - dz, ROW)
            span = pl.ds(pl.multiple_of(row * 512, 512), 512)
            block = jnp.concatenate([rows[row, column].astype(F32) for column in range(ROW)], axis=1)
            square = jnp.sum(block * block, axis=1, keepdims=True)
            block = (block * mgain[:, span]).astype(BF16)
            parts = [dot_rows(block, w[:, span]) for w in (wg, wu, pwg, pwu)]
            if sums is None:
                square_two, sums = square, parts
            else:
                square_two, sums = square_two + square, [a + b for a, b in zip(sums, parts)]
    inverse_two = lax.rsqrt(square_two * (1.0 / (KV * QK)) + EPSILON)
    gate_own, up_own, gate_other, up_other = [total * inverse_two for total in sums]
    hidden_own = (jax.nn.silu(gate_own) * up_own).astype(BF16)
    hidden_other = (jax.nn.silu(gate_other) * up_other).astype(BF16)

    lane_two = lax.broadcasted_iota(jnp.int32, (32, 128), 1)
    slot = me * 2 + tp
    for dz in (1, 3, 2, 0):
        cols = pl.ds(pl.multiple_of(lax.rem(z + dz, ROW) * 512, 512), 512)
        part = dot(hidden_own, wd[:, cols]) + dot(hidden_other, pwd[:, cols])
        for at in range(ROW):
            top = part[0:32, at * 128 : (at + 1) * 128]
            bottom = part[32:64, at * 128 : (at + 1) * 128]
            down_send[dz, at, 0] = jnp.where(lane_two < 64, top, pltpu.roll(bottom, 64, 1)).astype(BF16)
            down_send[dz, at, 1] = jnp.where(lane_two < 64, pltpu.roll(top, 64, 1), bottom).astype(BF16)
        for dy in (2, 1, 3, 0):
            column = lax.rem(y + dy, ROW)
            for core in (tp, other):
                if (dz, dy) != (0, 0) or core is other:
                    send(
                        down_send.at[dz, column, core], down_recv.at[slot], g_ssem, g_rsem,
                        kv=chip(dz, dy), tp=core,
                    )
    down_recv[slot] = down_send[0, y, tp]
    wait_for(down_recv.at[0:31], g_rsem)
    wait_for(resid.at[0], d_rsem)

    for at, ycols, zcols in ((0, early_y, early_z), (1, late_y, late_z)):
        wait_for(y1_recv.at[:, :, :, ycols], a_ssem.at[at])
        wait_for(z1_recv.at[:, :, :, zcols], a_ssem.at[at + 2])
        wait_for(y2_recv.at[:, :, ycols], b_ssem.at[at])
        wait_for(z2_recv.at[:, :, zcols], b_ssem.at[at + 2])
    wait_for(o_recv, o_ssem)
    wait_for(pwout, w_ssem.at[0])
    wait_for(pwg, w_ssem.at[1])
    wait_for(pwu, w_ssem.at[2])
    wait_for(pwd, w_ssem.at[3])

    @pl.when(tp == half)
    def _():
        wait_for(o_recv, c_ssem)

    @pl.when(tp != half)
    def _():
        wait_for(o_send, c_ssem)

    wait_for(resid.at[0], d_ssem)
    wait_for(rows.at[0:3], e_ssem)
    wait_for(rows.at[0, 0:3], e_ssem)
    wait_for(down_recv.at[0:31], g_ssem)


def finish(down_recv, resid, nmem, nnrm, nstab, out_h, nmem_h, nnrm_h, nstab_h, out, sem):
    copies = [(nmem.at[j], nmem_h.at[j]) for j in range(SEQ)]
    copies += [(nnrm, nnrm_h), (nstab, nstab_h), (out, out_h)]
    copies = [pltpu.make_async_copy(src, dst, sem.at[at]) for at, (src, dst) in enumerate(copies)]
    for copy in copies[:-1]:
        copy.start()
    pieces = []
    for core in range(2):
        total = down_recv[core].astype(F32)
        for j in range(1, KV):
            total = total + down_recv[2 * j + core].astype(F32)
        pieces += [total, pltpu.roll(total, 64, 1)]
    own = resid[...].astype(F32).reshape(128, 128)
    own = jnp.where(lax.axis_index("tp") == 0, own, pltpu.roll(own, 64, 1))
    summed = jnp.concatenate(pieces, axis=0) + own
    out[...] = jnp.transpose(summed)[0:64, :].astype(BF16)
    copies[-1].start()
    for copy in copies:
        copy.wait()


def body(tokens, mix_gain, w_query, w_key, w_value, w_outgate, w_gates, forget_bias, memory, normalizer, stabilizer,
         head_gain, w_out, mlp_gain, w_gate, w_up, w_down):
    args = (
        tokens, mix_gain.reshape(1, -1), w_query, w_key, w_value, w_outgate, w_gates.T, forget_bias.reshape(1, -1),
        memory, normalizer, stabilizer.T, head_gain, w_out, mlp_gain.reshape(1, -1), w_gate.T, w_up.T, w_down,
    )
    copies = [pltpu.VMEM(a.shape, a.dtype) for a in args]
    copies[6] = pltpu.VMEM((16, QK), BF16)
    dma = pltpu.SemaphoreType.DMA
    outs = (
        jax.ShapeDtypeStruct((64, 128), BF16),
        jax.ShapeDtypeStruct(memory.shape, F32),
        jax.ShapeDtypeStruct(normalizer.shape, F32),
        jax.ShapeDtypeStruct((HEADS, SEQ), F32),
    )
    parts = (jax.ShapeDtypeStruct((2 * KV, 32, 128), BF16), jax.ShapeDtypeStruct((2, 64, 128), BF16))
    results = pl.pallas_call(
        layer,
        name="layer",
        out_shape=tuple(pltpu.VMEM(o.shape, o.dtype) for o in parts + outs[1:]),
        in_specs=[pl.BlockSpec(memory_space=pltpu.HBM)] * len(args),
        out_specs=[pl.BlockSpec(memory_space=pltpu.VMEM)] * 5,
        scratch_shapes=copies + [
            pltpu.VMEM(w_gate.shape[::-1], BF16),
            pltpu.VMEM(w_up.shape[::-1], BF16),
            pltpu.VMEM(w_down.shape, BF16),
            pltpu.VMEM(w_out.shape, BF16),
            pltpu.VMEM((128, 128), F32),
            pltpu.VMEM((ROW, ROW, SEQ, 1152), BF16),
            pltpu.VMEM((ROW - 1, ROW, SEQ, 1152), BF16),
            pltpu.VMEM((ROW, ROW, SEQ, 1024), BF16),
            pltpu.VMEM((ROW - 1, ROW, SEQ, 1024), BF16),
            pltpu.VMEM((ROW, SEQ, 1152), BF16),
            pltpu.VMEM((ROW - 1, SEQ, 1152), BF16),
            pltpu.VMEM((ROW, SEQ, 1024), BF16),
            pltpu.VMEM((ROW - 1, SEQ, 1024), BF16),
            pltpu.VMEM((ROW, ROW, SEQ, 1024), BF16),
            pltpu.VMEM((KV - 1, SEQ, 1024), BF16),
            pltpu.VMEM((HEADS * SEQ, VD), F32),
            pltpu.VMEM((SEQ, HEADS * VD), BF16),
            pltpu.VMEM((2, KV // 2, SEQ, HEADS * VD), BF16),
            pltpu.VMEM((ROW, ROW, 64, 128), BF16),
            pltpu.VMEM((ROW, ROW, 2, 32, 128), BF16),
            pltpu.SemaphoreType.REGULAR, dma((len(args),)), dma((4,)), dma((4,)), dma((4,)), dma((4,)), dma, dma, dma((4,)), dma((4,)),
            dma, dma, dma, dma, dma, dma((4,)), dma, dma,
        ],
        compiler_params=pltpu.CompilerParams(
            collective_id=0, has_side_effects=True, vmem_limit_bytes=40 * 1024 * 1024
        ),
    )(*(pltpu.with_memory_space_constraint(a, pltpu.HBM) for a in args))
    out, new_memory, new_normalizer, new_stabilizer = pl.pallas_call(
        finish,
        name="finish",
        out_shape=outs,
        in_specs=[pl.BlockSpec(memory_space=pltpu.VMEM)] * 5,
        out_specs=[pl.BlockSpec(memory_space=pltpu.HBM)] * 4,
        scratch_shapes=[pltpu.VMEM((64, 128), BF16), dma((SEQ + 3,))],
        compiler_params=pltpu.CompilerParams(vmem_limit_bytes=8 * 1024 * 1024),
    )(*results)
    return out.T, new_memory, new_normalizer, new_stabilizer.T


def solution(mesh):
    in_specs = (
        P("dp", "kv"), P("kv"), P("kv", "tp"), P("kv", "tp"), P("kv", "tp"), P("kv", "tp"), P(), P("tp"),
        P(("dp", "kv"), "tp", None, None), P(("dp", "kv"), "tp", None), P(("dp", "kv"), "tp"), P("tp", None),
        P("tp", "kv"), P(), P(None, ("kv", "tp")), P(None, ("kv", "tp")), P(("kv", "tp"), None),
    )
    out_specs = (
        P("dp", ("kv", "tp")), P(("dp", "kv"), "tp", None, None), P(("dp", "kv"), "tp", None), P(("dp", "kv"), "tp"),
    )
    return jax.shard_map(body, mesh=mesh, in_specs=in_specs, out_specs=out_specs, check_vma=False)
```
